128 devices in a mesh: sp: 16 (over z, y), tp: 8 (over x, core).
Axes of the slice: x: 4, y: 4, z: 4, core: 2. Of those that a mesh axis runs over, the one named last changes fastest.
Arguments:
- stream_in: bfloat16 [8192, 4096], P('sp', 'tp'), may hold values from -12 to 12
- norm_gain: float32 [2, 4096], replicated, may hold values from 0.1 to 1.9
- value_proj: bfloat16 [2, 4096, 4096], P(None, 'sp', 'tp'), may hold values from -0.09375 to 0.09375
- gate_proj: bfloat16 [2, 4096, 4096], P(None, 'sp', 'tp'), may hold values from -0.09375 to 0.09375
- out_proj: bfloat16 [2, 4096, 4096], P(None, 'sp', 'tp'), may hold values from -0.1875 to 0.1875
- conv_taps: float32 [2, 4, 4096], replicated, may hold values from -3 to 3
- block_gates: bfloat16 [2, 2, 2, 4096, 128], P(None, None, None, 'tp'), may hold values from -0.5 to 0.5
- forget_rate: float32 [2, 2, 4096], replicated, may hold values from 0 to 0.05, as said below
Outputs:
- stream_out: bfloat16 [8192, 4096], P('sp', 'tp')
The draws below stay inside these ranges and needn't reach their ends.
Inputs may be any that keep to these rules, and one draw needn't show every extreme that they name: `forget_rate`: positive.
All inputs are finite; a program needn't handle non-finite values.
Results may differ from the reference program's by a relative error of at most 0.025.
Values may be sent and summed in bfloat16 or wider, within the bound.
A program may use at most 192 MiB of HBM per device.

```python
import math
import jax
import jax.numpy as jnp
from jax import lax

D = 4096
W = 4096
BLK = 128
LAYERS = 2
TOK_DEV = 512
TOKENS = 8192
N_TP = 8


def draw_stream_in(key, part):
    subkeys = jax.random.split(key, 6)
    base = jax.random.normal(subkeys[0], (TOKENS, D), jnp.float32)
    phase = jax.random.uniform(subkeys[1], (), jnp.float32, -math.pi, math.pi)
    position = jnp.arange(D).astype(jnp.float32) / D
    channel_scale = jnp.exp(0.9 * jnp.cos(2.0 * math.pi * position + phase) + jax.random.uniform(subkeys[2], (D,), jnp.float32, -0.3, 0.3))
    nblocks = (TOKENS + TOK_DEV - 1) // TOK_DEV
    block_mix = jax.random.normal(subkeys[3], (nblocks, D), jnp.float32)
    block_mix = block_mix * jax.random.uniform(subkeys[4], (nblocks, 1), jnp.float32, 0.5, 3.0)
    row_block = jnp.arange(TOKENS) // TOK_DEV
    result = base * channel_scale + block_mix[row_block]
    return jnp.clip(result, -12.0, 12.0).astype(jnp.bfloat16)


def draw_forget_rate(key, part):
    subkeys = jax.random.split(key, 3)
    shape = (LAYERS, 2, W)
    keep_share = 0.5
    slow_pick = jax.random.uniform(subkeys[0], shape, jnp.float32) < keep_share
    slow_rate = jnp.exp(jax.random.uniform(subkeys[1], shape, jnp.float32, math.log(0.02), math.log(0.2))) / TOKENS
    fast_hi = max(0.012, 0.4 / TOK_DEV)
    fast_rate = jnp.exp(jax.random.uniform(subkeys[2], shape, jnp.float32, math.log(fast_hi / 4.0), math.log(fast_hi)))
    return jnp.where(slow_pick, slow_rate, fast_rate)


def block_levels(stream_key, extent, shards, smallest, top_value):
    level, own = 1.0, jax.random.fold_in(stream_key, 6)
    for dim, blocks in shards:
        draws = jnp.exp(jax.random.uniform(jax.random.fold_in(own, dim), (blocks,), jnp.float32, smallest / len(shards), top_value / len(shards)))
        level = level * jnp.repeat(draws, extent[dim] // blocks).reshape([-1 if axis == dim else 1 for axis in range(len(extent))])
    return level


def scatter_about(own_key, dims, scale, reach, pieces=(), kind=jnp.bfloat16):
    level = block_levels(own_key, dims, pieces, -0.22, 0.18) if pieces else 1.0
    array = jax.random.normal(own_key, dims, jnp.float32) * scale * level
    return jnp.minimum(jnp.maximum(array, -reach), reach).astype(kind)


def setup_inputs(seed: int = 0) -> dict:
    seeds = jax.random.split(jax.random.key(seed), 9)
    stream_in = draw_stream_in(jax.random.fold_in(seeds[8], 71), 0)
    norm_gain = jnp.clip(1.0 + 0.18 * jax.random.normal(seeds[1], (LAYERS, D), jnp.float32), 0.1, 1.9)
    value_proj = scatter_about(seeds[2], (LAYERS, D, W), D ** -0.5, 0.09375, ((1, 16), (2, 8)))
    gate_proj = scatter_about(seeds[3], (LAYERS, D, W), D ** -0.5, 0.09375, ((1, 16), (2, 8)))
    out_proj = scatter_about(seeds[4], (LAYERS, D, W), (W // 4) ** -0.5, 0.1875, ((1, 16), (2, 8)))
    conv_taps = scatter_about(seeds[5], (LAYERS, 4, W), 0.8, 3.0, (), jnp.float32)
    block_gates = scatter_about(seeds[6], (LAYERS, 2, 2, W, BLK), BLK ** -0.5, 0.5, ((3, 8),))
    forget_rate = draw_forget_rate(jax.random.fold_in(seeds[8], 71), 0)
    return dict(stream_in=stream_in, norm_gain=norm_gain, value_proj=value_proj, gate_proj=gate_proj, out_proj=out_proj, conv_taps=conv_taps, block_gates=block_gates, forget_rate=forget_rate)


GATE_SCALE = 8.0
NORM_EPS = 1e-06

def pair_combine(earlier, latter):
    return (earlier[0] * latter[0], latter[0] * earlier[1] + latter[1])

def convolve(padded, taps_layer, length):
    values = padded.astype(jnp.float32)
    return sum((values[offset:offset + length] * taps_layer[offset] for offset in range(4)))

def gate_inputs(conv_out, gate_layer):
    count, width = conv_out.shape
    block_size = gate_layer.shape[-1]
    nblocks = width // block_size
    blocked = conv_out.reshape(count, nblocks, block_size)
    weights = gate_layer.astype(jnp.float32).reshape(4, nblocks, block_size, block_size)
    pre = jnp.einsum('tnc,gncd->gtnd', blocked, weights, precision=lax.Precision.HIGHEST)
    return pre.reshape(4, count, width)

def decay_inputs(conv_out, pre, rate_layer, direction):
    recur_gate = jax.nn.sigmoid(pre[2 * direction])
    input_gate = jax.nn.sigmoid(pre[2 * direction + 1])
    log_decay = -GATE_SCALE * recur_gate * rate_layer[direction]
    decay = jnp.exp(log_decay)
    drive = jnp.sqrt(-jnp.expm1(2.0 * log_decay)) * input_gate * conv_out
    return (decay, drive)

def reference(stream_in, norm_gain, value_proj, gate_proj, out_proj, conv_taps, block_gates, forget_rate):
    stream = stream_in
    length = stream_in.shape[0]
    group_width = W // N_TP
    for layer_index in range(LAYERS):
        values = stream.astype(jnp.float32)
        scale = lax.rsqrt(lax.optimization_barrier(jnp.mean(values * values, axis=1, keepdims=True)) + NORM_EPS)
        normed = (values * scale * norm_gain[layer_index]).astype(jnp.bfloat16)
        mix_in = jnp.dot(normed, value_proj[layer_index], preferred_element_type=jnp.float32).astype(jnp.bfloat16)
        gate_z = jnp.dot(normed, gate_proj[layer_index], preferred_element_type=jnp.float32).astype(jnp.bfloat16)
        padded = jnp.pad(mix_in, ((2, 1), (0, 0)))
        conv_out = convolve(padded, conv_taps[layer_index], length)
        pre = gate_inputs(conv_out, block_gates[layer_index])
        fwd_decay, fwd_drive = decay_inputs(conv_out, pre, forget_rate[layer_index], 0)
        bwd_decay, bwd_drive = decay_inputs(conv_out, pre, forget_rate[layer_index], 1)
        _, fwd_state = lax.associative_scan(pair_combine, (fwd_decay, fwd_drive), axis=0)
        _, bwd_flip = lax.associative_scan(pair_combine, (jnp.flip(bwd_decay, 0), jnp.flip(bwd_drive, 0)), axis=0)
        both = fwd_state + jnp.flip(bwd_flip, 0)
        mixed = (both * jax.nn.silu(gate_z.astype(jnp.float32))).astype(jnp.bfloat16)
        branch = jnp.zeros((length, D), jnp.float32)
        for group in range(N_TP):
            part = lax.dot_general(mixed[:, group * group_width:(group + 1) * group_width], out_proj[layer_index][:, group * group_width:(group + 1) * group_width], (((1,), (1,)), ((), ())), preferred_element_type=jnp.float32)
            rounded = lax.optimization_barrier(part.astype(jnp.bfloat16))
            branch = branch + rounded.astype(jnp.float32)
        stream = (values + branch).astype(jnp.bfloat16)
    return stream
```

```python
import functools

import jax
import jax.numpy as jnp
from jax import lax
from jax.experimental import pallas as pl
from jax.experimental.pallas import tpu as pltpu
from jax.sharding import PartitionSpec as P

GATE_SCALE = 8.0
NORM_EPS = 1e-06
MESH = pl.DeviceIdType.MESH
F32 = jnp.float32
BF16 = jnp.bfloat16
SEG = 8
ROWS = 64


def remote(src, dst, send_sem, recv_sem, dev):
    return pltpu.make_async_remote_copy(
        src_ref=src, dst_ref=dst, send_sem=send_sem, recv_sem=recv_sem, device_id=dev, device_id_type=MESH
    )


def greet(axis, count, me):
    barrier = pltpu.get_barrier_semaphore()
    for step in range(1, count):
        pl.semaphore_signal(barrier, inc=1, device_id={axis: lax.rem(me + step, count)}, device_id_type=MESH)
    return lambda: pl.semaphore_wait(barrier, count - 1)


def sigmoid(v):
    return 1.0 / (1.0 + jnp.exp(-v))


def drive_square(y):
    terms = [1.0, -1.0 / 2, 1.0 / 6, -1.0 / 24, 1.0 / 120, -1.0 / 720, 1.0 / 5040, -1.0 / 40320, 1.0 / 362880]
    total = jnp.full_like(y, terms[-1])
    for term in terms[-2::-1]:
        total = total * y + term
    return total * y


def in_row_steps(rows, body, size=ROWS):
    def step(k, carry):
        body(pl.ds(pl.multiple_of(k * size, size), size))
        return carry

    lax.fori_loop(0, rows // size, step, 0)


class Ring:
    def __init__(self, me, count):
        chips = count // 2
        self.chips = chips
        self.me = me
        self.x = me // 2
        self.c = lax.rem(me, 2)
        self.sib = self.x * 2 + 1 - self.c

    def at(self, step, other=False):
        core = 1 - self.c if other else self.c
        return lax.rem(self.x + step + self.chips, self.chips) * 2 + core


def gather_start(ring, own_ref, gain_ref, xg, ssg, send, recv, ssend, srecv, count):
    me = ring.me
    tokens = own_ref.shape[0]

    def fill(rows):
        v = own_ref[rows, :].astype(F32)
        xg[me, rows, :] = (v * gain_ref[...]).astype(BF16)

    in_row_steps(tokens, fill)
    half = tokens // 2
    a, b = pl.ds(0, half), pl.ds(half, half)
    right, left = ring.at(1), ring.at(-1)
    for k, (rows, dev) in enumerate(((a, right), (b, right), (b, left), (a, left))):
        part = xg.at[me, rows]
        remote(part, part, send.at[k], recv.at[k], {"tp": dev}).start()
    remote(xg.at[me], xg.at[me], send.at[6], recv.at[6], {"tp": ring.sib}).start()
    for k in range(tokens // 128):
        v = own_ref[pl.ds(k * 128, 128), :].astype(F32)
        total = jnp.sum(v * v, axis=1, keepdims=True)
        ssg[me, :, pl.ds(k * 128, 128)] = jnp.broadcast_to(total, (128, 128)).T[0:8, :]
    for step in range(1, count):
        dev = lax.rem(me + step, count)
        remote(ssg.at[me], ssg.at[me], ssend.at[dev], srecv.at[me], {"tp": dev}).start()


def gather_finish(ring, xg, ssg, send, recv, ssend, srecv, count):
    me = ring.me
    half = xg.shape[1] // 2
    a, b = pl.ds(0, half), pl.ds(half, half)
    right, left, far = ring.at(1), ring.at(-1), ring.at(2)

    def got(owner, rows, k):
        part = xg.at[owner, rows]
        remote(part, part, send.at[k], recv.at[k], {"tp": ring.sib}).wait_recv()
        return part

    def push(part, k, dev):
        remote(part, part, send.at[k], recv.at[k], {"tp": dev}).start()

    part = got(left, a, 0)
    push(part, 4, right)
    push(part, 7, ring.sib)
    part = got(right, b, 2)
    push(part, 5, left)
    push(part, 8, ring.sib)
    push(got(left, b, 1), 9, ring.sib)
    push(got(right, a, 3), 10, ring.sib)
    push(got(far, a, 4), 11, ring.sib)
    push(got(far, b, 5), 12, ring.sib)
    whole = xg.at[ring.sib]
    remote(whole, whole, send.at[6], recv.at[6], {"tp": ring.sib}).wait()
    owners = {7: (-1, a), 8: (1, b), 9: (-1, b), 10: (1, a), 11: (2, a), 12: (2, b)}
    for k, (step, rows) in owners.items():
        part = xg.at[ring.at(step, other=True), rows]
        remote(part, part, send.at[k], recv.at[k], {"tp": ring.sib}).wait()
    for k in range(6):
        part = xg.at[me, a]
        remote(part, part, send.at[k], recv.at[k], {"tp": right}).wait_send()
    for step in range(1, count):
        dev = lax.rem(me + step, count)
        remote(ssg.at[dev], ssg.at[dev], ssend.at[dev], srecv.at[dev], {"tp": dev}).wait()


def gather_kernel(count, own_ref, gain_ref, xg, ssg, send, recv, ssend, srecv):
    me = lax.axis_index("tp")
    ring = Ring(me, count)
    greet("tp", count, me)()
    gather_start(ring, own_ref, gain_ref, xg, ssg, send, recv, ssend, srecv, count)
    gather_finish(ring, xg, ssg, send, recv, ssend, srecv, count)


GATHER_SEMS = 13


def gather_call(own, gain, count, ident):
    tokens, feats = own.shape
    vmem = pl.BlockSpec(memory_space=pltpu.VMEM)
    return pl.pallas_call(
        functools.partial(gather_kernel, count),
        out_shape=(
            jax.ShapeDtypeStruct((count, tokens, feats), BF16),
            jax.ShapeDtypeStruct((count, 8, tokens), F32),
        ),
        in_specs=[vmem, vmem],
        out_specs=(vmem, vmem),
        scratch_shapes=[
            pltpu.SemaphoreType.DMA((GATHER_SEMS,)),
            pltpu.SemaphoreType.DMA((GATHER_SEMS,)),
            pltpu.SemaphoreType.DMA((count,)),
            pltpu.SemaphoreType.DMA((count,)),
        ],
        compiler_params=pltpu.CompilerParams(collective_id=ident, has_side_effects=True),
        cost_estimate=pl.CostEstimate(flops=20_000_000_000, bytes_accessed=8_000_000, transcendentals=0),
        name="tp_gather",
    )(own, gain)


def mix_kernel(
    count, features, xg_hbm, ssg, w_hbm, taps, rate, gates, out,
    xv, wv, acc_v, acc_g, mixb, mpad, sil, conv, convb, pre, a_f, u_f, a_b, u_b, col,
    halo_p, halo_n, seg, ent, msg, slots, ld, hsend, hrecv, csend, crecv,
):
    me = lax.axis_index("sp")
    tokens, width = mixb.shape
    blocks = xv.shape[0]
    depth = xv.shape[2]
    joined = greet("sp", count, me)

    def loads(p):
        rows = pl.ds(pl.multiple_of(p * depth, depth), depth)
        return (
            pltpu.make_async_copy(xg_hbm.at[p], xv.at[p], ld.at[0, p]),
            pltpu.make_async_copy(w_hbm.at[0, rows], wv.at[0, p], ld.at[1, p]),
            pltpu.make_async_copy(w_hbm.at[1, rows], wv.at[1, p], ld.at[2, p]),
        )

    for p in range(blocks):
        for copy in loads(p):
            copy.start()
    total = jnp.sum(ssg[...], axis=0)
    scale = lax.rsqrt(total / features + NORM_EPS)
    for k in range(tokens // 128):
        part = jnp.broadcast_to(scale[0:1, k * 128 : (k + 1) * 128], (128, 128))
        col[pl.ds(k * 128, 128), :] = part.T

    for p in range(blocks):
        for copy in loads(p):
            copy.wait()
        for side, acc in ((0, acc_v), (1, acc_g)):
            term = jnp.dot(xv[p], wv[side, p], preferred_element_type=F32)
            acc[...] = term if p == 0 else acc[...] + term

    def finish_v(rows):
        wide = jnp.concatenate([col[rows, :]] * (width // 128), axis=1)
        mix = (acc_v[rows, :] * wide).astype(BF16)
        mixb[rows, :] = mix
        acc_v[rows, :] = mix.astype(F32)

    in_row_steps(tokens, finish_v, 32)
    joined()
    head, tail = mixb.at[pl.ds(0, 16)], mixb.at[pl.ds(tokens - 16, 16)]
    to_next = remote(tail, halo_p, hsend.at[0], hrecv.at[0], {"sp": lax.rem(me + 1, count)})
    to_prev = remote(head, halo_n, hsend.at[1], hrecv.at[1], {"sp": lax.rem(me + count - 1, count)})
    to_next.start()
    to_prev.start()

    def finish_g(rows):
        wide = jnp.concatenate([col[rows, :]] * (width // 128), axis=1)
        gate = (acc_g[rows, :] * wide).astype(BF16).astype(F32)
        sil[rows, :] = gate * sigmoid(gate)
        mpad[pl.ds(pl.multiple_of(rows.start + 16, 16), rows.size), :] = acc_v[rows, :]

    in_row_steps(tokens, finish_g, 32)
    to_next.wait()
    to_prev.wait()
    sub = lax.broadcasted_iota(jnp.int32, (SEG, width), 0)
    before = halo_p[...].astype(F32)
    after = halo_n[...].astype(F32)
    for k in range(2):
        edge = jnp.where(me > 0, before[8 * k + 7 : 8 * k + 8, :], 0.0)
        blk = acc_v[pl.ds(tokens - 16 + 8 * k, 8), :]
        mpad[pl.ds(8 * k, 8), :] = jnp.where(sub == 0, jnp.broadcast_to(edge, (SEG, width)), pltpu.roll(blk, 1, 0))
    edge = jnp.where(me < count - 1, after[0:1, :], 0.0)
    blk = acc_v[pl.ds(0, 8), :]
    mpad[pl.ds(tokens + 16, 8), :] = jnp.where(
        sub == SEG - 1, jnp.broadcast_to(edge, (SEG, width)), pltpu.roll(blk, SEG - 1, 0)
    )

    def convolve(rows):
        parts = [
            mpad[pl.ds(pl.multiple_of(rows.start + 8 * k, 8), rows.size), :] * taps[k : k + 1, :] for k in range(4)
        ]
        value = (parts[0] + parts[1]) + (parts[2] + parts[3])
        conv[rows, :] = value
        convb[rows, :] = value.astype(BF16)

    in_row_steps(tokens, convolve, 32)
    for b in range(width // 128):
        pre[b] = jnp.dot(convb[:, b * 128 : (b + 1) * 128], gates[b], preferred_element_type=F32)

    for b in range(width // 128):
        lanes = pl.ds(b * 128, 128)
        rates = [-GATE_SCALE * rate[e : e + 1, lanes] for e in range(2)]

        def body(k, carry, b=b, lanes=lanes, rates=rates):
            p_f, h_f, p_b, h_b = carry
            rows = pl.ds(pl.multiple_of(k * ROWS, ROWS), ROWS)
            cv = conv[rows, lanes]
            kept = []
            for e, (a_ref, u_ref) in enumerate(((a_f, u_f), (a_b, u_b))):
                r = sigmoid(pre[b, rows, 256 * e : 256 * e + 128])
                i = sigmoid(pre[b, rows, 256 * e + 128 : 256 * e + 256])
                log_a = rates[e] * r
                decay = jnp.exp(log_a)
                drive = jnp.sqrt(drive_square(-2.0 * log_a)) * i * cv
                a_ref[rows, lanes] = decay
                u_ref[rows, lanes] = drive
                kept.append((decay, drive))
            for j in range(ROWS // 8):
                at = slice(8 * j, 8 * j + 8)
                d, u = kept[0][0][at], kept[0][1][at]
                h_f = d * h_f + u
                p_f = p_f * d
                d, u = kept[1][0][at], kept[1][1][at]
                h_b = h_b + p_b * u
                p_b = p_b * d
            return p_f, h_f, p_b, h_b

        one, zero = jnp.ones((SEG, 128), F32), jnp.zeros((SEG, 128), F32)
        done = lax.fori_loop(0, tokens // ROWS, body, (one, zero, one, zero))
        for k in range(4):
            seg[k, :, lanes] = done[k]

    sides = ((0, range(SEG)), (2, range(SEG - 1, -1, -1)))
    for e, (k, order) in enumerate(sides):
        prod = jnp.ones((1, width), F32)
        state = jnp.zeros((1, width), F32)
        for s in order:
            d = seg[k, s : s + 1, :]
            state = d * state + seg[k + 1, s : s + 1, :]
            prod = prod * d
        for b in range(width // 128):
            msg[e, b : b + 1, :] = prod[:, b * 128 : (b + 1) * 128]
            msg[e, 4 + b : 5 + b, :] = state[:, b * 128 : (b + 1) * 128]
    for step in range(1, count):
        dev = lax.rem(me + step, count)
        side = jnp.where(dev > me, 0, 1)
        remote(msg.at[side], slots.at[me], csend.at[dev], crecv.at[me], {"sp": dev}).start()
    slots[me] = jnp.zeros((8, 128), F32)
    for step in range(1, count):
        dev = lax.rem(me + step, count)
        remote(msg.at[0], slots.at[dev], csend.at[dev], crecv.at[dev], {"sp": dev}).wait()
    for e, (k, order) in enumerate(sides):
        carry = jnp.zeros((4, 128), F32)
        for q in range(count) if e == 0 else range(count - 1, -1, -1):
            live = (q < me) if e == 0 else (q > me)
            slot = slots[q]
            carry = jnp.where(live, slot[0:4] * carry + slot[4:8], carry)
        state = jnp.concatenate([carry[b : b + 1, :] for b in range(width // 128)], axis=1)
        for s in order:
            ent[e, s : s + 1, :] = state
            state = seg[k, s : s + 1, :] * state + seg[k + 1, s : s + 1, :]

    steps = tokens // SEG

    def again(k, carry):
        h_f, h_b = carry
        for j in range(4):
            fwd = pl.ds(pl.multiple_of((4 * k + j) * SEG, SEG), SEG)
            bwd = pl.ds(pl.multiple_of((steps - 1 - 4 * k - j) * SEG, SEG), SEG)
            h_f = a_f[fwd, :] * h_f + u_f[fwd, :]
            u_f[fwd, :] = h_f
            h_b = a_b[bwd, :] * h_b + u_b[bwd, :]
            u_b[bwd, :] = h_b
        return h_f, h_b

    lax.fori_loop(0, steps // 4, again, (ent[0], ent[1]))

    def gated(rows):
        out[rows, :] = ((u_f[rows, :] + u_b[rows, :]) * sil[rows, :]).astype(BF16)

    in_row_steps(tokens, gated, 32)


def mix_call(xg, ssg, weights, taps, rate, gates, count, ident):
    blocks, tokens, depth = xg.shape
    width = weights.shape[2]
    vmem = pl.BlockSpec(memory_space=pltpu.VMEM)
    hbm = pl.BlockSpec(memory_space=pl.ANY)
    full = pltpu.VMEM((tokens, width), F32)
    half = pltpu.VMEM((tokens, width), BF16)
    return pl.pallas_call(
        functools.partial(mix_kernel, count, float(blocks * depth)),
        out_shape=jax.ShapeDtypeStruct((tokens, width), BF16),
        in_specs=[hbm, vmem, hbm, vmem, vmem, vmem],
        out_specs=vmem,
        scratch_shapes=[
            pltpu.VMEM((blocks, tokens, depth), BF16),
            pltpu.VMEM((2, blocks, depth, width), BF16),
            full, full, half,
            pltpu.VMEM((tokens + 24, width), F32),
            full, full, half,
            pltpu.VMEM((width // 128, tokens, 512), F32),
            full, full, full, full,
            pltpu.VMEM((tokens, 128), F32),
            pltpu.VMEM((16, width), BF16),
            pltpu.VMEM((16, width), BF16),
            pltpu.VMEM((4, SEG, width), F32),
            pltpu.VMEM((2, SEG, width), F32),
            pltpu.VMEM((2, 8, 128), F32),
            pltpu.VMEM((count, 8, 128), F32),
            pltpu.SemaphoreType.DMA((3, blocks)),
            pltpu.SemaphoreType.DMA((2,)),
            pltpu.SemaphoreType.DMA((2,)),
            pltpu.SemaphoreType.DMA((count,)),
            pltpu.SemaphoreType.DMA((count,)),
        ],
        compiler_params=pltpu.CompilerParams(collective_id=ident, has_side_effects=True),
        cost_estimate=pl.CostEstimate(flops=20_000_000_000, bytes_accessed=14_000_000, transcendentals=0),
        name="mix",
    )(xg, ssg, weights, taps, rate, gates)


def reduce_kernel(count, mixed, w_hbm, own, out, wv, psend, precv, pown, fbuf, far_in, nbuf, near_in, ld, ds, dr, rs, rr):
    me = lax.axis_index("tp")
    ring = Ring(me, count)
    tokens, feats = own.shape
    half = tokens // 2
    a, b = pl.ds(0, half), pl.ds(half, half)
    right, left = ring.at(1), ring.at(-1)
    joined = greet("tp", count, me)
    order = (2, 1, -1, 0)

    def load(k, other):
        block = ring.at(order[k], other=other)
        rows = pl.ds(pl.multiple_of(block * feats, feats), feats)
        return pltpu.make_async_copy(w_hbm.at[rows], wv.at[2 * k + 1 - int(other)], ld.at[2 * k + 1 - int(other)])

    for k in range(4):
        load(k, True).start()
        load(k, False).start()
    joined()

    def product(k, other):
        load(k, other).wait()
        return lax.dot_general(
            mixed[...], wv[2 * k + 1 - int(other)], (((1,), (1,)), ((), ())), preferred_element_type=F32
        )

    def across(k):
        return remote(psend.at[k], precv.at[k], ds.at[k], dr.at[k], {"tp": ring.sib})

    def send(k, src, dst, dev):
        copy = remote(src, dst, rs.at[k], rr.at[k], {"tp": dev})
        copy.start()
        return copy

    def paired(k, rows, into=None):
        def body(r):
            at = pl.ds(pl.multiple_of(rows.start + r.start, 32), r.size)
            value = pown[k, at, :] + precv[k, at, :].astype(F32)
            if into is None:
                pown[k, at, :] = value
            else:
                into[at if into.shape[0] == tokens else r, :] = value.astype(BF16)

        in_row_steps(rows.size, body, 32)

    for k in range(4):
        psend[k] = product(k, True).astype(BF16)
        across(k).start()
        pown[k] = product(k, False)
        if k == 1:
            across(0).wait_recv()
            paired(0, a, fbuf)
            send(0, fbuf.at[a], far_in.at[0], right)
            paired(0, b, fbuf)
            send(1, fbuf.at[b], far_in.at[1], left)
        if k == 2:
            across(1).wait_recv()
            paired(1, b, nbuf.at[0])
            send(2, nbuf.at[0], near_in.at[0], right)
            paired(1, a)
        if k == 3:
            across(2).wait_recv()
            paired(2, a, nbuf.at[1])
            send(3, nbuf.at[1], near_in.at[1], left)
            paired(2, b)
    across(3).wait_recv()
    paired(3, pl.ds(0, tokens))

    def arrived(k, src, dst):
        remote(src, dst, rs.at[k], rr.at[k], {"tp": right}).wait_recv()

    def merged(k, rows, src, into):
        def body(r):
            at = pl.ds(pl.multiple_of(rows.start + r.start, 32), r.size)
            into[r, :] = (pown[k, at, :] + src[r, :].astype(F32)).astype(BF16)

        in_row_steps(half, body, 32)

    arrived(0, fbuf.at[a], far_in.at[0])
    merged(1, a, far_in.at[0], nbuf.at[2])
    send(4, nbuf.at[2], near_in.at[2], right)
    arrived(1, fbuf.at[b], far_in.at[1])
    merged(2, b, far_in.at[1], nbuf.at[3])
    send(5, nbuf.at[3], near_in.at[3], left)
    for k in range(4):
        arrived(2 + k, nbuf.at[k], near_in.at[k])

    def total(rows, one, two):
        def body(r):
            at = pl.ds(pl.multiple_of(rows.start + r.start, 32), r.size)
            branch = pown[3, at, :] + near_in[one, r, :].astype(F32) + near_in[two, r, :].astype(F32)
            out[at, :] = (own[at, :].astype(F32) + branch).astype(BF16)

        in_row_steps(half, body, 32)

    total(a, 1, 2)
    total(b, 0, 3)
    for k in range(4):
        across(k).wait_send()
    for k in range(6):
        remote(nbuf.at[0], near_in.at[0], rs.at[k], rr.at[k], {"tp": right}).wait_send()


def reduce_call(mixed, weights, own, count, ident):
    tokens, width = mixed.shape
    feats = own.shape[1]
    vmem = pl.BlockSpec(memory_space=pltpu.VMEM)
    hbm = pl.BlockSpec(memory_space=pl.ANY)
    half = tokens // 2
    return pl.pallas_call(
        functools.partial(reduce_kernel, count),
        out_shape=jax.ShapeDtypeStruct((tokens, feats), BF16),
        in_specs=[vmem, hbm, vmem],
        out_specs=vmem,
        scratch_shapes=[
            pltpu.VMEM((count, feats, width), BF16),
            pltpu.VMEM((4, tokens, feats), BF16),
            pltpu.VMEM((4, tokens, feats), BF16),
            pltpu.VMEM((4, tokens, feats), F32),
            pltpu.VMEM((tokens, feats), BF16),
            pltpu.VMEM((2, half, feats), BF16),
            pltpu.VMEM((4, half, feats), BF16),
            pltpu.VMEM((4, half, feats), BF16),
            pltpu.SemaphoreType.DMA((count,)),
            pltpu.SemaphoreType.DMA((4,)),
            pltpu.SemaphoreType.DMA((4,)),
            pltpu.SemaphoreType.DMA((6,)),
            pltpu.SemaphoreType.DMA((6,)),
        ],
        compiler_params=pltpu.CompilerParams(collective_id=ident, has_side_effects=True),
        cost_estimate=pl.CostEstimate(flops=20_000_000_000, bytes_accessed=8_000_000, transcendentals=0),
        name="tp_reduce",
    )(mixed, weights, own)


def per_device(
    n_sp, n_tp, stream_in, norm_gain, value_proj, gate_proj, out_proj, conv_taps, block_gates, forget_rate
):
    tp_rank = lax.axis_index("tp")
    tokens, feats = stream_in.shape
    width = value_proj.shape[2]
    layers = value_proj.shape[0]
    steps = tokens // SEG

    def gathered(array, dim):
        return lax.all_gather(array, "sp", axis=dim, tiled=True)

    def own_part(array, size):
        return lax.dynamic_slice_in_dim(array, tp_rank * size, size, array.ndim - 1)

    weights = []
    for layer in range(layers):
        pair = jnp.stack([value_proj[layer], gate_proj[layer]])
        weights.append((gathered(pair, 1), gathered(out_proj[layer], 0)))
    gain = own_part(norm_gain, feats)
    taps = own_part(conv_taps, width)
    rate = own_part(forget_rate, width)
    blocks = width // 128
    gates = block_gates.reshape(layers, 4, blocks, 128, 128).transpose(0, 2, 3, 1, 4).reshape(layers, blocks, 128, 512)
    stream = stream_in.reshape(SEG, steps, feats).transpose(1, 0, 2).reshape(tokens, feats)
    for layer in range(layers):
        both, out_w = weights[layer]
        xg, ssg = gather_call(stream, gain[layer : layer + 1], n_tp, 3 * layer)
        mixed = mix_call(xg, ssg, both, taps[layer], rate[layer], gates[layer], n_sp, 3 * layer + 1)
        stream = reduce_call(mixed, out_w, stream, n_tp, 3 * layer + 2)
    return stream.reshape(steps, SEG, feats).transpose(1, 0, 2).reshape(tokens, feats)


def solution(mesh):
    placed = (
        P("sp", "tp"),
        P(),
        P(None, "sp", "tp"),
        P(None, "sp", "tp"),
        P(None, "sp", "tp"),
        P(),
        P(None, None, None, "tp", None),
        P(),
    )
    body = functools.partial(per_device, mesh.shape["sp"], mesh.shape["tp"])
    return jax.shard_map(body, mesh=mesh, in_specs=placed, out_specs=P("sp", "tp"), check_vma=False)
```

```python
import functools

import jax
import jax.numpy as jnp
from jax import lax
from jax.experimental import pallas as pl
from jax.experimental.pallas import tpu as pltpu
from jax.sharding import PartitionSpec as P

GATE_SCALE = 8.0
NORM_EPS = 1e-06
MESH = pl.DeviceIdType.MESH
F32 = jnp.float32
BF16 = jnp.bfloat16
SEG = 8
ROWS = 64


def remote(src, dst, send_sem, recv_sem, dev):
    return pltpu.make_async_remote_copy(
        src_ref=src, dst_ref=dst, send_sem=send_sem, recv_sem=recv_sem, device_id=dev, device_id_type=MESH
    )


def greet(groups):
    barrier = pltpu.get_barrier_semaphore()
    for axis, count, me in groups:
        for step in range(1, count):
            pl.semaphore_signal(barrier, inc=1, device_id={axis: lax.rem(me + step, count)}, device_id_type=MESH)
    pl.semaphore_wait(barrier, sum(count - 1 for _, count, _ in groups))


def sigmoid(v):
    return 1.0 / (1.0 + jnp.exp(-v))


def drive_square(y):
    terms = [1.0, -1.0 / 2, 1.0 / 6, -1.0 / 24, 1.0 / 120, -1.0 / 720, 1.0 / 5040, -1.0 / 40320, 1.0 / 362880]
    total = jnp.full_like(y, terms[-1])
    for term in terms[-2::-1]:
        total = total * y + term
    return total * y


def in_row_steps(rows, body, size=ROWS):
    def step(k, carry):
        body(pl.ds(pl.multiple_of(k * size, size), size))
        return carry

    lax.fori_loop(0, rows // size, step, 0)


class Ring:
    def __init__(self, me, count):
        chips = count // 2
        self.chips = chips
        self.me = me
        self.x = me // 2
        self.c = lax.rem(me, 2)
        self.sib = self.x * 2 + 1 - self.c

    def at(self, step, other=False):
        core = 1 - self.c if other else self.c
        return lax.rem(self.x + step + self.chips, self.chips) * 2 + core


def gather_start(ring, own_ref, gain, xg, ssg, send, recv, ssend, srecv, count):
    me = ring.me
    tokens = own_ref.shape[0]

    def fill(rows):
        v = own_ref[rows, :].astype(F32)
        xg[me, rows, :] = (v * gain).astype(BF16)

    in_row_steps(tokens, fill)
    half = tokens // 2
    a, b = pl.ds(0, half), pl.ds(half, half)
    right, left = ring.at(1), ring.at(-1)
    for k, (rows, dev) in enumerate(((a, right), (b, right), (b, left), (a, left))):
        part = xg.at[me, rows]
        remote(part, part, send.at[k], recv.at[k], {"tp": dev}).start()
    remote(xg.at[me], xg.at[me], send.at[6], recv.at[6], {"tp": ring.sib}).start()
    for k in range(tokens // 128):
        v = own_ref[pl.ds(k * 128, 128), :].astype(F32)
        total = jnp.sum(v * v, axis=1, keepdims=True)
        ssg[me, :, pl.ds(k * 128, 128)] = jnp.broadcast_to(total, (128, 128)).T[0:8, :]
    for step in range(1, count):
        dev = lax.rem(me + step, count)
        remote(ssg.at[me], ssg.at[me], ssend.at[dev], srecv.at[me], {"tp": dev}).start()


def gather_finish(ring, xg, ssg, send, recv, ssend, srecv, count, pump):
    me = ring.me
    half = xg.shape[1] // 2
    a, b = pl.ds(0, half), pl.ds(half, half)
    right, left, far = ring.at(1), ring.at(-1), ring.at(2)

    def got(owner, rows, k):
        part = xg.at[owner, rows]
        remote(part, part, send.at[k], recv.at[k], {"tp": ring.sib}).wait_recv()
        return part

    def push(part, k, dev):
        remote(part, part, send.at[k], recv.at[k], {"tp": dev}).start()

    part = got(left, a, 0)
    push(part, 4, right)
    push(part, 7, ring.sib)
    part = got(right, b, 2)
    push(part, 5, left)
    push(part, 8, ring.sib)
    pump()
    push(got(left, b, 1), 9, ring.sib)
    push(got(right, a, 3), 10, ring.sib)
    pump()
    push(got(far, a, 4), 11, ring.sib)
    push(got(far, b, 5), 12, ring.sib)
    pump()
    whole = xg.at[ring.sib]
    remote(whole, whole, send.at[6], recv.at[6], {"tp": ring.sib}).wait()
    owners = {7: (-1, a), 8: (1, b), 9: (-1, b), 10: (1, a), 11: (2, a), 12: (2, b)}
    for k, (step, rows) in owners.items():
        part = xg.at[ring.at(step, other=True), rows]
        remote(part, part, send.at[k], recv.at[k], {"tp": ring.sib}).wait()
    for k in range(6):
        part = xg.at[me, a]
        remote(part, part, send.at[k], recv.at[k], {"tp": right}).wait_send()
    for step in range(1, count):
        dev = lax.rem(me + step, count)
        remote(ssg.at[dev], ssg.at[dev], ssend.at[dev], srecv.at[dev], {"tp": dev}).wait()


class Weights:
    def __init__(self, me, side, wvg, wo, gsend, grecv):
        self.y, self.z, self.side = lax.rem(me, side), me // side, side
        self.wvg, self.wo, self.gsend, self.grecv = wvg, wo, gsend, grecv
        self.waited = set()

    def idx(self, p, i, j):
        dy, dz = (i, j) if p == 0 else (j, i)
        return lax.rem(self.z + dz + self.side, self.side) * self.side + lax.rem(self.y + dy + self.side, self.side)

    def ref(self, unit, p, at):
        if unit % 2 == 0:
            return self.wvg.at[unit // 2, p, at]
        half = self.wo.shape[2] // 2
        return self.wo.at[unit // 2, at, pl.ds(p * half, half)]

    def push(self, unit, p, i, j, axis, d):
        ref = self.ref(unit, p, self.idx(p, i, j))
        di, dj = (d, 0) if axis == 0 else (0, d)
        slot = ((i - di) % 4) * 4 + (j - dj) % 4
        remote(
            ref, ref, self.gsend.at[2 * unit + p], self.grecv.at[2 * unit + p, slot], {"sp": self.idx(p, di, dj)}
        ).start()

    def arrive(self, unit, p, i, j):
        key = (unit, p, i % 4, j % 4)
        if key in self.waited or (i % 4, j % 4) == (0, 0):
            return
        self.waited.add(key)
        ref = self.ref(unit, p, self.idx(p, i, j))
        slot = (i % 4) * 4 + j % 4
        remote(
            ref, ref, self.gsend.at[2 * unit + p], self.grecv.at[2 * unit + p, slot], {"sp": self.idx(p, 1, 0)}
        ).wait_recv()

    def group(self, unit, p, i):
        for j in (0, -1, 1, 2):
            self.arrive(unit, p, i, j)

    def all(self, unit):
        for p in range(2):
            for i in (0, -1, 1, 2):
                self.group(unit, p, i)

    def opening(self, unit):
        for axis in range(2):
            for p in range(2):
                for d in (1, -1):
                    self.push(unit, p, 0, 0, axis, d)

    def events(self, unit):
        first = 1 if unit in (0, 3) else -1

        def turn(p, i, forward=None):
            def run():
                self.arrive(unit, p, i, 0)
                if forward:
                    self.push(unit, p, i, 0, 0, forward)
                for d in (1, -1):
                    self.push(unit, p, i, 0, 1, d)

            return run

        def relay(p, i):
            d = 1 if (i + unit) % 2 == 0 else -1

            def run():
                self.arrive(unit, p, i, -d)
                self.push(unit, p, i, -d, 1, d)

            return run

        both = range(2)
        early = [turn(p, -first, first) for p in both] + [turn(p, first) for p in both]
        early += [relay(p, 0) for p in both] + [turn(p, 2) for p in both]
        late = [relay(p, i) for i in (-1, 1) for p in both]
        last = [relay(p, 2) for p in both]
        return early, late, last

    def drain(self, unit):
        for p in range(2):
            if unit % 2 == 0:
                ref = self.wvg.at[unit // 2, p, pl.ds(0, 15)]
            else:
                half = self.wo.shape[2] // 2
                ref = self.wo.at[unit // 2, pl.ds(0, 15), pl.ds(p * half, half)]
            remote(ref, ref, self.gsend.at[2 * unit + p], self.grecv.at[2 * unit + p, 0], {"sp": self.idx(p, 1, 0)}).wait_send()


def whole_kernel(
    layers, n_sp, n_tp, features,
    stream_ref, gain_ref, wv_hbm, wg_hbm, wo_hbm, taps_ref, gates_ref, rate_ref, out,
    wvg, wo, xg, ssg, own, acc, mixb, mpad, sil, conv, convb, big, a_f, u_f, a_b, u_b, col,
    halo_p, halo_n, seg, ent, msg, slots,
    psend, precv, fbuf, far_in, nbuf, near_in,
    ld, gsend, grecv, asend, arecv, ssend, srecv, hsend, hrecv, csend, crecv, ds, dr, rs, rr,
):
    sp, tp = lax.axis_index("sp"), lax.axis_index("tp")
    tokens, width = mixb.shape
    feats = own.shape[1]
    ring = Ring(tp, n_tp)
    net = Weights(sp, 4, wvg, wo, gsend, grecv)
    pre = pown = big
    lanes_own = pl.ds(pl.multiple_of(tp * width, width), width)
    right, left = ring.at(1), ring.at(-1)

    loads = []
    for layer in range(layers):
        loads.append([
            pltpu.make_async_copy(wv_hbm.at[layer], wvg.at[layer, 0, sp], ld.at[3 * layer]),
            pltpu.make_async_copy(wg_hbm.at[layer], wvg.at[layer, 1, sp], ld.at[3 * layer + 1]),
        ])
        loads.append([pltpu.make_async_copy(wo_hbm.at[layer], wo.at[layer, sp], ld.at[3 * layer + 2])])
    for copies in loads:
        for copy in copies:
            copy.start()
    greet((("sp", n_sp, sp), ("tp", n_tp, tp)))

    queue = []

    def opening(unit):
        def run():
            for copy in loads[unit]:
                copy.wait()
            net.opening(unit)

        return run

    parts = [net.events(unit) for unit in range(2 * layers)]
    marks = {}
    queue.append(opening(0))
    for unit, (early, late, last) in enumerate(parts):
        queue.extend(early + late)
        if unit + 1 < len(parts):
            queue.append(opening(unit + 1))
        queue.extend(last)
        marks[unit] = len(queue)
    done = [0]

    def pump(n=1, upto=None):
        stop = min(done[0] + n, len(queue)) if upto is None else max(done[0], marks[upto])
        while done[0] < stop:
            queue[done[0]]()
            done[0] += 1

    def project(layer, p, i):
        def step(j, carry):
            at = net.idx(p, i, j)
            lanes = pl.ds(pl.multiple_of(lax.rem(at, 2) * 256, 256), 256)
            acc[p] += jnp.dot(xg[at // 2, :, lanes], wvg[layer, p, at], preferred_element_type=F32)
            return carry

        lax.fori_loop(0, 4, step, 0)

    def gather_begin(layer, source):
        gain = gain_ref[layer : layer + 1, lanes_own]
        gather_start(ring, source, gain, xg, ssg.at[layer], asend, arecv, ssend.at[layer], srecv.at[layer], n_tp)

    def gather_end(layer, count=1):
        gather_finish(
            ring, xg, ssg.at[layer], asend, arecv, ssend.at[layer], srecv.at[layer], n_tp, lambda: pump(count)
        )

    def column(layer):
        total = jnp.sum(ssg[layer], axis=0)
        scale = lax.rsqrt(total / features + NORM_EPS)
        for k in range(tokens // 128):
            part = jnp.broadcast_to(scale[0:1, k * 128 : (k + 1) * 128], (128, 128))
            col[pl.ds(k * 128, 128), :] = part.T

    def clear(rows):
        zero = jnp.zeros((rows.size, width), F32)
        acc[0, rows, :] = zero
        acc[1, rows, :] = zero

    def mix(layer):
        def finish_v(rows):
            wide = jnp.concatenate([col[rows, :]] * (width // 128), axis=1)
            value = (acc[0, rows, :] * wide).astype(BF16)
            mixb[rows, :] = value
            acc[0, rows, :] = value.astype(F32)

        in_row_steps(tokens, finish_v, 32)
        head, tail = mixb.at[pl.ds(0, 16)], mixb.at[pl.ds(tokens - 16, 16)]
        hs, hr = hsend.at[layer], hrecv.at[layer]
        to_next = remote(tail, halo_p.at[layer], hs.at[0], hr.at[0], {"sp": lax.rem(sp + 1, n_sp)})
        to_prev = remote(head, halo_n.at[layer], hs.at[1], hr.at[1], {"sp": lax.rem(sp + n_sp - 1, n_sp)})
        to_next.start()
        to_prev.start()

        def finish_g(rows):
            wide = jnp.concatenate([col[rows, :]] * (width // 128), axis=1)
            gate = (acc[1, rows, :] * wide).astype(BF16).astype(F32)
            sil[rows, :] = gate * sigmoid(gate)
            mpad[pl.ds(pl.multiple_of(rows.start + 16, 16), rows.size), :] = acc[0, rows, :]

        in_row_steps(tokens, finish_g, 32)
        pump(1)
        to_next.wait()
        to_prev.wait()
        sub = lax.broadcasted_iota(jnp.int32, (SEG, width), 0)
        before = halo_p[layer].astype(F32)
        after = halo_n[layer].astype(F32)
        for k in range(2):
            edge = jnp.where(sp > 0, before[8 * k + 7 : 8 * k + 8, :], 0.0)
            blk = acc[0, pl.ds(tokens - 16 + 8 * k, 8), :]
            mpad[pl.ds(8 * k, 8), :] = jnp.where(
                sub == 0, jnp.broadcast_to(edge, (SEG, width)), pltpu.roll(blk, 1, 0)
            )
        edge = jnp.where(sp < n_sp - 1, after[0:1, :], 0.0)
        blk = acc[0, pl.ds(0, 8), :]
        mpad[pl.ds(tokens + 16, 8), :] = jnp.where(
            sub == SEG - 1, jnp.broadcast_to(edge, (SEG, width)), pltpu.roll(blk, SEG - 1, 0)
        )
        taps = taps_ref[layer, :, lanes_own]

        def convolve(rows):
            terms = [
                mpad[pl.ds(pl.multiple_of(rows.start + 8 * k, 8), rows.size), :] * taps[k : k + 1, :]
                for k in range(4)
            ]
            value = (terms[0] + terms[1]) + (terms[2] + terms[3])
            conv[rows, :] = value
            convb[rows, :] = value.astype(BF16)

        in_row_steps(tokens, convolve, 32)
        for b in range(width // 128):
            maps = jnp.concatenate([gates_ref[layer, g, b] for g in range(4)], axis=1)
            pre[b] = jnp.dot(convb[:, b * 128 : (b + 1) * 128], maps, preferred_element_type=F32)
        pump(1)
        rate_all = -GATE_SCALE * rate_ref[layer, :, lanes_own]
        for b in range(width // 128):
            lanes = pl.ds(b * 128, 128)
            rates = [rate_all[e : e + 1, b * 128 : (b + 1) * 128] for e in range(2)]

            def body(k, carry, b=b, lanes=lanes, rates=rates):
                p_f, h_f, p_b, h_b = carry
                rows = pl.ds(pl.multiple_of(k * ROWS, ROWS), ROWS)
                cv = conv[rows, lanes]
                kept = []
                for e, (a_ref, u_ref) in enumerate(((a_f, u_f), (a_b, u_b))):
                    r = sigmoid(pre[b, rows, 256 * e : 256 * e + 128])
                    i = sigmoid(pre[b, rows, 256 * e + 128 : 256 * e + 256])
                    log_a = rates[e] * r
                    decay = jnp.exp(log_a)
                    drive = jnp.sqrt(drive_square(-2.0 * log_a)) * i * cv
                    a_ref[rows, lanes] = decay
                    u_ref[rows, lanes] = drive
                    kept.append((decay, drive))
                for j in range(ROWS // 8):
                    at = slice(8 * j, 8 * j + 8)
                    d, u = kept[0][0][at], kept[0][1][at]
                    h_f = d * h_f + u
                    p_f = p_f * d
                    d, u = kept[1][0][at], kept[1][1][at]
                    h_b = h_b + p_b * u
                    p_b = p_b * d
                return p_f, h_f, p_b, h_b

            one, zero = jnp.ones((SEG, 128), F32), jnp.zeros((SEG, 128), F32)
            ends = lax.fori_loop(0, tokens // ROWS, body, (one, zero, one, zero))
            for k in range(4):
                seg[k, :, lanes] = ends[k]
            pump(1)

        sides = ((0, range(SEG)), (2, range(SEG - 1, -1, -1)))
        for e, (k, order) in enumerate(sides):
            prod = jnp.ones((1, width), F32)
            state = jnp.zeros((1, width), F32)
            for s in order:
                d = seg[k, s : s + 1, :]
                state = d * state + seg[k + 1, s : s + 1, :]
                prod = prod * d
            for b in range(width // 128):
                msg[layer, e, b : b + 1, :] = prod[:, b * 128 : (b + 1) * 128]
                msg[layer, e, 4 + b : 5 + b, :] = state[:, b * 128 : (b + 1) * 128]
        cs, cr = csend.at[layer], crecv.at[layer]
        for step in range(1, n_sp):
            dev = lax.rem(sp + step, n_sp)
            side = jnp.where(dev > sp, 0, 1)
            remote(msg.at[layer, side], slots.at[layer, sp], cs.at[dev], cr.at[sp], {"sp": dev}).start()
        slots[layer, sp] = jnp.zeros((8, 128), F32)
        pump(1)
        for step in range(1, n_sp):
            dev = lax.rem(sp + step, n_sp)
            remote(msg.at[layer, 0], slots.at[layer, dev], cs.at[dev], cr.at[dev], {"sp": dev}).wait()
        for e, (k, order) in enumerate(sides):
            carry = jnp.zeros((4, 128), F32)
            for q in range(n_sp) if e == 0 else range(n_sp - 1, -1, -1):
                live = (q < sp) if e == 0 else (q > sp)
                slot = slots[layer, q]
                carry = jnp.where(live, slot[0:4] * carry + slot[4:8], carry)
            state = jnp.concatenate([carry[b : b + 1, :] for b in range(width // 128)], axis=1)
            for s in order:
                ent[e, s : s + 1, :] = state
                state = seg[k, s : s + 1, :] * state + seg[k + 1, s : s + 1, :]
        steps = tokens // SEG

        def again(k, carry):
            h_f, h_b = carry
            for j in range(4):
                fwd = pl.ds(pl.multiple_of((4 * k + j) * SEG, SEG), SEG)
                bwd = pl.ds(pl.multiple_of((steps - 1 - 4 * k - j) * SEG, SEG), SEG)
                h_f = a_f[fwd, :] * h_f + u_f[fwd, :]
                u_f[fwd, :] = h_f
                h_b = a_b[bwd, :] * h_b + u_b[bwd, :]
                u_b[bwd, :] = h_b
            return h_f, h_b

        lax.fori_loop(0, steps // 4, again, (ent[0], ent[1]))

        def gated(rows):
            mixb[rows, :] = ((u_f[rows, :] + u_b[rows, :]) * sil[rows, :]).astype(BF16)

        in_row_steps(tokens, gated, 32)

    half = tokens // 2
    top, low = pl.ds(0, half), pl.ds(half, half)

    def reduce(layer, source, target, count):
        order = (2, 1, -1, 0)

        def product(k, other):
            block = ring.at(order[k], other=other)
            terms = [
                lax.dot_general(
                    mixb[...], wo[layer, 2 * block + part], (((1,), (1,)), ((), ())), preferred_element_type=F32
                )
                for part in range(2)
            ]
            return terms

        def across(k):
            return remote(psend.at[k], precv.at[k], ds.at[k], dr.at[k], {"tp": ring.sib})

        def send(k, src, dst, dev):
            remote(src, dst, rs.at[k], rr.at[k], {"tp": dev}).start()

        def paired(k, rows, into=None):
            def body(r):
                at = pl.ds(pl.multiple_of(rows.start + r.start, 32), r.size)
                value = pown[k, at, :] + precv[k, at, :].astype(F32)
                if into is None:
                    pown[k, at, :] = value
                else:
                    into[at if into.shape[0] == tokens else r, :] = value.astype(BF16)

            in_row_steps(rows.size, body, 32)

        for k in range(4):
            for part, term in enumerate(product(k, True)):
                psend[k, :, part * 256 : (part + 1) * 256] = term.astype(BF16)
            across(k).start()
            for part, term in enumerate(product(k, False)):
                pown[k, :, part * 256 : (part + 1) * 256] = term
            if k == 1:
                across(0).wait_recv()
                paired(0, top, fbuf)
                send(0, fbuf.at[top], far_in.at[0], right)
                paired(0, low, fbuf)
                send(1, fbuf.at[low], far_in.at[1], left)
            if k == 2:
                across(1).wait_recv()
                paired(1, low, nbuf.at[0])
                send(2, nbuf.at[0], near_in.at[0], right)
                paired(1, top)
            if k == 3:
                across(2).wait_recv()
                paired(2, top, nbuf.at[1])
                send(3, nbuf.at[1], near_in.at[1], left)
                paired(2, low)
        across(3).wait_recv()
        paired(3, pl.ds(0, tokens))
        pump(count)

        def arrived(k, src, dst):
            remote(src, dst, rs.at[k], rr.at[k], {"tp": right}).wait_recv()

        def merged(k, rows, src, into):
            def body(r):
                at = pl.ds(pl.multiple_of(rows.start + r.start, 32), r.size)
                into[r, :] = (pown[k, at, :] + src[r, :].astype(F32)).astype(BF16)

            in_row_steps(half, body, 32)

        arrived(0, fbuf.at[top], far_in.at[0])
        merged(1, top, far_in.at[0], nbuf.at[2])
        send(4, nbuf.at[2], near_in.at[2], right)
        arrived(1, fbuf.at[low], far_in.at[1])
        merged(2, low, far_in.at[1], nbuf.at[3])
        send(5, nbuf.at[3], near_in.at[3], left)
        pump(count)
        for k in range(4):
            arrived(2 + k, nbuf.at[k], near_in.at[k])
            if k == 1:
                pump(count)

        def total(rows, one, two):
            def body(r):
                at = pl.ds(pl.multiple_of(rows.start + r.start, 32), r.size)
                branch = pown[3, at, :] + near_in[one, r, :].astype(F32) + near_in[two, r, :].astype(F32)
                target[at, :] = (source[at, :].astype(F32) + branch).astype(BF16)

            in_row_steps(half, body, 32)

        total(top, 1, 2)
        total(low, 0, 3)
        for k in range(4):
            across(k).wait_send()
        for k in range(6):
            remote(nbuf.at[0], near_in.at[0], rs.at[k], rr.at[k], {"tp": right}).wait_send()

    pump(1)
    gather_begin(0, stream_ref)
    in_row_steps(tokens, clear, 32)
    pump(2)
    gather_end(0, 2)
    column(0)
    for layer in range(layers):
        unit = 2 * layer
        if layer:
            pump(upto=unit)
        else:
            pump(len(parts[0][0]) + 1 - done[0])
        sets = [(i, p) for i in (0, -1, 1, 2) for p in range(2)]
        for n, (i, p) in enumerate(sets):
            if not layer:
                pump(1)
            net.group(unit, p, i)
            project(layer, p, i)
        mix(layer)
        pump(upto=unit + 1)
        net.all(unit + 1)
        if layer + 1 < layers:
            reduce(layer, stream_ref, own, 2)
            gather_begin(layer + 1, own)
            in_row_steps(tokens, clear, 32)
            gather_end(layer + 1, 2)
            column(layer + 1)
        else:
            reduce(layer, own, out, 0)
    for unit in range(2 * layers):
        net.drain(unit)


def whole_call(stream, gain, wv, wg, wo, taps, gates, rate, n_sp, n_tp):
    tokens, feats = stream.shape
    layers, rows, width = wv.shape
    half = tokens // 2
    blocks = width // 128
    vmem = pl.BlockSpec(memory_space=pltpu.VMEM)
    hbm = pl.BlockSpec(memory_space=pl.ANY)
    f32 = pltpu.VMEM((tokens, width), F32)
    b16 = pltpu.VMEM((tokens, width), BF16)
    dma = pltpu.SemaphoreType.DMA
    return pl.pallas_call(
        functools.partial(whole_kernel, layers, n_sp, n_tp, float(gain.shape[1])),
        out_shape=jax.ShapeDtypeStruct((tokens, feats), BF16),
        in_specs=[vmem, vmem, hbm, hbm, hbm, vmem, vmem, vmem],
        out_specs=vmem,
        scratch_shapes=[
            pltpu.VMEM((layers, 2, n_sp, rows, width), BF16),
            pltpu.VMEM((layers, n_sp, rows, width), BF16),
            pltpu.VMEM((n_tp, tokens, feats), BF16),
            pltpu.VMEM((layers, n_tp, 8, tokens), F32),
            b16,
            pltpu.VMEM((2, tokens, width), F32),
            b16,
            pltpu.VMEM((tokens + 24, width), F32),
            f32, f32, b16,
            pltpu.VMEM((4, tokens, 512), F32),
            f32, f32, f32, f32,
            pltpu.VMEM((tokens, 128), F32),
            pltpu.VMEM((layers, 16, width), BF16),
            pltpu.VMEM((layers, 16, width), BF16),
            pltpu.VMEM((4, SEG, width), F32),
            pltpu.VMEM((2, SEG, width), F32),
            pltpu.VMEM((layers, 2, 8, 128), F32),
            pltpu.VMEM((layers, n_sp, 8, 128), F32),
            pltpu.VMEM((4, tokens, feats), BF16),
            pltpu.VMEM((4, tokens, feats), BF16),
            pltpu.VMEM((tokens, feats), BF16),
            pltpu.VMEM((2, half, feats), BF16),
            pltpu.VMEM((4, half, feats), BF16),
            pltpu.VMEM((4, half, feats), BF16),
            dma((3 * layers,)),
            dma((4 * layers,)),
            dma((4 * layers, 16)),
            dma((13,)),
            dma((13,)),
            dma((layers, n_tp)),
            dma((layers, n_tp)),
            dma((layers, 2)),
            dma((layers, 2)),
            dma((layers, n_sp)),
            dma((layers, n_sp)),
            dma((4,)),
            dma((4,)),
            dma((6,)),
            dma((6,)),
        ],
        compiler_params=pltpu.CompilerParams(
            collective_id=0, has_side_effects=True, vmem_limit_bytes=63_000_000
        ),
        cost_estimate=pl.CostEstimate(flops=20_000_000_000, bytes_accessed=8_000_000, transcendentals=0),
        name="both_layers",
    )(stream, gain, wv, wg, wo, taps, gates, rate)


def per_device(
    n_sp, n_tp, stream_in, norm_gain, value_proj, gate_proj, out_proj, conv_taps, block_gates, forget_rate
):
    tokens, feats = stream_in.shape
    width = value_proj.shape[2]
    layers = value_proj.shape[0]
    steps = tokens // SEG
    gates = block_gates.reshape(layers, 4, width // 128, 128, 128)
    stream = stream_in.reshape(SEG, steps, feats).transpose(1, 0, 2).reshape(tokens, feats)
    stream = whole_call(
        stream, norm_gain, value_proj, gate_proj, out_proj, conv_taps, gates, forget_rate, n_sp, n_tp
    )
    return stream.reshape(steps, SEG, feats).transpose(1, 0, 2).reshape(tokens, feats)


def solution(mesh):
    placed = (
        P("sp", "tp"),
        P(),
        P(None, "sp", "tp"),
        P(None, "sp", "tp"),
        P(None, "sp", "tp"),
        P(),
        P(None, None, None, "tp", None),
        P(),
    )
    body = functools.partial(per_device, mesh.shape["sp"], mesh.shape["tp"])
    return jax.shard_map(body, mesh=mesh, in_specs=placed, out_specs=P("sp", "tp"), check_vma=False)
```

```python
import functools

import jax
import jax.numpy as jnp
from jax import lax
from jax.experimental import pallas as pl
from jax.experimental.pallas import tpu as pltpu
from jax.sharding import PartitionSpec as P

GATE_SCALE = 8.0
NORM_EPS = 1e-06
MESH = pl.DeviceIdType.MESH
F32 = jnp.float32
BF16 = jnp.bfloat16
SEG = 8
ROWS = 64


def remote(src, dst, send_sem, recv_sem, dev):
    return pltpu.make_async_remote_copy(
        src_ref=src, dst_ref=dst, send_sem=send_sem, recv_sem=recv_sem, device_id=dev, device_id_type=MESH
    )


def greet(groups):
    barrier = pltpu.get_barrier_semaphore()
    for axis, count, me in groups:
        for step in range(1, count):
            pl.semaphore_signal(barrier, inc=1, device_id={axis: lax.rem(me + step, count)}, device_id_type=MESH)
    pl.semaphore_wait(barrier, sum(count - 1 for _, count, _ in groups))


def sigmoid(v):
    return 1.0 / (1.0 + jnp.exp(-v))


def drive_square(y):
    terms = [1.0, -1.0 / 2, 1.0 / 6, -1.0 / 24, 1.0 / 120, -1.0 / 720, 1.0 / 5040, -1.0 / 40320, 1.0 / 362880]
    total = jnp.full_like(y, terms[-1])
    for term in terms[-2::-1]:
        total = total * y + term
    return total * y


def in_row_steps(rows, body, size=ROWS):
    def step(k, carry):
        body(pl.ds(pl.multiple_of(k * size, size), size))
        return carry

    lax.fori_loop(0, rows // size, step, 0)


class Ring:
    def __init__(self, me, count):
        chips = count // 2
        self.chips = chips
        self.me = me
        self.x = me // 2
        self.c = lax.rem(me, 2)
        self.sib = self.x * 2 + 1 - self.c

    def at(self, step, other=False):
        core = 1 - self.c if other else self.c
        return lax.rem(self.x + step + self.chips, self.chips) * 2 + core


def gather_fill(own_ref, gain, xg, ssg, me):
    tokens = own_ref.shape[0]

    def fill(rows):
        v = own_ref[rows, :].astype(F32)
        xg[me, rows, :] = (v * gain).astype(BF16)

    in_row_steps(tokens, fill)
    for k in range(tokens // 128):
        v = own_ref[pl.ds(k * 128, 128), :].astype(F32)
        total = jnp.sum(v * v, axis=1, keepdims=True)
        ssg[me, :, pl.ds(k * 128, 128)] = jnp.broadcast_to(total, (128, 128)).T[0:8, :]


def gather_start(ring, xg, ssg, send, recv, ssend, srecv, count):
    me = ring.me
    half = xg.shape[1] // 2
    a, b = pl.ds(0, half), pl.ds(half, half)
    right, left = ring.at(1), ring.at(-1)
    for k, (rows, dev) in enumerate(((a, right), (b, right), (b, left), (a, left))):
        part = xg.at[me, rows]
        remote(part, part, send.at[k], recv.at[k], {"tp": dev}).start()
    remote(xg.at[me], xg.at[me], send.at[6], recv.at[6], {"tp": ring.sib}).start()
    for step in range(1, count):
        dev = lax.rem(me + step, count)
        remote(ssg.at[me], ssg.at[me], ssend.at[dev], srecv.at[me], {"tp": dev}).start()


def gather_finish(ring, xg, ssg, send, recv, ssend, srecv, count, pump):
    me = ring.me
    half = xg.shape[1] // 2
    a, b = pl.ds(0, half), pl.ds(half, half)
    right, left, far = ring.at(1), ring.at(-1), ring.at(2)

    def got(owner, rows, k):
        part = xg.at[owner, rows]
        remote(part, part, send.at[k], recv.at[k], {"tp": ring.sib}).wait_recv()
        return part

    def push(part, k, dev):
        remote(part, part, send.at[k], recv.at[k], {"tp": dev}).start()

    part = got(left, a, 0)
    push(part, 4, right)
    push(part, 7, ring.sib)
    part = got(right, b, 2)
    push(part, 5, left)
    push(part, 8, ring.sib)
    pump()
    push(got(left, b, 1), 9, ring.sib)
    push(got(right, a, 3), 10, ring.sib)
    pump()
    push(got(far, a, 4), 11, ring.sib)
    push(got(far, b, 5), 12, ring.sib)
    pump()
    whole = xg.at[ring.sib]
    remote(whole, whole, send.at[6], recv.at[6], {"tp": ring.sib}).wait()
    owners = {7: (-1, a), 8: (1, b), 9: (-1, b), 10: (1, a), 11: (2, a), 12: (2, b)}
    for k, (step, rows) in owners.items():
        part = xg.at[ring.at(step, other=True), rows]
        remote(part, part, send.at[k], recv.at[k], {"tp": ring.sib}).wait()
    for k in range(6):
        part = xg.at[me, a]
        remote(part, part, send.at[k], recv.at[k], {"tp": right}).wait_send()
    for step in range(1, count):
        dev = lax.rem(me + step, count)
        remote(ssg.at[dev], ssg.at[dev], ssend.at[dev], srecv.at[dev], {"tp": dev}).wait()


class Weights:
    def __init__(self, me, side, wvg, wo, gsend, grecv):
        self.y, self.z, self.side = lax.rem(me, side), me // side, side
        self.wvg, self.wo, self.gsend, self.grecv = wvg, wo, gsend, grecv
        self.waited = set()

    def idx(self, p, i, j):
        dy, dz = (i, j) if p == 0 else (j, i)
        return lax.rem(self.z + dz + self.side, self.side) * self.side + lax.rem(self.y + dy + self.side, self.side)

    def ref(self, unit, p, at):
        if unit % 2 == 0:
            return self.wvg.at[unit // 2, p, at]
        half = self.wo.shape[2] // 2
        return self.wo.at[unit // 2, at, pl.ds(p * half, half)]

    def push(self, unit, p, i, j, axis, d):
        ref = self.ref(unit, p, self.idx(p, i, j))
        di, dj = (d, 0) if axis == 0 else (0, d)
        slot = ((i - di) % 4) * 4 + (j - dj) % 4
        remote(
            ref, ref, self.gsend.at[2 * unit + p], self.grecv.at[2 * unit + p, slot], {"sp": self.idx(p, di, dj)}
        ).start()

    def arrive(self, unit, p, i, j):
        key = (unit, p, i % 4, j % 4)
        if key in self.waited or (i % 4, j % 4) == (0, 0):
            return
        self.waited.add(key)
        ref = self.ref(unit, p, self.idx(p, i, j))
        slot = (i % 4) * 4 + j % 4
        remote(
            ref, ref, self.gsend.at[2 * unit + p], self.grecv.at[2 * unit + p, slot], {"sp": self.idx(p, 1, 0)}
        ).wait_recv()

    def group(self, unit, p, i):
        for j in (0, -1, 1, 2):
            self.arrive(unit, p, i, j)

    def all(self, unit):
        for p in range(2):
            for i in (0, -1, 1, 2):
                self.group(unit, p, i)

    def opening(self, unit):
        for axis in range(2):
            for p in range(2):
                for d in (1, -1):
                    self.push(unit, p, 0, 0, axis, d)

    def events(self, unit):
        first = 1 if unit in (0, 3) else -1

        def turn(p, i, forward=None):
            def run():
                self.arrive(unit, p, i, 0)
                if forward:
                    self.push(unit, p, i, 0, 0, forward)
                for d in (1, -1):
                    self.push(unit, p, i, 0, 1, d)

            return run

        def relay(p, i):
            d = 1 if (i + unit) % 2 == 0 else -1

            def run():
                self.arrive(unit, p, i, -d)
                self.push(unit, p, i, -d, 1, d)

            return run

        both = range(2)
        steps = [turn(p, -first, first) for p in both] + [turn(p, first) for p in both]
        steps += [relay(p, 0) for p in both] + [turn(p, 2) for p in both]
        return steps + [relay(p, i) for i in (-1, 1, 2) for p in both]

    def drain(self, unit):
        for p in range(2):
            if unit % 2 == 0:
                ref = self.wvg.at[unit // 2, p, pl.ds(0, 15)]
            else:
                half = self.wo.shape[2] // 2
                ref = self.wo.at[unit // 2, pl.ds(0, 15), pl.ds(p * half, half)]
            remote(ref, ref, self.gsend.at[2 * unit + p], self.grecv.at[2 * unit + p, 0], {"sp": self.idx(p, 1, 0)}).wait_send()


def whole_kernel(
    layers, n_sp, n_tp, features,
    stream_ref, gain_ref, wv_hbm, wg_hbm, wo_hbm, taps_ref, gates_ref, rate_ref, out,
    wvg, wo, xg, ssg, base, own, perm, acc, mixb, mpad, sil, conv, convb, big, a_f, u_f, a_b, u_b, col,
    halo_p, halo_n, seg, ent, msg, slots,
    psend, precv, fbuf, far_in, nbuf, near_in,
    ld, gsend, grecv, asend, arecv, ssend, srecv, hsend, hrecv, csend, crecv, ds, dr, rs, rr,
):
    sp, tp = lax.axis_index("sp"), lax.axis_index("tp")
    tokens, width = mixb.shape
    feats = own.shape[1]
    ring = Ring(tp, n_tp)
    net = Weights(sp, 4, wvg, wo, gsend, grecv)
    pre = pown = big
    lanes_own = pl.ds(pl.multiple_of(tp * width, width), width)
    right, left = ring.at(1), ring.at(-1)

    loads = []
    for layer in range(layers):
        loads.append([
            pltpu.make_async_copy(wv_hbm.at[layer], wvg.at[layer, 0, sp], ld.at[3 * layer]),
            pltpu.make_async_copy(wg_hbm.at[layer], wvg.at[layer, 1, sp], ld.at[3 * layer + 1]),
        ])
        loads.append([pltpu.make_async_copy(wo_hbm.at[layer], wo.at[layer, sp], ld.at[3 * layer + 2])])
    for copies in loads:
        for copy in copies:
            copy.start()
    queue = []

    def opening(unit):
        def run():
            for copy in loads[unit]:
                copy.wait()
            net.opening(unit)

        return run

    for unit in range(2 * layers):
        queue.append(opening(unit))
        queue.extend(net.events(unit))
    done = [0]

    def pump(n):
        stop = min(done[0] + n, len(queue))
        while done[0] < stop:
            queue[done[0]]()
            done[0] += 1

    def project(layer, p, i):
        def step(j, carry):
            at = net.idx(p, i, j)
            lanes = pl.ds(pl.multiple_of(lax.rem(at, 2) * 256, 256), 256)
            acc[p] += jnp.dot(xg[at // 2, :, lanes], wvg[layer, p, at], preferred_element_type=F32)
            return carry

        def pair(j, carry):
            block = lax.rem(net.z + i + net.side, net.side) * 2 + j
            both = wvg[layer, p, pl.ds(2 * block, 2)].reshape(feats, width)
            acc[p] += jnp.dot(xg[block], both, preferred_element_type=F32)
            return carry

        if p == 0:
            lax.fori_loop(0, 4, step, 0)
        else:
            lax.fori_loop(0, 2, pair, 0)

    def project_all(layer):
        def step(block, carry):
            for p in range(2):
                both = wvg[layer, p, pl.ds(2 * block, 2)].reshape(feats, width)
                acc[p] += jnp.dot(xg[block], both, preferred_element_type=F32)
            return carry

        lax.fori_loop(0, n_tp, step, 0)

    def gather_own(layer, source):
        gain = gain_ref[layer : layer + 1, lanes_own]
        gather_fill(source, gain, xg, ssg.at[layer], tp)

    def gather_begin(layer):
        gather_start(ring, xg, ssg.at[layer], asend, arecv, ssend.at[layer], srecv.at[layer], n_tp)

    def gather_end(layer, counts):
        pumps = iter(counts)
        gather_finish(
            ring, xg, ssg.at[layer], asend, arecv, ssend.at[layer], srecv.at[layer], n_tp, lambda: pump(next(pumps))
        )

    def column(layer):
        total = jnp.sum(ssg[layer], axis=0)
        scale = lax.rsqrt(total / features + NORM_EPS)
        for k in range(tokens // 128):
            part = jnp.broadcast_to(scale[0:1, k * 128 : (k + 1) * 128], (128, 128))
            col[pl.ds(k * 128, 128), :] = part.T

    def clear(rows):
        zero = jnp.zeros((rows.size, width), F32)
        acc[0, rows, :] = zero
        acc[1, rows, :] = zero

    def mix(layer):
        def finish_v(rows):
            wide = jnp.concatenate([col[rows, :]] * (width // 128), axis=1)
            value = (acc[0, rows, :] * wide).astype(BF16)
            mixb[rows, :] = value
            acc[0, rows, :] = value.astype(F32)

        in_row_steps(tokens, finish_v, 32)
        head, tail = mixb.at[pl.ds(0, 16)], mixb.at[pl.ds(tokens - 16, 16)]
        hs, hr = hsend.at[layer], hrecv.at[layer]
        to_next = remote(tail, halo_p.at[layer], hs.at[0], hr.at[0], {"sp": lax.rem(sp + 1, n_sp)})
        to_prev = remote(head, halo_n.at[layer], hs.at[1], hr.at[1], {"sp": lax.rem(sp + n_sp - 1, n_sp)})
        to_next.start()
        to_prev.start()

        def finish_g(rows):
            wide = jnp.concatenate([col[rows, :]] * (width // 128), axis=1)
            gate = (acc[1, rows, :] * wide).astype(BF16).astype(F32)
            sil[rows, :] = gate * sigmoid(gate)
            mpad[pl.ds(pl.multiple_of(rows.start + 16, 16), rows.size), :] = acc[0, rows, :]

        in_row_steps(tokens, finish_g, 32)
        pump(2)
        to_next.wait()
        to_prev.wait()
        sub = lax.broadcasted_iota(jnp.int32, (SEG, width), 0)
        before = halo_p[layer].astype(F32)
        after = halo_n[layer].astype(F32)
        for k in range(2):
            edge = jnp.where(sp > 0, before[8 * k + 7 : 8 * k + 8, :], 0.0)
            blk = acc[0, pl.ds(tokens - 16 + 8 * k, 8), :]
            mpad[pl.ds(8 * k, 8), :] = jnp.where(
                sub == 0, jnp.broadcast_to(edge, (SEG, width)), pltpu.roll(blk, 1, 0)
            )
        edge = jnp.where(sp < n_sp - 1, after[0:1, :], 0.0)
        blk = acc[0, pl.ds(0, 8), :]
        mpad[pl.ds(tokens + 16, 8), :] = jnp.where(
            sub == SEG - 1, jnp.broadcast_to(edge, (SEG, width)), pltpu.roll(blk, SEG - 1, 0)
        )
        taps = taps_ref[layer, :, lanes_own]

        def convolve(rows):
            terms = [
                mpad[pl.ds(pl.multiple_of(rows.start + 8 * k, 8), rows.size), :] * taps[k : k + 1, :]
                for k in range(4)
            ]
            value = (terms[0] + terms[1]) + (terms[2] + terms[3])
            conv[rows, :] = value
            convb[rows, :] = value.astype(BF16)

        in_row_steps(tokens, convolve, 32)
        for b in range(width // 128):
            maps = jnp.concatenate([gates_ref[layer, g, b] for g in range(4)], axis=1)
            pre[b] = jnp.dot(convb[:, b * 128 : (b + 1) * 128], maps, preferred_element_type=F32)
        pump(2)
        rate_all = -GATE_SCALE * rate_ref[layer, :, lanes_own]
        for b in range(width // 128):
            lanes = pl.ds(b * 128, 128)
            rates = [rate_all[e : e + 1, b * 128 : (b + 1) * 128] for e in range(2)]

            def body(k, carry, b=b, lanes=lanes, rates=rates):
                p_f, h_f, p_b, h_b = carry
                rows = pl.ds(pl.multiple_of(k * ROWS, ROWS), ROWS)
                cv = conv[rows, lanes]
                kept = []
                for e, (a_ref, u_ref) in enumerate(((a_f, u_f), (a_b, u_b))):
                    r = sigmoid(pre[b, rows, 256 * e : 256 * e + 128])
                    i = sigmoid(pre[b, rows, 256 * e + 128 : 256 * e + 256])
                    log_a = rates[e] * r
                    decay = jnp.exp(log_a)
                    drive = jnp.sqrt(drive_square(-2.0 * log_a)) * i * cv
                    a_ref[rows, lanes] = decay
                    u_ref[rows, lanes] = drive
                    kept.append((decay, drive))
                for j in range(ROWS // 8):
                    at = slice(8 * j, 8 * j + 8)
                    d, u = kept[0][0][at], kept[0][1][at]
                    h_f = d * h_f + u
                    p_f = p_f * d
                    d, u = kept[1][0][at], kept[1][1][at]
                    h_b = h_b + p_b * u
                    p_b = p_b * d
                return p_f, h_f, p_b, h_b

            one, zero = jnp.ones((SEG, 128), F32), jnp.zeros((SEG, 128), F32)
            ends = lax.fori_loop(0, tokens // ROWS, body, (one, zero, one, zero))
            for k in range(4):
                seg[k, :, lanes] = ends[k]
            if b in (0, 3):
                pump(2)

        sides = ((0, range(SEG)), (2, range(SEG - 1, -1, -1)))
        for e, (k, order) in enumerate(sides):
            prod = jnp.ones((1, width), F32)
            state = jnp.zeros((1, width), F32)
            for s in order:
                d = seg[k, s : s + 1, :]
                state = d * state + seg[k + 1, s : s + 1, :]
                prod = prod * d
            for b in range(width // 128):
                msg[layer, e, b : b + 1, :] = prod[:, b * 128 : (b + 1) * 128]
                msg[layer, e, 4 + b : 5 + b, :] = state[:, b * 128 : (b + 1) * 128]
        cs, cr = csend.at[layer], crecv.at[layer]
        for step in range(1, n_sp):
            dev = lax.rem(sp + step, n_sp)
            side = jnp.where(dev > sp, 0, 1)
            remote(msg.at[layer, side], slots.at[layer, sp], cs.at[dev], cr.at[sp], {"sp": dev}).start()
        slots[layer, sp] = jnp.zeros((8, 128), F32)
        pump(4)
        for step in range(1, n_sp):
            dev = lax.rem(sp + step, n_sp)
            remote(msg.at[layer, 0], slots.at[layer, dev], cs.at[dev], cr.at[dev], {"sp": dev}).wait()
        for e, (k, order) in enumerate(sides):
            carry = jnp.zeros((4, 128), F32)
            for q in range(n_sp) if e == 0 else range(n_sp - 1, -1, -1):
                live = (q < sp) if e == 0 else (q > sp)
                slot = slots[layer, q]
                carry = jnp.where(live, slot[0:4] * carry + slot[4:8], carry)
            state = jnp.concatenate([carry[b : b + 1, :] for b in range(width // 128)], axis=1)
            for s in order:
                ent[e, s : s + 1, :] = state
                state = seg[k, s : s + 1, :] * state + seg[k + 1, s : s + 1, :]
        def again(k, carry):
            h_f, h_b = carry
            for j in range(4):
                fwd = pl.ds(pl.multiple_of((4 * k + j) * SEG, SEG), SEG)
                bwd = pl.ds(pl.multiple_of((steps - 1 - 4 * k - j) * SEG, SEG), SEG)
                h_f = a_f[fwd, :] * h_f + u_f[fwd, :]
                u_f[fwd, :] = h_f
                h_b = a_b[bwd, :] * h_b + u_b[bwd, :]
                u_b[bwd, :] = h_b
            return h_f, h_b

        lax.fori_loop(0, steps // 4, again, (ent[0], ent[1]))

        def gated(rows):
            mixb[rows, :] = ((u_f[rows, :] + u_b[rows, :]) * sil[rows, :]).astype(BF16)

        in_row_steps(tokens, gated, 32)

    half = tokens // 2
    top, low = pl.ds(0, half), pl.ds(half, half)

    def reduce(layer, source, target, counts):
        order = (2, 1, -1, 0)

        def product(k, other):
            block = ring.at(order[k], other=other)
            terms = [
                lax.dot_general(
                    mixb[...], wo[layer, 2 * block + part], (((1,), (1,)), ((), ())), preferred_element_type=F32
                )
                for part in range(2)
            ]
            return terms

        def across(k):
            return remote(psend.at[k], precv.at[k], ds.at[k], dr.at[k], {"tp": ring.sib})

        def send(k, src, dst, dev):
            remote(src, dst, rs.at[k], rr.at[k], {"tp": dev}).start()

        def paired(k, rows, into=None):
            def body(r):
                at = pl.ds(pl.multiple_of(rows.start + r.start, 32), r.size)
                value = pown[k, at, :] + precv[k, at, :].astype(F32)
                if into is None:
                    pown[k, at, :] = value
                else:
                    into[at if into.shape[0] == tokens else r, :] = value.astype(BF16)

            in_row_steps(rows.size, body, 32)

        for k in range(4):
            for part, term in enumerate(product(k, True)):
                psend[k, :, part * 256 : (part + 1) * 256] = term.astype(BF16)
            across(k).start()
            for part, term in enumerate(product(k, False)):
                pown[k, :, part * 256 : (part + 1) * 256] = term
            if k == 1:
                across(0).wait_recv()
                paired(0, top, fbuf)
                send(0, fbuf.at[top], far_in.at[0], right)
                paired(0, low, fbuf)
                send(1, fbuf.at[low], far_in.at[1], left)
            if k == 2:
                across(1).wait_recv()
                paired(1, low, nbuf.at[0])
                send(2, nbuf.at[0], near_in.at[0], right)
                paired(1, top)
            if k == 3:
                across(2).wait_recv()
                paired(2, top, nbuf.at[1])
                send(3, nbuf.at[1], near_in.at[1], left)
                paired(2, low)
        across(3).wait_recv()
        paired(3, pl.ds(0, tokens))
        pump(counts[0])

        def arrived(k, src, dst):
            remote(src, dst, rs.at[k], rr.at[k], {"tp": right}).wait_recv()

        def merged(k, rows, src, into):
            def body(r):
                at = pl.ds(pl.multiple_of(rows.start + r.start, 32), r.size)
                into[r, :] = (pown[k, at, :] + src[r, :].astype(F32)).astype(BF16)

            in_row_steps(half, body, 32)

        arrived(0, fbuf.at[top], far_in.at[0])
        merged(1, top, far_in.at[0], nbuf.at[2])
        send(4, nbuf.at[2], near_in.at[2], right)
        arrived(1, fbuf.at[low], far_in.at[1])
        merged(2, low, far_in.at[1], nbuf.at[3])
        send(5, nbuf.at[3], near_in.at[3], left)
        pump(counts[1])
        for k in range(4):
            arrived(2 + k, nbuf.at[k], near_in.at[k])
            if k == 1:
                pump(counts[2])

        def total(rows, one, two):
            def body(r):
                at = pl.ds(pl.multiple_of(rows.start + r.start, 32), r.size)
                branch = pown[3, at, :] + near_in[one, r, :].astype(F32) + near_in[two, r, :].astype(F32)
                value = source[at, :].astype(F32) + branch
                if target is None:
                    for j in range(r.size // SEG):
                        for b in range(feats // 128):
                            perm[b, pl.ds(at.start // SEG + j, SEG, stride=steps), :] = value[
                                j * SEG : (j + 1) * SEG, b * 128 : (b + 1) * 128
                            ]
                else:
                    target[at, :] = value.astype(BF16)

            in_row_steps(half, body, 32)

        total(top, 1, 2)
        total(low, 0, 3)
        for k in range(4):
            across(k).wait_send()
        for k in range(6):
            remote(nbuf.at[0], near_in.at[0], rs.at[k], rr.at[k], {"tp": right}).wait_send()

    steps = tokens // SEG

    def spread(rows):
        for b in range(feats // 128):
            perm[b, rows, :] = stream_ref[rows, b * 128 : (b + 1) * 128].astype(F32)

    def collect(rows):
        first = rows.start // SEG
        for b in range(feats // 128):
            parts = [perm[b, pl.ds(first + j, SEG, stride=steps), :] for j in range(rows.size // SEG)]
            base[rows, b * 128 : (b + 1) * 128] = jnp.concatenate(parts, axis=0).astype(BF16)

    def finish(rows):
        for b in range(feats // 128):
            out[rows, b * 128 : (b + 1) * 128] = perm[b, rows, :].astype(BF16)

    in_row_steps(tokens, spread)
    in_row_steps(tokens, collect, 32)
    gather_own(0, base)
    greet((("sp", n_sp, sp), ("tp", n_tp, tp)))

    pump(1)
    gather_begin(0)
    in_row_steps(tokens, clear, 32)
    gather_end(0, (4, 2, 2))
    column(0)
    for layer in range(layers):
        unit = 2 * layer
        if layer:
            net.all(unit)
            project_all(layer)
        else:
            pump(4)
            for i in (0, -1, 1, 2):
                for p in range(2):
                    net.group(unit, p, i)
                    project(layer, p, i)
                if i == 0:
                    pump(3)
        mix(layer)
        pump(3)
        net.all(unit + 1)
        if layer + 1 < layers:
            reduce(layer, base, own, (0, 4, 2))
            gather_own(layer + 1, own)
            gather_begin(layer + 1)
            pump(2)
            in_row_steps(tokens, clear, 32)
            gather_end(layer + 1, (2, 2, 3))
            column(layer + 1)
        else:
            reduce(layer, own, None, (0, 0, 0))
            in_row_steps(tokens, finish)
    for unit in range(2 * layers):
        net.drain(unit)


def whole_call(stream, gain, wv, wg, wo, taps, gates, rate, n_sp, n_tp):
    tokens, feats = stream.shape
    layers, rows, width = wv.shape
    half = tokens // 2
    blocks = width // 128
    vmem = pl.BlockSpec(memory_space=pltpu.VMEM)
    hbm = pl.BlockSpec(memory_space=pl.ANY)
    f32 = pltpu.VMEM((tokens, width), F32)
    b16 = pltpu.VMEM((tokens, width), BF16)
    dma = pltpu.SemaphoreType.DMA
    return pl.pallas_call(
        functools.partial(whole_kernel, layers, n_sp, n_tp, float(gain.shape[1])),
        out_shape=jax.ShapeDtypeStruct((tokens, feats), BF16),
        in_specs=[vmem, vmem, hbm, hbm, hbm, vmem, vmem, vmem],
        out_specs=vmem,
        scratch_shapes=[
            pltpu.VMEM((layers, 2, n_sp, rows, width), BF16),
            pltpu.VMEM((layers, n_sp, rows, width), BF16),
            pltpu.VMEM((n_tp, tokens, feats), BF16),
            pltpu.VMEM((layers, n_tp, 8, tokens), F32),
            b16, b16,
            pltpu.VMEM((feats // 128, tokens, 128), F32),
            pltpu.VMEM((2, tokens, width), F32),
            b16,
            pltpu.VMEM((tokens + 24, width), F32),
            f32, f32, b16,
            pltpu.VMEM((4, tokens, 512), F32),
            f32, f32, f32, f32,
            pltpu.VMEM((tokens, 128), F32),
            pltpu.VMEM((layers, 16, width), BF16),
            pltpu.VMEM((layers, 16, width), BF16),
            pltpu.VMEM((4, SEG, width), F32),
            pltpu.VMEM((2, SEG, width), F32),
            pltpu.VMEM((layers, 2, 8, 128), F32),
            pltpu.VMEM((layers, n_sp, 8, 128), F32),
            pltpu.VMEM((4, tokens, feats), BF16),
            pltpu.VMEM((4, tokens, feats), BF16),
            pltpu.VMEM((tokens, feats), BF16),
            pltpu.VMEM((2, half, feats), BF16),
            pltpu.VMEM((4, half, feats), BF16),
            pltpu.VMEM((4, half, feats), BF16),
            dma((3 * layers,)),
            dma((4 * layers,)),
            dma((4 * layers, 16)),
            dma((13,)),
            dma((13,)),
            dma((layers, n_tp)),
            dma((layers, n_tp)),
            dma((layers, 2)),
            dma((layers, 2)),
            dma((layers, n_sp)),
            dma((layers, n_sp)),
            dma((4,)),
            dma((4,)),
            dma((6,)),
            dma((6,)),
        ],
        compiler_params=pltpu.CompilerParams(
            collective_id=0, has_side_effects=True, vmem_limit_bytes=63_000_000
        ),
        cost_estimate=pl.CostEstimate(flops=20_000_000_000, bytes_accessed=8_000_000, transcendentals=0),
        name="both_layers",
    )(stream, gain, wv, wg, wo, taps, gates, rate)


def per_device(
    n_sp, n_tp, stream_in, norm_gain, value_proj, gate_proj, out_proj, conv_taps, block_gates, forget_rate
):
    width = value_proj.shape[2]
    layers = value_proj.shape[0]
    gates = block_gates.reshape(layers, 4, width // 128, 128, 128)
    return whole_call(
        stream_in, norm_gain, value_proj, gate_proj, out_proj, conv_taps, gates, forget_rate, n_sp, n_tp
    )


def solution(mesh):
    placed = (
        P("sp", "tp"),
        P(),
        P(None, "sp", "tp"),
        P(None, "sp", "tp"),
        P(None, "sp", "tp"),
        P(),
        P(None, None, None, "tp", None),
        P(),
    )
    body = functools.partial(per_device, mesh.shape["sp"], mesh.shape["tp"])
    return jax.shard_map(body, mesh=mesh, in_specs=placed, out_specs=P("sp", "tp"), check_vma=False)
```

```python
import functools

import jax
import jax.numpy as jnp
from jax import lax
from jax.experimental import pallas as pl
from jax.experimental.pallas import tpu as pltpu
from jax.sharding import PartitionSpec as P

GATE_SCALE = 8.0
NORM_EPS = 1e-06
MESH = pl.DeviceIdType.MESH
F32 = jnp.float32
BF16 = jnp.bfloat16
SEG = 8
ROWS = 64
PLAN = ('000', '00', '0', '000', '01', '000', '', '', '', '01', '01', '', '11111', '', '11111', '', '', '', '1', '', '1', '2', '', '3', '2', '', '2', '2', '2', '', '2', '2', '2', '2', '2', '2', '223', '2', '', '', '2', '3', '', '333', '', '', '', '', '33', '3', '3', '', '33', '', '3', '33', '', '', '', '', '', '', '', '')


def remote(src, dst, send_sem, recv_sem, dev):
    return pltpu.make_async_remote_copy(
        src_ref=src, dst_ref=dst, send_sem=send_sem, recv_sem=recv_sem, device_id=dev, device_id_type=MESH
    )


def greet(groups):
    barrier = pltpu.get_barrier_semaphore()
    for axis, count, me in groups:
        for step in range(1, count):
            pl.semaphore_signal(barrier, inc=1, device_id={axis: lax.rem(me + step, count)}, device_id_type=MESH)
    return lambda: pl.semaphore_wait(barrier, sum(count - 1 for _, count, _ in groups))


def sigmoid(v):
    return 1.0 / (1.0 + jnp.exp(-v))


def drive_square(y):
    terms = [1.0, -1.0 / 2, 1.0 / 6, -1.0 / 24, 1.0 / 120, -1.0 / 720, 1.0 / 5040, -1.0 / 40320, 1.0 / 362880]
    total = jnp.full_like(y, terms[-1])
    for term in terms[-2::-1]:
        total = total * y + term
    return total * y


def in_row_steps(rows, body, size=ROWS, first=0):
    def step(k, carry):
        body(pl.ds(pl.multiple_of(first + k * size, size), size))
        return carry

    lax.fori_loop(0, rows // size, step, 0)


def aligned(at, size):
    return at if isinstance(at, int) else pl.multiple_of(at, size)


class Ring:
    def __init__(self, me, count):
        chips = count // 2
        self.chips = chips
        self.me = me
        self.x = me // 2
        self.c = lax.rem(me, 2)
        self.sib = self.x * 2 + 1 - self.c

    def at(self, step, other=False):
        core = 1 - self.c if other else self.c
        return lax.rem(self.x + step + self.chips, self.chips) * 2 + core


def gather_fill(own_ref, gain, xg, ssg, me, half=None):
    tokens = own_ref.shape[0]
    first, count = (0, tokens) if half is None else (half * tokens // 2, tokens // 2)

    def fill(rows):
        at = pl.ds(pl.multiple_of(first + rows.start, ROWS), rows.size)
        v = own_ref[at, :].astype(F32)
        xg[me, at, :] = (v * gain).astype(BF16)

    in_row_steps(count, fill)
    for k in range(first // 128, (first + count) // 128):
        v = own_ref[pl.ds(k * 128, 128), :].astype(F32)
        total = jnp.sum(v * v, axis=1, keepdims=True)
        ssg[me, :, pl.ds(k * 128, 128)] = jnp.broadcast_to(total, (128, 128)).T[0:8, :]


class Gather:
    def __init__(self, ring, xg, ssg, send, recv, ssend, srecv, count):
        self.ring, self.xg, self.ssg, self.count = ring, xg, ssg, count
        self.send, self.recv, self.ssend, self.srecv = send, recv, ssend, srecv
        half = xg.shape[1] // 2
        self.rows = (pl.ds(0, half), pl.ds(half, half))

    def push(self, part, k, dev):
        remote(part, part, self.send.at[k], self.recv.at[k], {"tp": dev}).start()

    def begin(self, half):
        ring = self.ring
        part = self.xg.at[ring.me, self.rows[half]]
        right, left = ring.at(1), ring.at(-1)
        if half == 0:
            self.push(part, 0, right)
            self.push(part, 3, left)
            self.push(part, 6, ring.sib)
        else:
            self.push(part, 2, left)
            self.push(part, 1, right)
            self.push(part, 13, ring.sib)

    def begin_squares(self):
        ring, ssg = self.ring, self.ssg
        for step in range(1, self.count):
            dev = lax.rem(ring.me + step, self.count)
            remote(ssg.at[ring.me], ssg.at[ring.me], self.ssend.at[dev], self.srecv.at[ring.me], {"tp": dev}).start()

    def got(self, k):
        ring = self.ring
        step, half = {0: (-1, 0), 1: (-1, 1), 2: (1, 1), 3: (1, 0), 4: (2, 0), 5: (2, 1)}[k]
        part = self.xg.at[ring.at(step), self.rows[half]]
        remote(part, part, self.send.at[k], self.recv.at[k], {"tp": ring.sib}).wait_recv()
        if k == 0:
            self.push(part, 4, ring.at(1))
        if k == 2:
            self.push(part, 5, ring.at(-1))
        self.push(part, 7 + k, ring.sib)

    def end(self):
        ring = self.ring
        owners = {6: (0, 0), 13: (0, 1), 7: (-1, 0), 8: (-1, 1), 9: (1, 1), 10: (1, 0), 11: (2, 0), 12: (2, 1)}
        for k, (step, half) in owners.items():
            part = self.xg.at[ring.at(step, other=True), self.rows[half]]
            remote(part, part, self.send.at[k], self.recv.at[k], {"tp": ring.sib}).wait()
        for k in range(6):
            part = self.xg.at[ring.me, self.rows[0]]
            remote(part, part, self.send.at[k], self.recv.at[k], {"tp": ring.at(1)}).wait_send()
        for step in range(1, self.count):
            dev = lax.rem(ring.me + step, self.count)
            remote(self.ssg.at[dev], self.ssg.at[dev], self.ssend.at[dev], self.srecv.at[dev], {"tp": dev}).wait()


class Weights:
    def __init__(self, me, side, wvg, wo, gsend, grecv):
        self.y, self.z, self.side = lax.rem(me, side), me // side, side
        self.wvg, self.wo, self.gsend, self.grecv = wvg, wo, gsend, grecv
        self.waited = set()

    def idx(self, p, i, j):
        dy, dz = (i, j) if p == 0 else (j, i)
        return lax.rem(self.z + dz + self.side, self.side) * self.side + lax.rem(self.y + dy + self.side, self.side)

    def ref(self, unit, p, at):
        if unit % 2 == 0:
            return self.wvg.at[unit // 2, p, at]
        half = self.wo.shape[2] // 2
        return self.wo.at[unit // 2, at, pl.ds(p * half, half)]

    def push(self, unit, p, i, j, axis, d):
        ref = self.ref(unit, p, self.idx(p, i, j))
        di, dj = (d, 0) if axis == 0 else (0, d)
        slot = ((i - di) % 4) * 4 + (j - dj) % 4
        remote(
            ref, ref, self.gsend.at[2 * unit + p], self.grecv.at[2 * unit + p, slot], {"sp": self.idx(p, di, dj)}
        ).start()

    def arrive(self, unit, p, i, j):
        key = (unit, p, i % 4, j % 4)
        if key in self.waited or (i % 4, j % 4) == (0, 0):
            return
        self.waited.add(key)
        ref = self.ref(unit, p, self.idx(p, i, j))
        slot = (i % 4) * 4 + j % 4
        remote(
            ref, ref, self.gsend.at[2 * unit + p], self.grecv.at[2 * unit + p, slot], {"sp": self.idx(p, 1, 0)}
        ).wait_recv()

    def group(self, unit, p, i):
        for j in (0, -1, 1, 2):
            self.arrive(unit, p, i, j)

    def all(self, unit):
        for p in range(2):
            for i in (0, -1, 1, 2):
                self.group(unit, p, i)

    def opening(self, unit):
        for axis in range(2):
            for p in range(2):
                for d in (1, -1):
                    self.push(unit, p, 0, 0, axis, d)

    def events(self, unit):
        first = 1 if unit in (0, 3) else -1

        def turn(p, i, forward=None):
            def run():
                self.arrive(unit, p, i, 0)
                if forward:
                    self.push(unit, p, i, 0, 0, forward)
                for d in (1, -1):
                    self.push(unit, p, i, 0, 1, d)

            return run

        def relay(p, i):
            d = 1 if (i + unit) % 2 == 0 else -1

            def run():
                self.arrive(unit, p, i, -d)
                self.push(unit, p, i, -d, 1, d)

            return run

        both = range(2)
        steps = [turn(p, -first, first) for p in both] + [turn(p, first) for p in both]
        steps += [relay(p, 0) for p in both] + [turn(p, 2) for p in both]
        return steps + [relay(p, i) for i in (-1, 1, 2) for p in both]

    def drain(self, unit):
        for p in range(2):
            if unit % 2 == 0:
                ref = self.wvg.at[unit // 2, p, pl.ds(0, 15)]
            else:
                half = self.wo.shape[2] // 2
                ref = self.wo.at[unit // 2, pl.ds(0, 15), pl.ds(p * half, half)]
            remote(ref, ref, self.gsend.at[2 * unit + p], self.grecv.at[2 * unit + p, 0], {"sp": self.idx(p, 1, 0)}).wait_send()


def whole_kernel(
    layers, n_sp, n_tp, features,
    stream_ref, gain_ref, wv_hbm, wg_hbm, wo_hbm, taps_ref, gates_ref, rate_ref, out,
    wvg, wo, xg, ssg, base, own, perm, acc, mixb, mpad, sil, conv, convb, big, a_f, u_f, a_b, u_b, col,
    halo_p, halo_n, seg, ent, msg, slots,
    psend, precv, fbuf, far_in, nbuf, near_in,
    ld, gsend, grecv, asend, arecv, ssend, srecv, hsend, hrecv, csend, crecv, ds, dr, rs, rr,
):
    sp, tp = lax.axis_index("sp"), lax.axis_index("tp")
    tokens, width = mixb.shape
    feats = own.shape[1]
    joined = greet((("sp", n_sp, sp), ("tp", n_tp, tp)))
    ring = Ring(tp, n_tp)
    net = Weights(sp, 4, wvg, wo, gsend, grecv)
    pre = pown = big
    lanes_own = pl.ds(pl.multiple_of(tp * width, width), width)
    right, left = ring.at(1), ring.at(-1)

    loads = []
    for layer in range(layers):
        loads.append([
            pltpu.make_async_copy(wv_hbm.at[layer], wvg.at[layer, 0, sp], ld.at[3 * layer]),
            pltpu.make_async_copy(wg_hbm.at[layer], wvg.at[layer, 1, sp], ld.at[3 * layer + 1]),
        ])
        loads.append([pltpu.make_async_copy(wo_hbm.at[layer], wo.at[layer, sp], ld.at[3 * layer + 2])])
    for copies in loads:
        for copy in copies:
            copy.start()
    def opening(unit):
        for copy in loads[unit]:
            copy.wait()
        net.opening(unit)

    waiting = [iter([functools.partial(opening, unit)] + net.events(unit)) for unit in range(2 * layers)]
    plan = iter(PLAN)

    def slot():
        for unit in next(plan):
            next(waiting[int(unit)])()

    def project(layer, p, i):
        if p == 0:
            spots = [net.idx(p, i, j) for j in range(4)]
            halves = [pl.ds(pl.multiple_of(lax.rem(at, 2) * 256, 256), 256) for at in spots]
            terms = [
                jnp.dot(xg[at // 2, :, lanes], wvg[layer, p, at], preferred_element_type=F32)
                for at, lanes in zip(spots, halves)
            ]
        else:
            first = lax.rem(net.z + i + net.side, net.side) * 2
            terms = [
                jnp.dot(
                    xg[first + j],
                    wvg[layer, p, pl.ds(2 * (first + j), 2)].reshape(feats, width),
                    preferred_element_type=F32,
                )
                for j in range(2)
            ]
        acc[p] += functools.reduce(jnp.add, terms)

    gathers = [
        Gather(ring, xg, ssg.at[layer], asend, arecv, ssend.at[layer], srecv.at[layer], n_tp)
        for layer in range(layers)
    ]

    def gather_own(layer, source, half=None):
        gain = gain_ref[layer : layer + 1, lanes_own]
        gather_fill(source, gain, xg, ssg.at[layer], tp, half)

    def column(layer):
        total = jnp.sum(ssg[layer], axis=0)
        scale = lax.rsqrt(total / features + NORM_EPS)
        for k in range(tokens // 128):
            part = jnp.broadcast_to(scale[0:1, k * 128 : (k + 1) * 128], (128, 128))
            col[pl.ds(k * 128, 128), :] = part.T

    def clear(rows):
        zero = jnp.zeros((rows.size, width), F32)
        acc[0, rows, :] = zero
        acc[1, rows, :] = zero

    def mix(layer):
        def finish_v(rows):
            wide = jnp.concatenate([col[rows, :]] * (width // 128), axis=1)
            value = (acc[0, rows, :] * wide).astype(BF16)
            mixb[rows, :] = value
            acc[0, rows, :] = value.astype(F32)

        finish_v(pl.ds(0, 32))
        finish_v(pl.ds(tokens - 32, 32))
        head, tail = mixb.at[pl.ds(0, 16)], mixb.at[pl.ds(tokens - 16, 16)]
        hs, hr = hsend.at[layer], hrecv.at[layer]
        to_next = remote(tail, halo_p.at[layer], hs.at[0], hr.at[0], {"sp": lax.rem(sp + 1, n_sp)})
        to_prev = remote(head, halo_n.at[layer], hs.at[1], hr.at[1], {"sp": lax.rem(sp + n_sp - 1, n_sp)})
        to_next.start()
        to_prev.start()

        def finish_g(rows):
            wide = jnp.concatenate([col[rows, :]] * (width // 128), axis=1)
            gate = (acc[1, rows, :] * wide).astype(BF16).astype(F32)
            sil[rows, :] = gate * sigmoid(gate)
            mpad[pl.ds(aligned(rows.start + 16, 16), rows.size), :] = acc[0, rows, :]

        in_row_steps(tokens - 64, finish_v, 32, 32)
        in_row_steps(tokens, finish_g, 32)
        taps = taps_ref[layer, :, lanes_own]
        maps = [jnp.concatenate([gates_ref[layer, g, b] for g in range(4)], axis=1) for b in range(width // 128)]
        quarter = tokens // 4

        def gate_maps(rows):
            for b in range(width // 128):
                pre[b, rows, :] = jnp.dot(convb[rows, b * 128 : (b + 1) * 128], maps[b], preferred_element_type=F32)

        def convolve(rows):
            terms = [
                mpad[pl.ds(aligned(rows.start + 8 * k, 8), rows.size), :] * taps[k : k + 1, :]
                for k in range(4)
            ]
            value = (terms[0] + terms[1]) + (terms[2] + terms[3])
            conv[rows, :] = value
            convb[rows, :] = value.astype(BF16)

        in_row_steps(tokens - 64, convolve, 32, 32)
        gate_maps(pl.ds(quarter, 2 * quarter))
        slot()
        to_next.wait()
        to_prev.wait()
        sub = lax.broadcasted_iota(jnp.int32, (SEG, width), 0)
        before = halo_p[layer].astype(F32)
        after = halo_n[layer].astype(F32)
        for k in range(2):
            edge = jnp.where(sp > 0, before[8 * k + 7 : 8 * k + 8, :], 0.0)
            blk = acc[0, pl.ds(tokens - 16 + 8 * k, 8), :]
            mpad[pl.ds(8 * k, 8), :] = jnp.where(
                sub == 0, jnp.broadcast_to(edge, (SEG, width)), pltpu.roll(blk, 1, 0)
            )
        edge = jnp.where(sp < n_sp - 1, after[0:1, :], 0.0)
        blk = acc[0, pl.ds(0, 8), :]
        mpad[pl.ds(tokens + 16, 8), :] = jnp.where(
            sub == SEG - 1, jnp.broadcast_to(edge, (SEG, width)), pltpu.roll(blk, SEG - 1, 0)
        )
        convolve(pl.ds(0, 32))
        convolve(pl.ds(tokens - 32, 32))
        slot()
        gate_maps(pl.ds(0, quarter))
        gate_maps(pl.ds(3 * quarter, quarter))
        slot()
        rate_all = -GATE_SCALE * rate_ref[layer, :, lanes_own]
        for b in range(width // 128):
            lanes = pl.ds(b * 128, 128)
            rates = [rate_all[e : e + 1, b * 128 : (b + 1) * 128] for e in range(2)]

            def body(k, carry, b=b, lanes=lanes, rates=rates):
                p_f, h_f, p_b, h_b = carry
                rows = pl.ds(pl.multiple_of(k * ROWS, ROWS), ROWS)
                cv = conv[rows, lanes]
                kept = []
                for e, (a_ref, u_ref) in enumerate(((a_f, u_f), (a_b, u_b))):
                    r = sigmoid(pre[b, rows, 256 * e : 256 * e + 128])
                    i = sigmoid(pre[b, rows, 256 * e + 128 : 256 * e + 256])
                    log_a = rates[e] * r
                    decay = jnp.exp(log_a)
                    drive = jnp.sqrt(drive_square(-2.0 * log_a)) * i * cv
                    a_ref[rows, lanes] = decay
                    u_ref[rows, lanes] = drive
                    kept.append((decay, drive))
                for j in range(ROWS // 8):
                    at = slice(8 * j, 8 * j + 8)
                    d, u = kept[0][0][at], kept[0][1][at]
                    h_f = d * h_f + u
                    p_f = p_f * d
                    d, u = kept[1][0][at], kept[1][1][at]
                    h_b = h_b + p_b * u
                    p_b = p_b * d
                return p_f, h_f, p_b, h_b

            one, zero = jnp.ones((SEG, 128), F32), jnp.zeros((SEG, 128), F32)
            ends = lax.fori_loop(0, tokens // ROWS, body, (one, zero, one, zero))
            for k in range(4):
                seg[k, :, lanes] = ends[k]
            slot()

        sides = ((0, range(SEG)), (2, range(SEG - 1, -1, -1)))
        for e, (k, order) in enumerate(sides):
            prod = jnp.ones((1, width), F32)
            state = jnp.zeros((1, width), F32)
            for s in order:
                d = seg[k, s : s + 1, :]
                state = d * state + seg[k + 1, s : s + 1, :]
                prod = prod * d
            for b in range(width // 128):
                msg[layer, e, b : b + 1, :] = prod[:, b * 128 : (b + 1) * 128]
                msg[layer, e, 4 + b : 5 + b, :] = state[:, b * 128 : (b + 1) * 128]
        cs, cr = csend.at[layer], crecv.at[layer]
        for step in range(1, n_sp):
            dev = lax.rem(sp + step, n_sp)
            side = jnp.where(dev > sp, 0, 1)
            remote(msg.at[layer, side], slots.at[layer, sp], cs.at[dev], cr.at[sp], {"sp": dev}).start()
        slots[layer, sp] = jnp.zeros((8, 128), F32)
        slot()
        for step in range(1, n_sp):
            dev = lax.rem(sp + step, n_sp)
            remote(msg.at[layer, 0], slots.at[layer, dev], cs.at[dev], cr.at[dev], {"sp": dev}).wait()
        for e, (k, order) in enumerate(sides):
            carry = jnp.zeros((4, 128), F32)
            for q in range(n_sp) if e == 0 else range(n_sp - 1, -1, -1):
                live = (q < sp) if e == 0 else (q > sp)
                entry = slots[layer, q]
                carry = jnp.where(live, entry[0:4] * carry + entry[4:8], carry)
            state = jnp.concatenate([carry[b : b + 1, :] for b in range(width // 128)], axis=1)
            for s in order:
                ent[e, s : s + 1, :] = state
                state = seg[k, s : s + 1, :] * state + seg[k + 1, s : s + 1, :]
        def again(k, carry):
            h_f, h_b = carry
            for j in range(4):
                fwd = pl.ds(pl.multiple_of((4 * k + j) * SEG, SEG), SEG)
                bwd = pl.ds(pl.multiple_of((steps - 1 - 4 * k - j) * SEG, SEG), SEG)
                h_f = a_f[fwd, :] * h_f + u_f[fwd, :]
                u_f[fwd, :] = h_f
                h_b = a_b[bwd, :] * h_b + u_b[bwd, :]
                u_b[bwd, :] = h_b
            return h_f, h_b

        lax.fori_loop(0, steps // 4, again, (ent[0], ent[1]))

        def gated(rows):
            mixb[rows, :] = ((u_f[rows, :] + u_b[rows, :]) * sil[rows, :]).astype(BF16)

        in_row_steps(tokens, gated, 32)
        slot()

    half = tokens // 2
    top, low = pl.ds(0, half), pl.ds(half, half)

    def reduce(layer, source, target, chained):
        order = (2, 1, -1, 0)

        def product(k, other):
            block = ring.at(order[k], other=other)
            terms = [
                lax.dot_general(
                    mixb[...], wo[layer, 2 * block + part], (((1,), (1,)), ((), ())), preferred_element_type=F32
                )
                for part in range(2)
            ]
            return terms

        def across(k):
            return remote(psend.at[k], precv.at[k], ds.at[k], dr.at[k], {"tp": ring.sib})

        def send(k, src, dst, dev):
            remote(src, dst, rs.at[k], rr.at[k], {"tp": dev}).start()

        def paired(k, rows, into=None):
            def body(r):
                at = pl.ds(pl.multiple_of(rows.start + r.start, 32), r.size)
                value = pown[k, at, :] + precv[k, at, :].astype(F32)
                if into is None:
                    pown[k, at, :] = value
                else:
                    into[at if into.shape[0] == tokens else r, :] = value.astype(BF16)

            in_row_steps(rows.size, body, 32)

        for k in range(4):
            for part, term in enumerate(product(k, True)):
                psend[k, :, part * 256 : (part + 1) * 256] = term.astype(BF16)
            across(k).start()
            for part, term in enumerate(product(k, False)):
                pown[k, :, part * 256 : (part + 1) * 256] = term
            if k == 1:
                across(0).wait_recv()
                paired(0, top, fbuf)
                send(0, fbuf.at[top], far_in.at[0], right)
                paired(0, low, fbuf)
                send(1, fbuf.at[low], far_in.at[1], left)
            if k == 2:
                across(1).wait_recv()
                paired(1, low, nbuf.at[0])
                if not chained:
                    send(2, nbuf.at[0], near_in.at[0], right)
                paired(1, top)
            if k == 3:
                across(2).wait_recv()
                paired(2, top, nbuf.at[1])
                send(3, nbuf.at[1], near_in.at[1], left)
                paired(2, low)
            slot()
        across(3).wait_recv()
        paired(3, pl.ds(0, tokens))
        slot()

        def arrived(k, src, dst):
            remote(src, dst, rs.at[k], rr.at[k], {"tp": right}).wait_recv()

        def merged(k, rows, src, into):
            def body(r):
                at = pl.ds(pl.multiple_of(rows.start + r.start, 32), r.size)
                into[r, :] = (pown[k, at, :] + src[r, :].astype(F32)).astype(BF16)

            in_row_steps(half, body, 32)

        arrived(0, fbuf.at[top], far_in.at[0])
        merged(1, top, far_in.at[0], nbuf.at[2])
        send(4, nbuf.at[2], near_in.at[2], right)
        if chained:
            send(2, nbuf.at[0], near_in.at[0], right)
        arrived(1, fbuf.at[low], far_in.at[1])
        merged(2, low, far_in.at[1], nbuf.at[3])
        send(5, nbuf.at[3], near_in.at[3], left)
        slot()

        def total(rows, one, two):
            def body(r):
                at = pl.ds(pl.multiple_of(rows.start + r.start, 32), r.size)
                branch = pown[3, at, :] + near_in[one, r, :].astype(F32) + near_in[two, r, :].astype(F32)
                value = source[at, :].astype(F32) + branch
                target[at, :] = value.astype(BF16)

            in_row_steps(half, body, 32)

        if chained:
            gather = gathers[layer + 1]
            for k in (1, 2):
                arrived(2 + k, nbuf.at[k], near_in.at[k])
                if k == 1:
                    slot()
            total(top, 1, 2)
            gather_own(layer + 1, target, 0)
            gather.begin(0)
            slot()
            for k in (0, 3):
                arrived(2 + k, nbuf.at[k], near_in.at[k])
                if k == 0:
                    slot()
            total(low, 0, 3)
            gather_own(layer + 1, target, 1)
            gather.begin(1)
            gather.begin_squares()
            in_row_steps(tokens, clear, 32)
            slot()
        else:
            for k in range(4):
                arrived(2 + k, nbuf.at[k], near_in.at[k])
                if k == 1:
                    slot()
            total(top, 1, 2)
            total(low, 0, 3)
        for k in range(4):
            across(k).wait_send()
        for k in range(6):
            remote(nbuf.at[0], near_in.at[0], rs.at[k], rr.at[k], {"tp": right}).wait_send()

    steps = tokens // SEG

    def spread(rows):
        for b in range(feats // 128):
            perm[b, rows, :] = stream_ref[rows, b * 128 : (b + 1) * 128].astype(F32)

    def collect(rows):
        first = rows.start // SEG
        for b in range(feats // 128):
            parts = [perm[b, pl.ds(first + j, SEG, stride=steps), :] for j in range(rows.size // SEG)]
            base[rows, b * 128 : (b + 1) * 128] = jnp.concatenate(parts, axis=0).astype(BF16)

    in_row_steps(tokens, spread)
    in_row_steps(tokens, collect, 32)
    gather_own(0, base)
    joined()

    slot()
    gather = gathers[0]
    gather.begin(0)
    gather.begin(1)
    gather.begin_squares()
    in_row_steps(tokens, clear, 32)
    slot()
    for pair in ((0, 2), (1, 3), (4, 5)):
        for k in pair:
            gather.got(k)
        slot()
    gather.end()
    column(0)
    slot()
    for layer in range(layers):
        unit = 2 * layer
        for i in (0, -1, 1, 2):
            for p in range(2):
                slot()
                net.group(unit, p, i)
                project(layer, p, i)
        mix(layer)
        net.all(unit + 1)
        if layer + 1 < layers:
            reduce(layer, base, own, True)
            gather = gathers[layer + 1]
            for k in (0, 3, 2, 1, 4, 5):
                gather.got(k)
                slot()
            gather.end()
            column(layer + 1)
            slot()
        else:
            reduce(layer, own, out, False)
    for unit in range(2 * layers):
        net.drain(unit)


def whole_call(stream, gain, wv, wg, wo, taps, gates, rate, n_sp, n_tp):
    tokens, feats = stream.shape
    layers, rows, width = wv.shape
    half = tokens // 2
    blocks = width // 128
    vmem = pl.BlockSpec(memory_space=pltpu.VMEM)
    hbm = pl.BlockSpec(memory_space=pl.ANY)
    f32 = pltpu.VMEM((tokens, width), F32)
    b16 = pltpu.VMEM((tokens, width), BF16)
    dma = pltpu.SemaphoreType.DMA
    return pl.pallas_call(
        functools.partial(whole_kernel, layers, n_sp, n_tp, float(gain.shape[1])),
        out_shape=jax.ShapeDtypeStruct((tokens, feats), BF16),
        in_specs=[vmem, vmem, hbm, hbm, hbm, vmem, vmem, vmem],
        out_specs=vmem,
        scratch_shapes=[
            pltpu.VMEM((layers, 2, n_sp, rows, width), BF16),
            pltpu.VMEM((layers, n_sp, rows, width), BF16),
            pltpu.VMEM((n_tp, tokens, feats), BF16),
            pltpu.VMEM((layers, n_tp, 8, tokens), F32),
            b16, b16,
            pltpu.VMEM((feats // 128, tokens, 128), F32),
            pltpu.VMEM((2, tokens, width), F32),
            b16,
            pltpu.VMEM((tokens + 24, width), F32),
            f32, f32, b16,
            pltpu.VMEM((4, tokens, 512), F32),
            f32, f32, f32, f32,
            pltpu.VMEM((tokens, 128), F32),
            pltpu.VMEM((layers, 16, width), BF16),
            pltpu.VMEM((layers, 16, width), BF16),
            pltpu.VMEM((4, SEG, width), F32),
            pltpu.VMEM((2, SEG, width), F32),
            pltpu.VMEM((layers, 2, 8, 128), F32),
            pltpu.VMEM((layers, n_sp, 8, 128), F32),
            pltpu.VMEM((4, tokens, feats), BF16),
            pltpu.VMEM((4, tokens, feats), BF16),
            pltpu.VMEM((tokens, feats), BF16),
            pltpu.VMEM((2, half, feats), BF16),
            pltpu.VMEM((4, half, feats), BF16),
            pltpu.VMEM((4, half, feats), BF16),
            dma((3 * layers,)),
            dma((4 * layers,)),
            dma((4 * layers, 16)),
            dma((14,)),
            dma((14,)),
            dma((layers, n_tp)),
            dma((layers, n_tp)),
            dma((layers, 2)),
            dma((layers, 2)),
            dma((layers, n_sp)),
            dma((layers, n_sp)),
            dma((4,)),
            dma((4,)),
            dma((6,)),
            dma((6,)),
        ],
        compiler_params=pltpu.CompilerParams(
            collective_id=0, has_side_effects=True, vmem_limit_bytes=63_000_000
        ),
        cost_estimate=pl.CostEstimate(flops=20_000_000_000, bytes_accessed=8_000_000, transcendentals=0),
        name="both_layers",
    )(stream, gain, wv, wg, wo, taps, gates, rate)


def per_device(
    n_sp, n_tp, stream_in, norm_gain, value_proj, gate_proj, out_proj, conv_taps, block_gates, forget_rate
):
    width = value_proj.shape[2]
    layers = value_proj.shape[0]
    gates = block_gates.reshape(layers, 4, width // 128, 128, 128)
    stream = whole_call(
        stream_in, norm_gain, value_proj, gate_proj, out_proj, conv_taps, gates, forget_rate, n_sp, n_tp
    )
    tokens, feats = stream.shape
    return stream.reshape(tokens // SEG, SEG, feats).transpose(1, 0, 2).reshape(tokens, feats)


def solution(mesh):
    placed = (
        P("sp", "tp"),
        P(),
        P(None, "sp", "tp"),
        P(None, "sp", "tp"),
        P(None, "sp", "tp"),
        P(),
        P(None, None, None, "tp", None),
        P(),
    )
    body = functools.partial(per_device, mesh.shape["sp"], mesh.shape["tp"])
    return jax.shard_map(body, mesh=mesh, in_specs=placed, out_specs=P("sp", "tp"), check_vma=False)
```

```python
import functools

import jax
import jax.numpy as jnp
from jax import lax
from jax.experimental import pallas as pl
from jax.experimental.pallas import tpu as pltpu
from jax.sharding import PartitionSpec as P

GATE_SCALE = 8.0
NORM_EPS = 1e-06
MESH = pl.DeviceIdType.MESH
F32 = jnp.float32
BF16 = jnp.bfloat16
SEG = 8
ROWS = 64
PLAN = ('000', '00', '000', '001', '', '0', '', '0', '0010111', '1', '1', '', '1', '', '1111', '', '', '', '', '', '', '1112', '', '', '2', '', '2', '22', '', '22', '22', '2', '22', '23', '', '22', '', '33', '', '', '', '', '', '', '', '3', '', '3', '33333', '', '', '', '', '', '', '33333', '', '', '', '', '', '', '', '')


def remote(src, dst, send_sem, recv_sem, dev):
    return pltpu.make_async_remote_copy(
        src_ref=src, dst_ref=dst, send_sem=send_sem, recv_sem=recv_sem, device_id=dev, device_id_type=MESH
    )


def greet(groups):
    barrier = pltpu.get_barrier_semaphore()
    for axis, count, me in groups:
        for step in range(1, count):
            pl.semaphore_signal(barrier, inc=1, device_id={axis: lax.rem(me + step, count)}, device_id_type=MESH)
    return lambda: pl.semaphore_wait(barrier, sum(count - 1 for _, count, _ in groups))


def sigmoid(v):
    return 1.0 / (1.0 + jnp.exp(-v))


def drive_square(y):
    terms = [1.0, -1.0 / 2, 1.0 / 6, -1.0 / 24, 1.0 / 120, -1.0 / 720, 1.0 / 5040, -1.0 / 40320, 1.0 / 362880]
    total = jnp.full_like(y, terms[-1])
    for term in terms[-2::-1]:
        total = total * y + term
    return total * y


def in_row_steps(rows, body, size=ROWS, first=0):
    def step(k, carry):
        body(pl.ds(pl.multiple_of(first + k * size, size), size))
        return carry

    lax.fori_loop(0, rows // size, step, 0)


def aligned(at, size):
    return at if isinstance(at, int) else pl.multiple_of(at, size)


class Ring:
    def __init__(self, me, count):
        chips = count // 2
        self.chips = chips
        self.me = me
        self.x = me // 2
        self.c = lax.rem(me, 2)
        self.sib = self.x * 2 + 1 - self.c

    def at(self, step, other=False):
        core = 1 - self.c if other else self.c
        return lax.rem(self.x + step + self.chips, self.chips) * 2 + core


def gather_fill(own_ref, gain, xg, ssg, me, half=None):
    tokens = own_ref.shape[0]
    first, count = (0, tokens) if half is None else (half * tokens // 2, tokens // 2)

    def fill(rows):
        at = pl.ds(pl.multiple_of(first + rows.start, ROWS), rows.size)
        v = own_ref[at, :].astype(F32)
        xg[me, at, :] = (v * gain).astype(BF16)

    in_row_steps(count, fill)
    for k in range(first // 128, (first + count) // 128):
        v = own_ref[pl.ds(k * 128, 128), :].astype(F32)
        total = jnp.sum(v * v, axis=1, keepdims=True)
        ssg[me, :, pl.ds(k * 128, 128)] = jnp.broadcast_to(total, (128, 128)).T[0:8, :]


class Gather:
    def __init__(self, ring, xg, ssg, send, recv, ssend, srecv, count):
        self.ring, self.xg, self.ssg, self.count = ring, xg, ssg, count
        self.send, self.recv, self.ssend, self.srecv = send, recv, ssend, srecv
        half = xg.shape[1] // 2
        self.rows = (pl.ds(0, half), pl.ds(half, half))

    def push(self, part, k, dev):
        remote(part, part, self.send.at[k], self.recv.at[k], {"tp": dev}).start()

    def begin(self, half):
        ring = self.ring
        part = self.xg.at[ring.me, self.rows[half]]
        right, left = ring.at(1), ring.at(-1)
        if half == 0:
            self.push(part, 0, right)
            self.push(part, 3, left)
            self.push(part, 6, ring.sib)
        else:
            self.push(part, 2, left)
            self.push(part, 1, right)
            self.push(part, 13, ring.sib)

    def begin_squares(self):
        ring, ssg = self.ring, self.ssg
        for step in range(1, self.count):
            dev = lax.rem(ring.me + step, self.count)
            remote(ssg.at[ring.me], ssg.at[ring.me], self.ssend.at[dev], self.srecv.at[ring.me], {"tp": dev}).start()

    def got(self, k):
        ring = self.ring
        step, half = {0: (-1, 0), 1: (-1, 1), 2: (1, 1), 3: (1, 0), 4: (2, 0), 5: (2, 1)}[k]
        part = self.xg.at[ring.at(step), self.rows[half]]
        remote(part, part, self.send.at[k], self.recv.at[k], {"tp": ring.sib}).wait_recv()
        if k == 0:
            self.push(part, 4, ring.at(1))
        if k == 2:
            self.push(part, 5, ring.at(-1))
        self.push(part, 7 + k, ring.sib)

    def end(self):
        ring = self.ring
        owners = {6: (0, 0), 13: (0, 1), 7: (-1, 0), 8: (-1, 1), 9: (1, 1), 10: (1, 0), 11: (2, 0), 12: (2, 1)}
        for k, (step, half) in owners.items():
            part = self.xg.at[ring.at(step, other=True), self.rows[half]]
            remote(part, part, self.send.at[k], self.recv.at[k], {"tp": ring.sib}).wait()
        for k in range(6):
            part = self.xg.at[ring.me, self.rows[0]]
            remote(part, part, self.send.at[k], self.recv.at[k], {"tp": ring.at(1)}).wait_send()
        for step in range(1, self.count):
            dev = lax.rem(ring.me + step, self.count)
            remote(self.ssg.at[dev], self.ssg.at[dev], self.ssend.at[dev], self.srecv.at[dev], {"tp": dev}).wait()


class Weights:
    def __init__(self, me, side, wvg, wo, gsend, grecv):
        self.y, self.z, self.side = lax.rem(me, side), me // side, side
        self.wvg, self.wo, self.gsend, self.grecv = wvg, wo, gsend, grecv
        self.waited = set()

    def idx(self, p, i, j):
        dy, dz = (i, j) if p == 0 else (j, i)
        return lax.rem(self.z + dz + self.side, self.side) * self.side + lax.rem(self.y + dy + self.side, self.side)

    def ref(self, unit, p, at):
        if unit % 2 == 0:
            return self.wvg.at[unit // 2, p, at]
        half = self.wo.shape[2] // 2
        return self.wo.at[unit // 2, at, pl.ds(p * half, half)]

    def push(self, unit, p, i, j, axis, d):
        ref = self.ref(unit, p, self.idx(p, i, j))
        di, dj = (d, 0) if axis == 0 else (0, d)
        slot = ((i - di) % 4) * 4 + (j - dj) % 4
        remote(
            ref, ref, self.gsend.at[2 * unit + p], self.grecv.at[2 * unit + p, slot], {"sp": self.idx(p, di, dj)}
        ).start()

    def arrive(self, unit, p, i, j):
        key = (unit, p, i % 4, j % 4)
        if key in self.waited or (i % 4, j % 4) == (0, 0):
            return
        self.waited.add(key)
        ref = self.ref(unit, p, self.idx(p, i, j))
        slot = (i % 4) * 4 + j % 4
        remote(
            ref, ref, self.gsend.at[2 * unit + p], self.grecv.at[2 * unit + p, slot], {"sp": self.idx(p, 1, 0)}
        ).wait_recv()

    def group(self, unit, p, i):
        for j in (0, -1, 1, 2):
            self.arrive(unit, p, i, j)

    def all(self, unit):
        for p in range(2):
            for i in (0, -1, 1, 2):
                self.group(unit, p, i)

    def opening(self, unit):
        for axis in range(2):
            for p in range(2):
                for d in (1, -1):
                    self.push(unit, p, 0, 0, axis, d)

    def events(self, unit):
        first = 1 if unit in (0, 3) else -1

        def turn(p, i, forward=None):
            def run():
                self.arrive(unit, p, i, 0)
                if forward:
                    self.push(unit, p, i, 0, 0, forward)
                for d in (1, -1):
                    self.push(unit, p, i, 0, 1, d)

            return run

        def relay(p, i):
            d = 1 if (i + unit) % 2 == 0 else -1

            def run():
                self.arrive(unit, p, i, -d)
                self.push(unit, p, i, -d, 1, d)

            return run

        both = range(2)
        steps = [turn(p, -first, first) for p in both] + [turn(p, first) for p in both]
        steps += [relay(p, 0) for p in both] + [turn(p, 2) for p in both]
        return steps + [relay(p, i) for i in (-1, 1, 2) for p in both]

    def drain(self, unit):
        for p in range(2):
            if unit % 2 == 0:
                ref = self.wvg.at[unit // 2, p, pl.ds(0, 15)]
            else:
                half = self.wo.shape[2] // 2
                ref = self.wo.at[unit // 2, pl.ds(0, 15), pl.ds(p * half, half)]
            remote(ref, ref, self.gsend.at[2 * unit + p], self.grecv.at[2 * unit + p, 0], {"sp": self.idx(p, 1, 0)}).wait_send()


def whole_kernel(
    layers, n_sp, n_tp, features,
    stream_hbm, gain_hbm, wv_hbm, wg_hbm, wo_hbm, taps_hbm, gates_hbm, rate_hbm, out_hbm,
    wvg, wo, xg, ssg, base, own, perm, acc, mixb, mpad, sil, conv, convb, big, a_f, u_f, a_b, u_b, col,
    halo_p, halo_n, seg, ent, msg, slots,
    psend, precv, fbuf, far_in, nbuf, near_in,
    stream_ref, gain_ref, taps_ref, gates_ref, rate_ref, ld, ins, outs, gsend, grecv, asend, arecv, ssend, srecv, hsend, hrecv, csend, crecv, ds, dr, rs, rr,
):
    sp, tp = lax.axis_index("sp"), lax.axis_index("tp")
    tokens, width = mixb.shape
    feats = own.shape[1]
    joined = greet((("sp", n_sp, sp), ("tp", n_tp, tp)))
    ring = Ring(tp, n_tp)
    net = Weights(sp, 4, wvg, wo, gsend, grecv)
    pre = pown = big
    lanes_own = pl.ds(pl.multiple_of(tp * width, width), width)
    right, left = ring.at(1), ring.at(-1)

    inputs = [
        pltpu.make_async_copy(stream_hbm, stream_ref, ins.at[0]),
        pltpu.make_async_copy(gain_hbm.at[:, lanes_own], gain_ref, ins.at[1]),
        pltpu.make_async_copy(taps_hbm.at[:, :, lanes_own], taps_ref, ins.at[2]),
        pltpu.make_async_copy(gates_hbm, gates_ref, ins.at[3]),
        pltpu.make_async_copy(rate_hbm.at[:, :, lanes_own], rate_ref, ins.at[4]),
    ]
    for copy in inputs:
        copy.start()
    loads = []
    for layer in range(layers):
        loads.append([
            pltpu.make_async_copy(wv_hbm.at[layer], wvg.at[layer, 0, sp], ld.at[3 * layer]),
            pltpu.make_async_copy(wg_hbm.at[layer], wvg.at[layer, 1, sp], ld.at[3 * layer + 1]),
        ])
        loads.append([pltpu.make_async_copy(wo_hbm.at[layer], wo.at[layer, sp], ld.at[3 * layer + 2])])
    for copies in loads:
        for copy in copies:
            copy.start()
    def opening(unit):
        for copy in loads[unit]:
            copy.wait()
        net.opening(unit)

    waiting = [iter([functools.partial(opening, unit)] + net.events(unit)) for unit in range(2 * layers)]
    plan = iter(PLAN)

    def slot():
        for unit in next(plan):
            next(waiting[int(unit)])()

    def project(layer, p, i):
        if p == 0:
            spots = [net.idx(p, i, j) for j in range(4)]
            halves = [pl.ds(pl.multiple_of(lax.rem(at, 2) * 256, 256), 256) for at in spots]
            terms = [
                jnp.dot(xg[at // 2, :, lanes], wvg[layer, p, at], preferred_element_type=F32)
                for at, lanes in zip(spots, halves)
            ]
        else:
            first = lax.rem(net.z + i + net.side, net.side) * 2
            terms = [
                jnp.dot(
                    xg[first + j],
                    wvg[layer, p, pl.ds(2 * (first + j), 2)].reshape(feats, width),
                    preferred_element_type=F32,
                )
                for j in range(2)
            ]
        acc[p] += functools.reduce(jnp.add, terms)

    gathers = [
        Gather(ring, xg, ssg.at[layer], asend, arecv, ssend.at[layer], srecv.at[layer], n_tp)
        for layer in range(layers)
    ]

    def gather_own(layer, source, half=None):
        gain = gain_ref[layer : layer + 1, :]
        gather_fill(source, gain, xg, ssg.at[layer], tp, half)

    def column(layer):
        total = jnp.sum(ssg[layer], axis=0)
        scale = lax.rsqrt(total / features + NORM_EPS)
        for k in range(tokens // 128):
            part = jnp.broadcast_to(scale[0:1, k * 128 : (k + 1) * 128], (128, 128))
            col[pl.ds(k * 128, 128), :] = part.T

    def clear(rows):
        zero = jnp.zeros((rows.size, width), F32)
        acc[0, rows, :] = zero
        acc[1, rows, :] = zero

    def mix(layer):
        def finish_v(rows):
            wide = jnp.concatenate([col[rows, :]] * (width // 128), axis=1)
            value = (acc[0, rows, :] * wide).astype(BF16)
            mixb[rows, :] = value
            acc[0, rows, :] = value.astype(F32)

        if not layer:
            for copy in inputs[2:]:
                copy.wait()
        finish_v(pl.ds(0, 32))
        finish_v(pl.ds(tokens - 32, 32))
        head, tail = mixb.at[pl.ds(0, 16)], mixb.at[pl.ds(tokens - 16, 16)]
        hs, hr = hsend.at[layer], hrecv.at[layer]
        to_next = remote(tail, halo_p.at[layer], hs.at[0], hr.at[0], {"sp": lax.rem(sp + 1, n_sp)})
        to_prev = remote(head, halo_n.at[layer], hs.at[1], hr.at[1], {"sp": lax.rem(sp + n_sp - 1, n_sp)})
        to_next.start()
        to_prev.start()

        def finish_g(rows):
            wide = jnp.concatenate([col[rows, :]] * (width // 128), axis=1)
            gate = (acc[1, rows, :] * wide).astype(BF16).astype(F32)
            sil[rows, :] = gate * sigmoid(gate)
            mpad[pl.ds(aligned(rows.start + 16, 16), rows.size), :] = acc[0, rows, :]

        in_row_steps(tokens - 64, finish_v, 32, 32)
        in_row_steps(tokens, finish_g, 32)
        taps = taps_ref[layer]
        maps = [jnp.concatenate([gates_ref[layer, g, b] for g in range(4)], axis=1) for b in range(width // 128)]
        quarter = tokens // 4

        def gate_maps(rows):
            for b in range(width // 128):
                pre[b, rows, :] = jnp.dot(convb[rows, b * 128 : (b + 1) * 128], maps[b], preferred_element_type=F32)

        def convolve(rows):
            terms = [
                mpad[pl.ds(aligned(rows.start + 8 * k, 8), rows.size), :] * taps[k : k + 1, :]
                for k in range(4)
            ]
            value = (terms[0] + terms[1]) + (terms[2] + terms[3])
            conv[rows, :] = value
            convb[rows, :] = value.astype(BF16)

        in_row_steps(tokens - 64, convolve, 32, 32)
        gate_maps(pl.ds(quarter, 2 * quarter))
        slot()
        to_next.wait()
        to_prev.wait()
        sub = lax.broadcasted_iota(jnp.int32, (SEG, width), 0)
        before = halo_p[layer].astype(F32)
        after = halo_n[layer].astype(F32)
        for k in range(2):
            edge = jnp.where(sp > 0, before[8 * k + 7 : 8 * k + 8, :], 0.0)
            blk = acc[0, pl.ds(tokens - 16 + 8 * k, 8), :]
            mpad[pl.ds(8 * k, 8), :] = jnp.where(
                sub == 0, jnp.broadcast_to(edge, (SEG, width)), pltpu.roll(blk, 1, 0)
            )
        edge = jnp.where(sp < n_sp - 1, after[0:1, :], 0.0)
        blk = acc[0, pl.ds(0, 8), :]
        mpad[pl.ds(tokens + 16, 8), :] = jnp.where(
            sub == SEG - 1, jnp.broadcast_to(edge, (SEG, width)), pltpu.roll(blk, SEG - 1, 0)
        )
        convolve(pl.ds(0, 32))
        convolve(pl.ds(tokens - 32, 32))
        slot()
        gate_maps(pl.ds(0, quarter))
        gate_maps(pl.ds(3 * quarter, quarter))
        slot()
        rate_all = -GATE_SCALE * rate_ref[layer]
        for b in range(width // 128):
            lanes = pl.ds(b * 128, 128)
            rates = [rate_all[e : e + 1, b * 128 : (b + 1) * 128] for e in range(2)]

            def body(k, carry, b=b, lanes=lanes, rates=rates):
                p_f, h_f, p_b, h_b = carry
                rows = pl.ds(pl.multiple_of(k * ROWS, ROWS), ROWS)
                cv = conv[rows, lanes]
                kept = []
                for e, (a_ref, u_ref) in enumerate(((a_f, u_f), (a_b, u_b))):
                    r = sigmoid(pre[b, rows, 256 * e : 256 * e + 128])
                    i = sigmoid(pre[b, rows, 256 * e + 128 : 256 * e + 256])
                    log_a = rates[e] * r
                    decay = jnp.exp(log_a)
                    drive = jnp.sqrt(drive_square(-2.0 * log_a)) * i * cv
                    a_ref[rows, lanes] = decay
                    u_ref[rows, lanes] = drive
                    kept.append((decay, drive))
                for j in range(ROWS // 8):
                    at = slice(8 * j, 8 * j + 8)
                    d, u = kept[0][0][at], kept[0][1][at]
                    h_f = d * h_f + u
                    p_f = p_f * d
                    d, u = kept[1][0][at], kept[1][1][at]
                    h_b = h_b + p_b * u
                    p_b = p_b * d
                return p_f, h_f, p_b, h_b

            one, zero = jnp.ones((SEG, 128), F32), jnp.zeros((SEG, 128), F32)
            ends = lax.fori_loop(0, tokens // ROWS, body, (one, zero, one, zero))
            for k in range(4):
                seg[k, :, lanes] = ends[k]
            slot()

        sides = ((0, range(SEG)), (2, range(SEG - 1, -1, -1)))
        for e, (k, order) in enumerate(sides):
            prod = jnp.ones((1, width), F32)
            state = jnp.zeros((1, width), F32)
            for s in order:
                d = seg[k, s : s + 1, :]
                state = d * state + seg[k + 1, s : s + 1, :]
                prod = prod * d
            for b in range(width // 128):
                msg[layer, e, b : b + 1, :] = prod[:, b * 128 : (b + 1) * 128]
                msg[layer, e, 4 + b : 5 + b, :] = state[:, b * 128 : (b + 1) * 128]
        cs, cr = csend.at[layer], crecv.at[layer]
        for step in range(1, n_sp):
            dev = lax.rem(sp + step, n_sp)
            side = jnp.where(dev > sp, 0, 1)
            remote(msg.at[layer, side], slots.at[layer, sp], cs.at[dev], cr.at[sp], {"sp": dev}).start()
        slots[layer, sp] = jnp.zeros((8, 128), F32)
        slot()
        for step in range(1, n_sp):
            dev = lax.rem(sp + step, n_sp)
            remote(msg.at[layer, 0], slots.at[layer, dev], cs.at[dev], cr.at[dev], {"sp": dev}).wait()
        for e, (k, order) in enumerate(sides):
            carry = jnp.zeros((4, 128), F32)
            for q in range(n_sp) if e == 0 else range(n_sp - 1, -1, -1):
                live = (q < sp) if e == 0 else (q > sp)
                entry = slots[layer, q]
                carry = jnp.where(live, entry[0:4] * carry + entry[4:8], carry)
            state = jnp.concatenate([carry[b : b + 1, :] for b in range(width // 128)], axis=1)
            for s in order:
                ent[e, s : s + 1, :] = state
                state = seg[k, s : s + 1, :] * state + seg[k + 1, s : s + 1, :]
        def again(k, carry):
            h_f, h_b = carry
            for j in range(4):
                fwd = pl.ds(pl.multiple_of((4 * k + j) * SEG, SEG), SEG)
                bwd = pl.ds(pl.multiple_of((steps - 1 - 4 * k - j) * SEG, SEG), SEG)
                h_f = a_f[fwd, :] * h_f + u_f[fwd, :]
                u_f[fwd, :] = h_f
                h_b = a_b[bwd, :] * h_b + u_b[bwd, :]
                u_b[bwd, :] = h_b
            return h_f, h_b

        lax.fori_loop(0, steps // 4, again, (ent[0], ent[1]))

        def gated(rows):
            mixb[rows, :] = ((u_f[rows, :] + u_b[rows, :]) * sil[rows, :]).astype(BF16)

        in_row_steps(tokens, gated, 32)
        slot()

    half = tokens // 2
    top, low = pl.ds(0, half), pl.ds(half, half)

    def result(rows):
        return pltpu.make_async_copy(base.at[rows], out_hbm.at[rows], outs.at[rows.start // half])

    def reduce(layer, source, target, chained):
        order = (2, 1, -1, 0)

        def product(k, other):
            block = ring.at(order[k], other=other)
            terms = [
                lax.dot_general(
                    mixb[...], wo[layer, 2 * block + part], (((1,), (1,)), ((), ())), preferred_element_type=F32
                )
                for part in range(2)
            ]
            return terms

        def across(k):
            return remote(psend.at[k], precv.at[k], ds.at[k], dr.at[k], {"tp": ring.sib})

        def send(k, src, dst, dev):
            remote(src, dst, rs.at[k], rr.at[k], {"tp": dev}).start()

        def paired(k, rows, into=None):
            def body(r):
                at = pl.ds(pl.multiple_of(rows.start + r.start, 32), r.size)
                value = pown[k, at, :] + precv[k, at, :].astype(F32)
                if into is None:
                    pown[k, at, :] = value
                else:
                    into[at if into.shape[0] == tokens else r, :] = value.astype(BF16)

            in_row_steps(rows.size, body, 32)

        for k in range(4):
            for part, term in enumerate(product(k, True)):
                psend[k, :, part * 256 : (part + 1) * 256] = term.astype(BF16)
            across(k).start()
            for part, term in enumerate(product(k, False)):
                pown[k, :, part * 256 : (part + 1) * 256] = term
            if k == 1:
                across(0).wait_recv()
                paired(0, top, fbuf)
                send(0, fbuf.at[top], far_in.at[0], right)
                paired(0, low, fbuf)
                send(1, fbuf.at[low], far_in.at[1], left)
            if k == 2:
                across(1).wait_recv()
                paired(1, low, nbuf.at[0])
                if not chained:
                    send(2, nbuf.at[0], near_in.at[0], right)
                paired(1, top)
            if k == 3:
                across(2).wait_recv()
                paired(2, top, nbuf.at[1])
                send(3, nbuf.at[1], near_in.at[1], left)
                paired(2, low)
            slot()
        across(3).wait_recv()
        paired(3, pl.ds(0, tokens))
        slot()

        def arrived(k, src, dst):
            remote(src, dst, rs.at[k], rr.at[k], {"tp": right}).wait_recv()

        def merged(k, rows, src, into):
            def body(r):
                at = pl.ds(pl.multiple_of(rows.start + r.start, 32), r.size)
                into[r, :] = (pown[k, at, :] + src[r, :].astype(F32)).astype(BF16)

            in_row_steps(half, body, 32)

        arrived(0, fbuf.at[top], far_in.at[0])
        merged(1, top, far_in.at[0], nbuf.at[2])
        send(4, nbuf.at[2], near_in.at[2], right)
        if chained:
            send(2, nbuf.at[0], near_in.at[0], right)
        arrived(1, fbuf.at[low], far_in.at[1])
        merged(2, low, far_in.at[1], nbuf.at[3])
        send(5, nbuf.at[3], near_in.at[3], left)
        slot()

        def total(rows, one, two):
            def body(r):
                at = pl.ds(pl.multiple_of(rows.start + r.start, 32), r.size)
                branch = pown[3, at, :] + near_in[one, r, :].astype(F32) + near_in[two, r, :].astype(F32)
                value = source[at, :].astype(F32) + branch
                target[at, :] = value.astype(BF16)

            in_row_steps(half, body, 32)

        if chained:
            gather = gathers[layer + 1]
            for k in (1, 2):
                arrived(2 + k, nbuf.at[k], near_in.at[k])
                if k == 1:
                    slot()
            total(top, 1, 2)
            gather_own(layer + 1, target, 0)
            gather.begin(0)
            slot()
            for k in (0, 3):
                arrived(2 + k, nbuf.at[k], near_in.at[k])
                if k == 0:
                    slot()
            total(low, 0, 3)
            gather_own(layer + 1, target, 1)
            gather.begin(1)
            gather.begin_squares()
            in_row_steps(tokens, clear, 32)
            slot()
        else:
            for k in range(4):
                arrived(2 + k, nbuf.at[k], near_in.at[k])
                if k == 1:
                    slot()
            total(top, 1, 2)
            result(top).start()
            total(low, 0, 3)
            result(low).start()
        for k in range(4):
            across(k).wait_send()
        for k in range(6):
            remote(nbuf.at[0], near_in.at[0], rs.at[k], rr.at[k], {"tp": right}).wait_send()

    steps = tokens // SEG

    def spread(rows):
        for b in range(feats // 128):
            perm[b, rows, :] = stream_ref[rows, b * 128 : (b + 1) * 128].astype(F32)

    def collect(rows):
        first = rows.start // SEG
        for b in range(feats // 128):
            parts = [perm[b, pl.ds(first + j, SEG, stride=steps), :] for j in range(rows.size // SEG)]
            base[rows, b * 128 : (b + 1) * 128] = jnp.concatenate(parts, axis=0).astype(BF16)

    inputs[0].wait()
    in_row_steps(tokens, spread)
    in_row_steps(tokens, collect, 32)
    inputs[1].wait()
    gather_own(0, base)
    joined()

    slot()
    gather = gathers[0]
    gather.begin(0)
    gather.begin(1)
    gather.begin_squares()
    in_row_steps(tokens, clear, 32)
    slot()
    for pair in ((0, 2), (1, 3), (4, 5)):
        for k in pair:
            gather.got(k)
        slot()
    gather.end()
    column(0)
    slot()
    for layer in range(layers):
        unit = 2 * layer
        for i in (0, -1, 1, 2):
            for p in range(2):
                slot()
                net.group(unit, p, i)
                project(layer, p, i)
        mix(layer)
        net.all(unit + 1)
        if layer + 1 < layers:
            reduce(layer, base, own, True)
            gather = gathers[layer + 1]
            for k in (0, 3, 2, 1, 4, 5):
                gather.got(k)
                slot()
            gather.end()
            column(layer + 1)
            slot()
        else:
            reduce(layer, own, base, False)
            result(top).wait()
            result(low).wait()
    for unit in range(2 * layers):
        net.drain(unit)


def whole_call(stream, gain, wv, wg, wo, taps, gates, rate, n_sp, n_tp):
    tokens, feats = stream.shape
    layers, rows, width = wv.shape
    half = tokens // 2
    blocks = width // 128
    hbm = pl.BlockSpec(memory_space=pl.ANY)
    f32 = pltpu.VMEM((tokens, width), F32)
    b16 = pltpu.VMEM((tokens, width), BF16)
    dma = pltpu.SemaphoreType.DMA
    return pl.pallas_call(
        functools.partial(whole_kernel, layers, n_sp, n_tp, float(gain.shape[1])),
        out_shape=jax.ShapeDtypeStruct((tokens, feats), BF16),
        in_specs=[hbm] * 8,
        out_specs=hbm,
        scratch_shapes=[
            pltpu.VMEM((layers, 2, n_sp, rows, width), BF16),
            pltpu.VMEM((layers, n_sp, rows, width), BF16),
            pltpu.VMEM((n_tp, tokens, feats), BF16),
            pltpu.VMEM((layers, n_tp, 8, tokens), F32),
            b16, b16,
            pltpu.VMEM((feats // 128, tokens, 128), F32),
            pltpu.VMEM((2, tokens, width), F32),
            b16,
            pltpu.VMEM((tokens + 24, width), F32),
            f32, f32, b16,
            pltpu.VMEM((4, tokens, 512), F32),
            f32, f32, f32, f32,
            pltpu.VMEM((tokens, 128), F32),
            pltpu.VMEM((layers, 16, width), BF16),
            pltpu.VMEM((layers, 16, width), BF16),
            pltpu.VMEM((4, SEG, width), F32),
            pltpu.VMEM((2, SEG, width), F32),
            pltpu.VMEM((layers, 2, 8, 128), F32),
            pltpu.VMEM((layers, n_sp, 8, 128), F32),
            pltpu.VMEM((4, tokens, feats), BF16),
            pltpu.VMEM((4, tokens, feats), BF16),
            pltpu.VMEM((tokens, feats), BF16),
            pltpu.VMEM((2, half, feats), BF16),
            pltpu.VMEM((4, half, feats), BF16),
            pltpu.VMEM((4, half, feats), BF16),
            b16,
            pltpu.VMEM((layers, feats), F32),
            pltpu.VMEM((layers, 4, width), F32),
            pltpu.VMEM(gates.shape, BF16),
            pltpu.VMEM((layers, 2, width), F32),
            dma((3 * layers,)),
            dma((5,)),
            dma((2,)),
            dma((4 * layers,)),
            dma((4 * layers, 16)),
            dma((14,)),
            dma((14,)),
            dma((layers, n_tp)),
            dma((layers, n_tp)),
            dma((layers, 2)),
            dma((layers, 2)),
            dma((layers, n_sp)),
            dma((layers, n_sp)),
            dma((4,)),
            dma((4,)),
            dma((6,)),
            dma((6,)),
        ],
        compiler_params=pltpu.CompilerParams(
            collective_id=0, has_side_effects=True, vmem_limit_bytes=63_000_000
        ),
        cost_estimate=pl.CostEstimate(flops=20_000_000_000, bytes_accessed=8_000_000, transcendentals=0),
        name="both_layers",
    )(stream, gain, wv, wg, wo, taps, gates, rate)


def per_device(
    n_sp, n_tp, stream_in, norm_gain, value_proj, gate_proj, out_proj, conv_taps, block_gates, forget_rate
):
    width = value_proj.shape[2]
    layers = value_proj.shape[0]
    gates = block_gates.reshape(layers, 4, width // 128, 128, 128)
    stream = whole_call(
        stream_in, norm_gain, value_proj, gate_proj, out_proj, conv_taps, gates, forget_rate, n_sp, n_tp
    )
    tokens, feats = stream.shape
    return stream.reshape(tokens // SEG, SEG, feats).transpose(1, 0, 2).reshape(tokens, feats)


def solution(mesh):
    placed = (
        P("sp", "tp"),
        P(),
        P(None, "sp", "tp"),
        P(None, "sp", "tp"),
        P(None, "sp", "tp"),
        P(),
        P(None, None, None, "tp", None),
        P(),
    )
    body = functools.partial(per_device, mesh.shape["sp"], mesh.shape["tp"])
    return jax.shard_map(body, mesh=mesh, in_specs=placed, out_specs=P("sp", "tp"), check_vma=False)
```

```python
import functools

import jax
import jax.numpy as jnp
from jax import lax
from jax.experimental import pallas as pl
from jax.experimental.pallas import tpu as pltpu
from jax.sharding import PartitionSpec as P

GATE_SCALE = 8.0
NORM_EPS = 1e-06
MESH = pl.DeviceIdType.MESH
F32 = jnp.float32
BF16 = jnp.bfloat16
EDGE = 16
SEG = 8
ROWS = 64
PLAN = ('000', '00', '000', '001', '', '0', '', '0', '0010111', '1', '1', '', '1', '', '1111', '', '', '', '', '', '', '1112', '', '', '2', '', '2', '22', '', '22', '22', '2', '22', '23', '', '22', '', '33', '', '', '', '', '', '', '', '3', '', '3', '33333', '', '', '', '', '', '', '33333', '', '', '', '', '', '', '', '')


def remote(src, dst, send_sem, recv_sem, dev):
    return pltpu.make_async_remote_copy(
        src_ref=src, dst_ref=dst, send_sem=send_sem, recv_sem=recv_sem, device_id=dev, device_id_type=MESH
    )


def greet(groups):
    barrier = pltpu.get_barrier_semaphore()
    for axis, count, me in groups:
        for step in range(1, count):
            pl.semaphore_signal(barrier, inc=1, device_id={axis: lax.rem(me + step, count)}, device_id_type=MESH)
    return lambda: pl.semaphore_wait(barrier, sum(count - 1 for _, count, _ in groups))


def sigmoid(v):
    return 1.0 / (1.0 + jnp.exp(-v))


def drive_square(y):
    terms = [0.999999999543, -0.499999943611, 0.166665528456, -0.0416580188735, 0.00830184073719, -0.00132924407794, 0.000140574729006]
    total = jnp.full_like(y, terms[-1])
    for term in terms[-2::-1]:
        total = total * y + term
    return total * y


def in_row_steps(rows, body, size=ROWS, first=0):
    def step(k, carry):
        body(pl.ds(pl.multiple_of(first + k * size, size), size))
        return carry

    lax.fori_loop(0, rows // size, step, 0)


def aligned(at, size):
    return at if isinstance(at, int) else pl.multiple_of(at, size)


class Ring:
    def __init__(self, me, count):
        chips = count // 2
        self.chips = chips
        self.me = me
        self.x = me // 2
        self.c = lax.rem(me, 2)
        self.sib = self.x * 2 + 1 - self.c

    def at(self, step, other=False):
        core = 1 - self.c if other else self.c
        return lax.rem(self.x + step + self.chips, self.chips) * 2 + core


def gather_fill(own_ref, gain, xg, ssg, me, half=None):
    tokens = own_ref.shape[0]
    first, count = (0, tokens) if half is None else (half * tokens // 2, tokens // 2)

    def fill(rows):
        at = pl.ds(pl.multiple_of(first + rows.start, ROWS), rows.size)
        v = own_ref[at, :].astype(F32)
        xg[me, at, :] = (v * gain).astype(BF16)

    in_row_steps(count, fill)
    for k in range(first // 128, (first + count) // 128):
        v = own_ref[pl.ds(k * 128, 128), :].astype(F32)
        total = jnp.sum(v * v, axis=1, keepdims=True)
        ssg[me, :, pl.ds(k * 128, 128)] = jnp.broadcast_to(total, (128, 128)).T[0:8, :]


class Gather:
    def __init__(self, ring, xg, ssg, send, recv, ssend, srecv, count):
        self.ring, self.xg, self.ssg, self.count = ring, xg, ssg, count
        self.send, self.recv, self.ssend, self.srecv = send, recv, ssend, srecv
        half = (xg.shape[1] - EDGE) // 2
        self.rows = (pl.ds(0, half), pl.ds(half, half))

    def push(self, part, k, dev):
        remote(part, part, self.send.at[0], self.recv.at[min(k, 6)], {"tp": dev}).start()

    def begin(self, half):
        ring = self.ring
        part = self.xg.at[ring.me, self.rows[half]]
        right, left = ring.at(1), ring.at(-1)
        if half == 0:
            self.push(part, 0, right)
            self.push(part, 3, left)
            self.push(part, 6, ring.sib)
        else:
            self.push(part, 2, left)
            self.push(part, 1, right)
            self.push(part, 13, ring.sib)

    def begin_squares(self):
        ring, ssg = self.ring, self.ssg
        for step in range(1, self.count):
            dev = lax.rem(ring.me + step, self.count)
            remote(ssg.at[ring.me], ssg.at[ring.me], self.ssend, self.srecv, {"tp": dev}).start()

    def got(self, k):
        ring = self.ring
        step, half = {0: (-1, 0), 1: (-1, 1), 2: (1, 1), 3: (1, 0), 4: (2, 0), 5: (2, 1)}[k]
        part = self.xg.at[ring.at(step), self.rows[half]]
        remote(part, part, self.send.at[0], self.recv.at[k], {"tp": ring.sib}).wait_recv()
        if k == 0:
            self.push(part, 4, ring.at(1))
        if k == 2:
            self.push(part, 5, ring.at(-1))
        self.push(part, 7 + k, ring.sib)

    def end(self):
        count, dev = self.count, {"tp": self.ring.sib}
        half = self.rows[0].size
        came = self.xg.at[:, pl.ds(0, half)]
        remote(came, came, self.send.at[0], self.recv.at[6], dev).wait_recv()
        sent = self.xg.at[pl.ds(0, count - 1), pl.ds(0, 2 * half)]
        remote(sent, sent, self.send.at[0], self.recv.at[6], dev).wait_send()
        others = self.ssg.at[pl.ds(0, count - 1)]
        remote(others, others, self.ssend, self.srecv, dev).wait()


class Weights:
    def __init__(self, me, side, wvg, wo, gsend, grecv):
        self.y, self.z, self.side = lax.rem(me, side), me // side, side
        self.wvg, self.wo, self.gsend, self.grecv = wvg, wo, gsend, grecv
        self.waited = set()

    def idx(self, p, i, j):
        dy, dz = (i, j) if p == 0 else (j, i)
        return lax.rem(self.z + dz + self.side, self.side) * self.side + lax.rem(self.y + dy + self.side, self.side)

    def ref(self, unit, p, at):
        if unit % 2 == 0:
            return self.wvg.at[unit // 2, p, at]
        half = self.wo.shape[2] // 2
        return self.wo.at[unit // 2, at, pl.ds(p * half, half)]

    def push(self, unit, p, i, j, axis, d):
        ref = self.ref(unit, p, self.idx(p, i, j))
        di, dj = (d, 0) if axis == 0 else (0, d)
        slot = ((i - di) % 4) * 4 + (j - dj) % 4
        remote(
            ref, ref, self.gsend.at[2 * unit + p], self.grecv.at[2 * unit + p, slot], {"sp": self.idx(p, di, dj)}
        ).start()

    def arrive(self, unit, p, i, j):
        key = (unit, p, i % 4, j % 4)
        if key in self.waited or (i % 4, j % 4) == (0, 0):
            return
        self.waited.add(key)
        ref = self.ref(unit, p, self.idx(p, i, j))
        slot = (i % 4) * 4 + j % 4
        remote(
            ref, ref, self.gsend.at[2 * unit + p], self.grecv.at[2 * unit + p, slot], {"sp": self.idx(p, 1, 0)}
        ).wait_recv()

    def group(self, unit, p, i):
        for j in (0, -1, 1, 2):
            self.arrive(unit, p, i, j)

    def all(self, unit):
        for p in range(2):
            for i in (0, -1, 1, 2):
                self.group(unit, p, i)

    def opening(self, unit):
        for axis in range(2):
            for p in range(2):
                for d in (1, -1):
                    self.push(unit, p, 0, 0, axis, d)

    def events(self, unit):
        first = 1 if unit in (0, 3) else -1

        def turn(p, i, forward=None):
            def run():
                self.arrive(unit, p, i, 0)
                if forward:
                    self.push(unit, p, i, 0, 0, forward)
                for d in (1, -1):
                    self.push(unit, p, i, 0, 1, d)

            return run

        def relay(p, i):
            d = 1 if (i + unit) % 2 == 0 else -1

            def run():
                self.arrive(unit, p, i, -d)
                self.push(unit, p, i, -d, 1, d)

            return run

        both = range(2)
        steps = [turn(p, -first, first) for p in both] + [turn(p, first) for p in both]
        steps += [relay(p, 0) for p in both] + [turn(p, 2) for p in both]
        return steps + [relay(p, i) for i in (-1, 1, 2) for p in both]

    def drain(self, unit):
        for p in range(2):
            if unit % 2 == 0:
                ref = self.wvg.at[unit // 2, p, pl.ds(0, 15)]
            else:
                half = self.wo.shape[2] // 2
                ref = self.wo.at[unit // 2, pl.ds(0, 15), pl.ds(p * half, half)]
            remote(ref, ref, self.gsend.at[2 * unit + p], self.grecv.at[2 * unit + p, 0], {"sp": self.idx(p, 1, 0)}).wait_send()


def whole_kernel(
    layers, n_sp, n_tp, features,
    stream_hbm, gain_hbm, wv_hbm, wg_hbm, wo_hbm, taps_hbm, gates_hbm, rate_hbm, out_hbm,
    wvg, wo, xg, ssg, edge, near, tok, base, own, perm, acc, mixb, mpad, sil, conv, convb, big, a_f, u_f, a_b, u_b, col,
    seg, ent, msg, slots,
    psend, precv, fbuf, far_in, nbuf, near_in,
    stream_ref, gain_ref, taps_ref, gates_ref, rate_ref, ld, ins, outs, gsend, grecv, asend, arecv, ssend, srecv, hsend, hrecv, esend, erecv, csend, crecv, ds, dr, rs, rr,
):
    sp, tp = lax.axis_index("sp"), lax.axis_index("tp")
    tokens, width = mixb.shape
    feats = own.shape[1]
    joined = greet((("sp", n_sp, sp), ("tp", n_tp, tp)))
    ring = Ring(tp, n_tp)
    net = Weights(sp, 4, wvg, wo, gsend, grecv)
    pre = pown = big
    lanes_own = pl.ds(pl.multiple_of(tp * width, width), width)
    right, left = ring.at(1), ring.at(-1)

    inputs = [
        pltpu.make_async_copy(stream_hbm, stream_ref, ins.at[0]),
        pltpu.make_async_copy(gain_hbm, gain_ref, ins.at[1]),
        pltpu.make_async_copy(taps_hbm.at[:, :, lanes_own], taps_ref, ins.at[2]),
        pltpu.make_async_copy(gates_hbm, gates_ref, ins.at[3]),
        pltpu.make_async_copy(rate_hbm.at[:, :, lanes_own], rate_ref, ins.at[4]),
    ]
    for copy in inputs:
        copy.start()
    loads = []
    for layer in range(layers):
        loads.append([
            pltpu.make_async_copy(wv_hbm.at[layer], wvg.at[layer, 0, sp], ld.at[3 * layer]),
            pltpu.make_async_copy(wg_hbm.at[layer], wvg.at[layer, 1, sp], ld.at[3 * layer + 1]),
        ])
        loads.append([pltpu.make_async_copy(wo_hbm.at[layer], wo.at[layer, sp], ld.at[3 * layer + 2])])
    for copies in loads:
        for copy in copies:
            copy.start()
    def opening(unit):
        for copy in loads[unit]:
            copy.wait()
        net.opening(unit)

    waiting = [iter([functools.partial(opening, unit)] + net.events(unit)) for unit in range(2 * layers)]
    plan = iter(PLAN)

    def slot():
        for unit in next(plan):
            next(waiting[int(unit)])()

    def project(layer, p, i):
        if p == 0:
            spots = [net.idx(p, i, j) for j in range(4)]
            halves = [pl.ds(pl.multiple_of(lax.rem(at, 2) * 256, 256), 256) for at in spots]
            terms = [
                jnp.dot(xg[at // 2, :, lanes], wvg[layer, p, at], preferred_element_type=F32)
                for at, lanes in zip(spots, halves)
            ]
        else:
            first = lax.rem(net.z + i + net.side, net.side) * 2
            terms = [
                jnp.dot(
                    xg[first + j, 0:tokens, :],
                    wvg[layer, p, pl.ds(2 * (first + j), 2)].reshape(feats, width),
                    preferred_element_type=F32,
                )
                for j in range(2)
            ]
        total = functools.reduce(jnp.add, terms)
        acc[p, 0 : total.shape[0], :] += total

    def edge_send(layer, source):
        ends = (source[0:16, :].astype(F32), source[tokens - 16 : tokens, :].astype(F32))
        spots = ((0, 0), (1, 7), (1, 15))
        lines = [
            ends[side][row : row + 1, b * 128 : (b + 1) * 128] for side, row in spots for b in range(feats // 128)
        ]
        tok[layer] = jnp.concatenate(lines + [jnp.zeros((16 - len(lines), 128), F32)], axis=0).astype(BF16)
        for k in range(2):
            edge_copy(layer, k).start()

    def edge_copy(layer, k):
        place = lax.rem(sp + (1 if k == 0 else n_sp - 1), n_sp)
        return remote(tok.at[layer], near.at[layer, k], hsend.at[layer, k], hrecv.at[layer, k], {"sp": place})

    def edge_share(layer):
        for k in range(2):
            edge_copy(layer, k).wait()
        rows = lax.broadcasted_iota(jnp.int32, (16, 128), 0)
        after = jnp.where(sp < n_sp - 1, near[layer, 1].astype(F32), 0.0)
        before = jnp.where(sp > 0, near[layer, 0].astype(F32), 0.0)
        edge[layer, tp] = jnp.where(rows < 4, after, before).astype(BF16)
        for step in range(1, n_tp):
            dev = lax.rem(tp + step, n_tp)
            remote(
                edge.at[layer, tp], edge.at[layer, tp], esend.at[layer], erecv.at[layer], {"tp": dev}
            ).start()

    def edge_rows(layer):
        whole = edge.at[layer, pl.ds(0, n_tp - 1)]
        remote(whole, whole, esend.at[layer], erecv.at[layer], {"tp": ring.sib}).wait()
        squares = jnp.zeros((16, 128), F32)
        for block in range(n_tp):
            values = edge[layer, block].astype(F32)
            squares = squares + values * values
            lines = []
            for r in range(3):
                parts = [values[4 * r + b : 4 * r + b + 1, :] for b in range(feats // 128)]
                lines.append(jnp.concatenate(parts, axis=1))
            gain = gain_ref[layer : layer + 1, pl.ds(block * feats, feats)]
            rows = jnp.concatenate(lines, axis=0) * gain
            filled = jnp.concatenate([rows, jnp.zeros((EDGE - 3, feats), F32)], axis=0)
            xg[block, pl.ds(tokens, EDGE), :] = filled.astype(BF16)
        sums = jnp.sum(squares, axis=1, keepdims=True)
        return [
            lax.rsqrt(jnp.sum(sums[4 * r : 4 * r + 4, :], axis=0, keepdims=True) / features + NORM_EPS)
            for r in range(3)
        ]

    gathers = [
        Gather(ring, xg, ssg.at[layer], asend, arecv, ssend.at[layer], srecv.at[layer], n_tp)
        for layer in range(layers)
    ]

    def gather_own(layer, source, half=None):
        gain = gain_ref[layer : layer + 1, lanes_own]
        gather_fill(source, gain, xg, ssg.at[layer], tp, half)

    def column(layer):
        total = jnp.sum(ssg[layer], axis=0)
        scale = lax.rsqrt(total / features + NORM_EPS)
        for k in range(tokens // 128):
            part = jnp.broadcast_to(scale[0:1, k * 128 : (k + 1) * 128], (128, 128))
            col[pl.ds(k * 128, 128), :] = part.T

    def clear(rows):
        zero = jnp.zeros((rows.size, width), F32)
        acc[0, rows, :] = zero
        acc[1, rows, :] = zero

    def clear_all():
        in_row_steps(tokens, clear, 32)
        acc[0, pl.ds(tokens, EDGE), :] = jnp.zeros((EDGE, width), F32)

    def mix(layer, scales):
        def finish_v(rows):
            wide = jnp.concatenate([col[rows, :]] * (width // 128), axis=1)
            value = (acc[0, rows, :] * wide).astype(BF16)
            mixb[rows, :] = value
            acc[0, rows, :] = value.astype(F32)

        if not layer:
            for copy in inputs[2:]:
                copy.wait()

        def finish_g(rows):
            wide = jnp.concatenate([col[rows, :]] * (width // 128), axis=1)
            gate = (acc[1, rows, :] * wide).astype(BF16).astype(F32)
            sil[rows, :] = gate * sigmoid(gate)
            mpad[pl.ds(aligned(rows.start + 16, 16), rows.size), :] = acc[0, rows, :]

        in_row_steps(tokens, finish_v, 32)
        in_row_steps(tokens, finish_g, 32)
        slot()
        edges = [
            (acc[0, tokens + r : tokens + r + 1, :] * scales[r]).astype(BF16).astype(F32) for r in range(3)
        ]
        sub = lax.broadcasted_iota(jnp.int32, (SEG, width), 0)
        for k in range(2):
            blk = acc[0, pl.ds(tokens - 16 + 8 * k, 8), :]
            mpad[pl.ds(8 * k, 8), :] = jnp.where(
                sub == 0, jnp.broadcast_to(edges[1 + k], (SEG, width)), pltpu.roll(blk, 1, 0)
            )
        blk = acc[0, pl.ds(0, 8), :]
        mpad[pl.ds(tokens + 16, 8), :] = jnp.where(
            sub == SEG - 1, jnp.broadcast_to(edges[0], (SEG, width)), pltpu.roll(blk, SEG - 1, 0)
        )
        taps = taps_ref[layer]
        maps = [jnp.concatenate([gates_ref[layer, g, b] for g in range(4)], axis=1) for b in range(width // 128)]

        def gate_maps(rows):
            for b in range(width // 128):
                pre[b, rows, :] = jnp.dot(convb[rows, b * 128 : (b + 1) * 128], maps[b], preferred_element_type=F32)

        def convolve(rows):
            terms = [
                mpad[pl.ds(aligned(rows.start + 8 * k, 8), rows.size), :] * taps[k : k + 1, :]
                for k in range(4)
            ]
            value = (terms[0] + terms[1]) + (terms[2] + terms[3])
            conv[rows, :] = value
            convb[rows, :] = value.astype(BF16)

        in_row_steps(tokens, convolve, 32)
        slot()
        gate_maps(pl.ds(0, tokens))
        slot()
        rate_all = -GATE_SCALE * rate_ref[layer]
        for b in range(width // 128):
            lanes = pl.ds(b * 128, 128)
            rates = [rate_all[e : e + 1, b * 128 : (b + 1) * 128] for e in range(2)]

            def body(k, carry, b=b, lanes=lanes, rates=rates):
                p_f, h_f, p_b, h_b = carry
                rows = pl.ds(pl.multiple_of(k * ROWS, ROWS), ROWS)
                cv = conv[rows, lanes]
                kept = []
                for e, (a_ref, u_ref) in enumerate(((a_f, u_f), (a_b, u_b))):
                    r = sigmoid(pre[b, rows, 256 * e : 256 * e + 128])
                    i = sigmoid(pre[b, rows, 256 * e + 128 : 256 * e + 256])
                    log_a = rates[e] * r
                    decay = jnp.exp(log_a)
                    drive = jnp.sqrt(drive_square(-2.0 * log_a)) * i * cv
                    a_ref[rows, lanes] = decay
                    u_ref[rows, lanes] = drive
                    kept.append((decay, drive))
                for j in range(ROWS // 8):
                    at = slice(8 * j, 8 * j + 8)
                    d, u = kept[0][0][at], kept[0][1][at]
                    h_f = d * h_f + u
                    p_f = p_f * d
                    d, u = kept[1][0][at], kept[1][1][at]
                    h_b = h_b + p_b * u
                    p_b = p_b * d
                return p_f, h_f, p_b, h_b

            one, zero = jnp.ones((SEG, 128), F32), jnp.zeros((SEG, 128), F32)
            ends = lax.fori_loop(0, tokens // ROWS, body, (one, zero, one, zero))
            for k in range(4):
                seg[k, :, lanes] = ends[k]
            slot()

        sides = ((0, range(SEG)), (2, range(SEG - 1, -1, -1)))
        for e, (k, order) in enumerate(sides):
            prod = jnp.ones((1, width), F32)
            state = jnp.zeros((1, width), F32)
            for s in order:
                d = seg[k, s : s + 1, :]
                state = d * state + seg[k + 1, s : s + 1, :]
                prod = prod * d
            for b in range(width // 128):
                msg[layer, e, b : b + 1, :] = prod[:, b * 128 : (b + 1) * 128]
                msg[layer, e, 4 + b : 5 + b, :] = state[:, b * 128 : (b + 1) * 128]
        cs, cr = csend.at[layer], crecv.at[layer]
        for step in range(1, n_sp):
            dev = lax.rem(sp + step, n_sp)
            side = jnp.where(dev > sp, 0, 1)
            remote(msg.at[layer, side], slots.at[layer, sp], cs, cr, {"sp": dev}).start()
        slots[layer, sp] = jnp.zeros((8, 128), F32)
        slot()
        others = slots.at[layer, pl.ds(0, n_sp - 1)]
        remote(others, others, cs, cr, {"sp": lax.rem(sp + 1, n_sp)}).wait()
        for e, (k, order) in enumerate(sides):
            carry = jnp.zeros((4, 128), F32)
            for q in range(n_sp) if e == 0 else range(n_sp - 1, -1, -1):
                live = (q < sp) if e == 0 else (q > sp)
                entry = slots[layer, q]
                carry = jnp.where(live, entry[0:4] * carry + entry[4:8], carry)
            state = jnp.concatenate([carry[b : b + 1, :] for b in range(width // 128)], axis=1)
            for s in order:
                ent[e, s : s + 1, :] = state
                state = seg[k, s : s + 1, :] * state + seg[k + 1, s : s + 1, :]
        def again(k, carry):
            h_f, h_b = carry
            for j in range(4):
                fwd = pl.ds(pl.multiple_of((4 * k + j) * SEG, SEG), SEG)
                bwd = pl.ds(pl.multiple_of((steps - 1 - 4 * k - j) * SEG, SEG), SEG)
                h_f = a_f[fwd, :] * h_f + u_f[fwd, :]
                u_f[fwd, :] = h_f
                h_b = a_b[bwd, :] * h_b + u_b[bwd, :]
                u_b[bwd, :] = h_b
            return h_f, h_b

        lax.fori_loop(0, steps // 4, again, (ent[0], ent[1]))

        def gated(rows):
            mixb[rows, :] = ((u_f[rows, :] + u_b[rows, :]) * sil[rows, :]).astype(BF16)

        in_row_steps(tokens, gated, 32)
        slot()

    half = tokens // 2
    top, low = pl.ds(0, half), pl.ds(half, half)

    def result(rows):
        return pltpu.make_async_copy(base.at[rows], out_hbm.at[rows], outs.at[rows.start // half])

    def reduce(layer, source, target, chained):
        order = (2, 1, -1, 0)

        def product(k, other):
            block = ring.at(order[k], other=other)
            terms = [
                lax.dot_general(
                    mixb[...], wo[layer, 2 * block + part], (((1,), (1,)), ((), ())), preferred_element_type=F32
                )
                for part in range(2)
            ]
            return terms

        def across(k):
            return remote(psend.at[k], precv.at[k], ds.at[0], dr.at[k], {"tp": ring.sib})

        def send(k, src, dst, dev):
            remote(src, dst, rs.at[0], rr.at[k], {"tp": dev}).start()

        def paired(k, rows, into=None):
            def body(r):
                at = pl.ds(pl.multiple_of(rows.start + r.start, 32), r.size)
                value = pown[k, at, :] + precv[k, at, :].astype(F32)
                if into is None:
                    pown[k, at, :] = value
                else:
                    into[at if into.shape[0] == tokens else r, :] = value.astype(BF16)

            in_row_steps(rows.size, body, 32)

        for k in range(4):
            for part, term in enumerate(product(k, True)):
                psend[k, :, part * 256 : (part + 1) * 256] = term.astype(BF16)
            across(k).start()
            for part, term in enumerate(product(k, False)):
                pown[k, :, part * 256 : (part + 1) * 256] = term
            if k == 1:
                across(0).wait_recv()
                paired(0, top, fbuf)
                send(0, fbuf.at[top], far_in.at[0], right)
                paired(0, low, fbuf)
                send(1, fbuf.at[low], far_in.at[1], left)
            if k == 2:
                across(1).wait_recv()
                paired(1, low, nbuf.at[0])
                if not chained:
                    send(2, nbuf.at[0], near_in.at[0], right)
                paired(1, top)
            if k == 3:
                across(2).wait_recv()
                paired(2, top, nbuf.at[1])
                send(3, nbuf.at[1], near_in.at[1], left)
                paired(2, low)
            slot()
        across(3).wait_recv()
        paired(3, pl.ds(0, tokens))
        slot()

        def arrived(k, src, dst):
            remote(src, dst, rs.at[0], rr.at[k], {"tp": right}).wait_recv()

        def merged(k, rows, src, into):
            def body(r):
                at = pl.ds(pl.multiple_of(rows.start + r.start, 32), r.size)
                into[r, :] = (pown[k, at, :] + src[r, :].astype(F32)).astype(BF16)

            in_row_steps(half, body, 32)

        arrived(0, fbuf.at[top], far_in.at[0])
        merged(1, top, far_in.at[0], nbuf.at[2])
        send(4, nbuf.at[2], near_in.at[2], right)
        if chained:
            send(2, nbuf.at[0], near_in.at[0], right)
        arrived(1, fbuf.at[low], far_in.at[1])
        merged(2, low, far_in.at[1], nbuf.at[3])
        send(5, nbuf.at[3], near_in.at[3], left)
        slot()

        def total(rows, one, two):
            def body(r):
                at = pl.ds(pl.multiple_of(rows.start + r.start, 32), r.size)
                branch = pown[3, at, :] + near_in[one, r, :].astype(F32) + near_in[two, r, :].astype(F32)
                value = source[at, :].astype(F32) + branch
                target[at, :] = value.astype(BF16)

            in_row_steps(half, body, 32)

        if chained:
            gather = gathers[layer + 1]
            for k in (1, 2):
                arrived(2 + k, nbuf.at[k], near_in.at[k])
                if k == 1:
                    slot()
            total(top, 1, 2)
            gather_own(layer + 1, target, 0)
            gather.begin(0)
            slot()
            for k in (0, 3):
                arrived(2 + k, nbuf.at[k], near_in.at[k])
                if k == 0:
                    slot()
            total(low, 0, 3)
            gather_own(layer + 1, target, 1)
            gather.begin(1)
            gather.begin_squares()
            edge_send(layer + 1, target)
            clear_all()
            slot()
        else:
            for k in range(4):
                arrived(2 + k, nbuf.at[k], near_in.at[k])
                if k == 1:
                    slot()
            total(top, 1, 2)
            result(top).start()
            total(low, 0, 3)
            result(low).start()
        remote(psend, precv, ds.at[0], dr.at[0], {"tp": ring.sib}).wait_send()
        six = psend.at[pl.ds(0, 3)]
        remote(six, six, rs.at[0], rr.at[0], {"tp": right}).wait_send()

    steps = tokens // SEG

    def spread(rows):
        for b in range(feats // 128):
            perm[b, rows, :] = stream_ref[rows, b * 128 : (b + 1) * 128].astype(F32)

    def collect(rows):
        first = rows.start // SEG
        for b in range(feats // 128):
            parts = [perm[b, pl.ds(first + j, SEG, stride=steps), :] for j in range(rows.size // SEG)]
            base[rows, b * 128 : (b + 1) * 128] = jnp.concatenate(parts, axis=0).astype(BF16)

    inputs[0].wait()
    in_row_steps(tokens, spread)
    in_row_steps(tokens, collect, 32)
    inputs[1].wait()
    gather_own(0, base)
    joined()

    slot()
    gather = gathers[0]
    gather.begin(0)
    gather.begin(1)
    gather.begin_squares()
    edge_send(0, base)
    clear_all()
    slot()
    for pair in ((0, 2), (1, 3), (4, 5)):
        for k in pair:
            gather.got(k)
        if pair[0] == 0:
            edge_share(0)
        slot()
    gather.end()
    scales = edge_rows(0)
    column(0)
    slot()
    for layer in range(layers):
        unit = 2 * layer
        for i in (0, -1, 1, 2):
            for p in range(2):
                slot()
                net.group(unit, p, i)
                project(layer, p, i)
        mix(layer, scales)
        net.all(unit + 1)
        if layer + 1 < layers:
            reduce(layer, base, own, True)
            gather = gathers[layer + 1]
            for k in (0, 3, 2, 1, 4, 5):
                gather.got(k)
                if k == 2:
                    edge_share(layer + 1)
                slot()
            gather.end()
            scales = edge_rows(layer + 1)
            column(layer + 1)
            slot()
        else:
            reduce(layer, own, base, False)
            result(top).wait()
            result(low).wait()
    for unit in range(2 * layers):
        net.drain(unit)


def whole_call(stream, gain, wv, wg, wo, taps, gates, rate, n_sp, n_tp):
    tokens, feats = stream.shape
    layers, rows, width = wv.shape
    half = tokens // 2
    blocks = width // 128
    hbm = pl.BlockSpec(memory_space=pl.ANY)
    f32 = pltpu.VMEM((tokens, width), F32)
    b16 = pltpu.VMEM((tokens, width), BF16)
    dma = pltpu.SemaphoreType.DMA
    return pl.pallas_call(
        functools.partial(whole_kernel, layers, n_sp, n_tp, float(gain.shape[1])),
        out_shape=jax.ShapeDtypeStruct((tokens, feats), BF16),
        in_specs=[hbm] * 8,
        out_specs=hbm,
        scratch_shapes=[
            pltpu.VMEM((layers, 2, n_sp, rows, width), BF16),
            pltpu.VMEM((layers, n_sp, rows, width), BF16),
            pltpu.VMEM((n_tp, tokens + EDGE, feats), BF16),
            pltpu.VMEM((layers, n_tp, 8, tokens), F32),
            pltpu.VMEM((layers, n_tp, 16, 128), BF16),
            pltpu.VMEM((layers, 2, 16, 128), BF16),
            pltpu.VMEM((layers, 16, 128), BF16),
            b16, b16,
            pltpu.VMEM((feats // 128, tokens, 128), F32),
            pltpu.VMEM((2, tokens + EDGE, width), F32),
            b16,
            pltpu.VMEM((tokens + 24, width), F32),
            f32, f32, b16,
            pltpu.VMEM((4, tokens, 512), F32),
            f32, f32, f32, f32,
            pltpu.VMEM((tokens, 128), F32),
            pltpu.VMEM((4, SEG, width), F32),
            pltpu.VMEM((2, SEG, width), F32),
            pltpu.VMEM((layers, 2, 8, 128), F32),
            pltpu.VMEM((layers, n_sp, 8, 128), F32),
            pltpu.VMEM((4, tokens, feats), BF16),
            pltpu.VMEM((4, tokens, feats), BF16),
            pltpu.VMEM((tokens, feats), BF16),
            pltpu.VMEM((2, half, feats), BF16),
            pltpu.VMEM((4, half, feats), BF16),
            pltpu.VMEM((4, half, feats), BF16),
            b16,
            pltpu.VMEM(gain.shape, F32),
            pltpu.VMEM((layers, 4, width), F32),
            pltpu.VMEM(gates.shape, BF16),
            pltpu.VMEM((layers, 2, width), F32),
            dma((3 * layers,)),
            dma((5,)),
            dma((2,)),
            dma((4 * layers,)),
            dma((4 * layers, 16)),
            dma((1,)),
            dma((7,)),
            dma((layers,)),
            dma((layers,)),
            dma((layers, 2)),
            dma((layers, 2)),
            dma((layers,)),
            dma((layers,)),
            dma((layers,)),
            dma((layers,)),
            dma((1,)),
            dma((4,)),
            dma((1,)),
            dma((6,)),
        ],
        compiler_params=pltpu.CompilerParams(
            collective_id=0, has_side_effects=True, vmem_limit_bytes=63_000_000
        ),
        cost_estimate=pl.CostEstimate(flops=20_000_000_000, bytes_accessed=8_000_000, transcendentals=0),
        name="both_layers",
    )(stream, gain, wv, wg, wo, taps, gates, rate)


def per_device(
    n_sp, n_tp, stream_in, norm_gain, value_proj, gate_proj, out_proj, conv_taps, block_gates, forget_rate
):
    width = value_proj.shape[2]
    layers = value_proj.shape[0]
    gates = block_gates.reshape(layers, 4, width // 128, 128, 128)
    stream = whole_call(
        stream_in, norm_gain, value_proj, gate_proj, out_proj, conv_taps, gates, forget_rate, n_sp, n_tp
    )
    tokens, feats = stream.shape
    return stream.reshape(tokens // SEG, SEG, feats).transpose(1, 0, 2).reshape(tokens, feats)


def solution(mesh):
    placed = (
        P("sp", "tp"),
        P(),
        P(None, "sp", "tp"),
        P(None, "sp", "tp"),
        P(None, "sp", "tp"),
        P(),
        P(None, None, None, "tp", None),
        P(),
    )
    body = functools.partial(per_device, mesh.shape["sp"], mesh.shape["tp"])
    return jax.shard_map(body, mesh=mesh, in_specs=placed, out_specs=P("sp", "tp"), check_vma=False)
```

```python
import functools

import jax
import jax.numpy as jnp
from jax import lax
from jax.experimental import pallas as pl
from jax.experimental.pallas import tpu as pltpu
from jax.sharding import PartitionSpec as P

GATE_SCALE = 8.0
NORM_EPS = 1e-06
MESH = pl.DeviceIdType.MESH
F32 = jnp.float32
BF16 = jnp.bfloat16
EDGE = 16
SEG = 8
ROWS = 64
PLAN = ('0', '00', '00', '00', '01', '00', '00', '001', '1011', '1', '1', '', '1', '1', '', '', '', '', '11', '', '', '11112', '', '', '2', '2', '2', '2', '22', '', '2', '2', '222', '2', '3', '22', '', '3', '3', '', '', '', '', '', '33', '', '', '', '333', '3', '', '', '3', '', '', '33', '', '33', '3', '', '', '', '')


def remote(src, dst, send_sem, recv_sem, dev):
    return pltpu.make_async_remote_copy(
        src_ref=src, dst_ref=dst, send_sem=send_sem, recv_sem=recv_sem, device_id=dev, device_id_type=MESH
    )


def greet(groups):
    barrier = pltpu.get_barrier_semaphore()
    for axis, count, me in groups:
        for step in range(1, count):
            pl.semaphore_signal(barrier, inc=1, device_id={axis: lax.rem(me + step, count)}, device_id_type=MESH)
    return lambda: pl.semaphore_wait(barrier, sum(count - 1 for _, count, _ in groups))


def sigmoid(v):
    return 1.0 / (1.0 + jnp.exp(-v))


def drive_square(y):
    terms = [0.999999999543, -0.499999943611, 0.166665528456, -0.0416580188735, 0.00830184073719, -0.00132924407794, 0.000140574729006]
    total = jnp.full_like(y, terms[-1])
    for term in terms[-2::-1]:
        total = total * y + term
    return total * y


def in_row_steps(rows, body, size=ROWS, first=0):
    def step(k, carry):
        body(pl.ds(pl.multiple_of(first + k * size, size), size))
        return carry

    lax.fori_loop(0, rows // size, step, 0)


def aligned(at, size):
    return at if isinstance(at, int) else pl.multiple_of(at, size)


class Ring:
    def __init__(self, me, count):
        chips = count // 2
        self.chips = chips
        self.me = me
        self.x = me // 2
        self.c = lax.rem(me, 2)
        self.sib = self.x * 2 + 1 - self.c

    def at(self, step, other=False):
        core = 1 - self.c if other else self.c
        return lax.rem(self.x + step + self.chips, self.chips) * 2 + core


def gather_fill(own_ref, gain, xg, ssg, me, half=None):
    tokens = own_ref.shape[0]
    first, count = (0, tokens) if half is None else (half * tokens // 2, tokens // 2)

    def fill(rows):
        at = pl.ds(pl.multiple_of(first + rows.start, ROWS), rows.size)
        v = own_ref[at, :].astype(F32)
        xg[me, at, :] = (v * gain).astype(BF16)

    in_row_steps(count, fill)
    for k in range(first // 128, (first + count) // 128):
        v = own_ref[pl.ds(k * 128, 128), :].astype(F32)
        total = jnp.sum(v * v, axis=1, keepdims=True)
        ssg[me, :, pl.ds(k * 128, 128)] = jnp.broadcast_to(total, (128, 128)).T[0:8, :]


class Gather:
    def __init__(self, ring, xg, ssg, send, recv, ssend, srecv, count):
        self.ring, self.xg, self.ssg, self.count = ring, xg, ssg, count
        self.send, self.recv, self.ssend, self.srecv = send, recv, ssend, srecv
        half = (xg.shape[1] - EDGE) // 2
        self.rows = (pl.ds(0, half), pl.ds(half, half))

    def push(self, part, k, dev):
        remote(part, part, self.send.at[0], self.recv.at[min(k, 6)], {"tp": dev}).start()

    def begin(self, half):
        ring = self.ring
        part = self.xg.at[ring.me, self.rows[half]]
        right, left = ring.at(1), ring.at(-1)
        if half == 0:
            self.push(part, 0, right)
            self.push(part, 3, left)
            self.push(part, 6, ring.sib)
        else:
            self.push(part, 2, left)
            self.push(part, 1, right)
            self.push(part, 13, ring.sib)

    def begin_squares(self):
        ring, ssg = self.ring, self.ssg
        for step in range(1, self.count):
            dev = lax.rem(ring.me + step, self.count)
            remote(ssg.at[ring.me], ssg.at[ring.me], self.ssend, self.srecv, {"tp": dev}).start()

    def got(self, k):
        ring = self.ring
        step, half = {0: (-1, 0), 1: (-1, 1), 2: (1, 1), 3: (1, 0), 4: (2, 0), 5: (2, 1)}[k]
        part = self.xg.at[ring.at(step), self.rows[half]]
        remote(part, part, self.send.at[0], self.recv.at[k], {"tp": ring.sib}).wait_recv()
        if k == 0:
            self.push(part, 4, ring.at(1))
        if k == 2:
            self.push(part, 5, ring.at(-1))
        self.push(part, 7 + k, ring.sib)

    def end(self):
        count, dev = self.count, {"tp": self.ring.sib}
        half = self.rows[0].size
        came = self.xg.at[:, pl.ds(0, half)]
        remote(came, came, self.send.at[0], self.recv.at[6], dev).wait_recv()
        sent = self.xg.at[pl.ds(0, count - 1), pl.ds(0, 2 * half)]
        remote(sent, sent, self.send.at[0], self.recv.at[6], dev).wait_send()
        others = self.ssg.at[pl.ds(0, count - 1)]
        remote(others, others, self.ssend, self.srecv, dev).wait()


class Weights:
    def __init__(self, me, side, wvg, wo, gsend, grecv):
        self.y, self.z, self.side = lax.rem(me, side), me // side, side
        self.wvg, self.wo, self.gsend, self.grecv = wvg, wo, gsend, grecv
        self.waited = set()

    def idx(self, p, i, j):
        dy, dz = (i, j) if p == 0 else (j, i)
        return lax.rem(self.z + dz + self.side, self.side) * self.side + lax.rem(self.y + dy + self.side, self.side)

    def ref(self, unit, p, at):
        if unit % 2 == 0:
            return self.wvg.at[unit // 2, p, at]
        half = self.wo.shape[2] // 2
        return self.wo.at[unit // 2, at, pl.ds(p * half, half)]

    def push(self, unit, p, i, j, axis, d):
        ref = self.ref(unit, p, self.idx(p, i, j))
        di, dj = (d, 0) if axis == 0 else (0, d)
        slot = ((i - di) % 4) * 4 + (j - dj) % 4
        remote(
            ref, ref, self.gsend.at[2 * unit + p], self.grecv.at[2 * unit + p, slot], {"sp": self.idx(p, di, dj)}
        ).start()

    def arrive(self, unit, p, i, j):
        key = (unit, p, i % 4, j % 4)
        if key in self.waited or (i % 4, j % 4) == (0, 0):
            return
        self.waited.add(key)
        ref = self.ref(unit, p, self.idx(p, i, j))
        slot = (i % 4) * 4 + j % 4
        remote(
            ref, ref, self.gsend.at[2 * unit + p], self.grecv.at[2 * unit + p, slot], {"sp": self.idx(p, 1, 0)}
        ).wait_recv()

    def group(self, unit, p, i):
        for j in (0, -1, 1, 2):
            self.arrive(unit, p, i, j)

    def all(self, unit):
        for p in range(2):
            for i in (0, -1, 1, 2):
                self.group(unit, p, i)

    def opening(self, unit):
        for axis in range(2):
            for p in range(2):
                for d in (1, -1):
                    self.push(unit, p, 0, 0, axis, d)

    def events(self, unit):
        first = 1 if unit in (0, 3) else -1

        def turn(p, i, forward=None):
            def run():
                self.arrive(unit, p, i, 0)
                if forward:
                    self.push(unit, p, i, 0, 0, forward)
                for d in (1, -1):
                    self.push(unit, p, i, 0, 1, d)

            return run

        def relay(p, i):
            d = 1 if (i + unit) % 2 == 0 else -1

            def run():
                self.arrive(unit, p, i, -d)
                self.push(unit, p, i, -d, 1, d)

            return run

        both = range(2)
        steps = [turn(p, -first, first) for p in both] + [turn(p, first) for p in both]
        steps += [relay(p, 0) for p in both] + [turn(p, 2) for p in both]
        return steps + [relay(p, i) for i in (-1, 1, 2) for p in both]

    def drain(self, unit):
        for p in range(2):
            if unit % 2 == 0:
                ref = self.wvg.at[unit // 2, p, pl.ds(0, 15)]
            else:
                half = self.wo.shape[2] // 2
                ref = self.wo.at[unit // 2, pl.ds(0, 15), pl.ds(p * half, half)]
            remote(ref, ref, self.gsend.at[2 * unit + p], self.grecv.at[2 * unit + p, 0], {"sp": self.idx(p, 1, 0)}).wait_send()


def whole_kernel(
    layers, n_sp, n_tp, features,
    stream_hbm, gain_hbm, wv_hbm, wg_hbm, wo_hbm, taps_hbm, gates_hbm, rate_hbm, out_hbm,
    wvg, wo, xg, ssg, edge, near, tok, base, own, perm, acc, mixb, mpad, sil, conv, convb, big, a_f, u_f, a_b, u_b, col,
    seg, ent, msg, slots,
    psend, precv, fbuf, far_in, nbuf, near_in,
    stream_ref, gain_ref, taps_ref, gates_ref, rate_ref, ld, ins, outs, gsend, grecv, asend, arecv, ssend, srecv, hsend, hrecv, esend, erecv, csend, crecv, ds, dr, rs, rr,
):
    sp, tp = lax.axis_index("sp"), lax.axis_index("tp")
    tokens, width = mixb.shape
    feats = own.shape[1]
    joined = greet((("sp", n_sp, sp), ("tp", n_tp, tp)))
    ring = Ring(tp, n_tp)
    net = Weights(sp, 4, wvg, wo, gsend, grecv)
    pre = pown = big
    lanes_own = pl.ds(pl.multiple_of(tp * width, width), width)
    right, left = ring.at(1), ring.at(-1)

    inputs = [
        pltpu.make_async_copy(stream_hbm, stream_ref, ins.at[0]),
        pltpu.make_async_copy(gain_hbm, gain_ref, ins.at[1]),
        pltpu.make_async_copy(taps_hbm.at[:, :, lanes_own], taps_ref, ins.at[2]),
        pltpu.make_async_copy(gates_hbm, gates_ref, ins.at[3]),
        pltpu.make_async_copy(rate_hbm.at[:, :, lanes_own], rate_ref, ins.at[4]),
    ]
    for copy in inputs:
        copy.start()
    loads = []
    for layer in range(layers):
        loads.append([
            pltpu.make_async_copy(wv_hbm.at[layer], wvg.at[layer, 0, sp], ld.at[3 * layer]),
            pltpu.make_async_copy(wg_hbm.at[layer], wvg.at[layer, 1, sp], ld.at[3 * layer + 1]),
        ])
        loads.append([pltpu.make_async_copy(wo_hbm.at[layer], wo.at[layer, sp], ld.at[3 * layer + 2])])
    for copies in loads:
        for copy in copies:
            copy.start()
    def opening(unit):
        for copy in loads[unit]:
            copy.wait()
        net.opening(unit)

    waiting = [iter([functools.partial(opening, unit)] + net.events(unit)) for unit in range(2 * layers)]
    plan = iter(PLAN)

    def slot():
        for unit in next(plan):
            next(waiting[int(unit)])()

    def project(layer, p, i):
        if p == 0:
            spots = [net.idx(p, i, j) for j in range(4)]
            halves = [pl.ds(pl.multiple_of(lax.rem(at, 2) * 256, 256), 256) for at in spots]
            terms = [
                jnp.dot(xg[at // 2, :, lanes], wvg[layer, p, at], preferred_element_type=F32)
                for at, lanes in zip(spots, halves)
            ]
        else:
            first = lax.rem(net.z + i + net.side, net.side) * 2
            terms = [
                jnp.dot(
                    xg[first + j, 0:tokens, :],
                    wvg[layer, p, pl.ds(2 * (first + j), 2)].reshape(feats, width),
                    preferred_element_type=F32,
                )
                for j in range(2)
            ]
        total = functools.reduce(jnp.add, terms)
        acc[p, 0 : total.shape[0], :] += total

    def edge_send(layer, source):
        ends = (source[0:16, :].astype(F32), source[tokens - 16 : tokens, :].astype(F32))
        spots = ((0, 0), (1, 7), (1, 15))
        lines = [
            ends[side][row : row + 1, b * 128 : (b + 1) * 128] for side, row in spots for b in range(feats // 128)
        ]
        tok[layer] = jnp.concatenate(lines + [jnp.zeros((16 - len(lines), 128), F32)], axis=0).astype(BF16)
        for k in range(2):
            edge_copy(layer, k).start()

    def edge_copy(layer, k):
        place = lax.rem(sp + (1 if k == 0 else n_sp - 1), n_sp)
        return remote(tok.at[layer], near.at[layer, k], hsend.at[layer, k], hrecv.at[layer, k], {"sp": place})

    def edge_share(layer):
        for k in range(2):
            edge_copy(layer, k).wait()
        rows = lax.broadcasted_iota(jnp.int32, (16, 128), 0)
        after = jnp.where(sp < n_sp - 1, near[layer, 1].astype(F32), 0.0)
        before = jnp.where(sp > 0, near[layer, 0].astype(F32), 0.0)
        edge[layer, tp] = jnp.where(rows < 4, after, before).astype(BF16)
        for step in range(1, n_tp):
            dev = lax.rem(tp + step, n_tp)
            remote(
                edge.at[layer, tp], edge.at[layer, tp], esend.at[layer], erecv.at[layer], {"tp": dev}
            ).start()

    def edge_rows(layer):
        whole = edge.at[layer, pl.ds(0, n_tp - 1)]
        remote(whole, whole, esend.at[layer], erecv.at[layer], {"tp": ring.sib}).wait()
        squares = jnp.zeros((16, 128), F32)
        for block in range(n_tp):
            values = edge[layer, block].astype(F32)
            squares = squares + values * values
            lines = []
            for r in range(3):
                parts = [values[4 * r + b : 4 * r + b + 1, :] for b in range(feats // 128)]
                lines.append(jnp.concatenate(parts, axis=1))
            gain = gain_ref[layer : layer + 1, pl.ds(block * feats, feats)]
            rows = jnp.concatenate(lines, axis=0) * gain
            filled = jnp.concatenate([rows, jnp.zeros((EDGE - 3, feats), F32)], axis=0)
            xg[block, pl.ds(tokens, EDGE), :] = filled.astype(BF16)
        sums = jnp.sum(squares, axis=1, keepdims=True)
        return [
            lax.rsqrt(jnp.sum(sums[4 * r : 4 * r + 4, :], axis=0, keepdims=True) / features + NORM_EPS)
            for r in range(3)
        ]

    gathers = [
        Gather(ring, xg, ssg.at[layer], asend, arecv, ssend.at[layer], srecv.at[layer], n_tp)
        for layer in range(layers)
    ]

    def gather_own(layer, source, half=None):
        gain = gain_ref[layer : layer + 1, lanes_own]
        gather_fill(source, gain, xg, ssg.at[layer], tp, half)

    def column(layer):
        total = jnp.sum(ssg[layer], axis=0)
        scale = lax.rsqrt(total / features + NORM_EPS)
        for k in range(tokens // 128):
            part = jnp.broadcast_to(scale[0:1, k * 128 : (k + 1) * 128], (128, 128))
            col[pl.ds(k * 128, 128), :] = part.T

    def clear(rows):
        zero = jnp.zeros((rows.size, width), F32)
        acc[0, rows, :] = zero
        acc[1, rows, :] = zero

    def clear_all():
        in_row_steps(tokens, clear, 32)
        acc[0, pl.ds(tokens, EDGE), :] = jnp.zeros((EDGE, width), F32)

    def mix(layer, scales):
        def finish_v(rows):
            wide = jnp.concatenate([col[rows, :]] * (width // 128), axis=1)
            value = (acc[0, rows, :] * wide).astype(BF16)
            mixb[rows, :] = value
            acc[0, rows, :] = value.astype(F32)

        if not layer:
            for copy in inputs[2:]:
                copy.wait()

        def finish_g(rows):
            wide = jnp.concatenate([col[rows, :]] * (width // 128), axis=1)
            gate = (acc[1, rows, :] * wide).astype(BF16).astype(F32)
            sil[rows, :] = gate * sigmoid(gate)
            mpad[pl.ds(aligned(rows.start + 16, 16), rows.size), :] = acc[0, rows, :]

        in_row_steps(tokens, finish_v, 32)
        in_row_steps(tokens, finish_g, 32)
        slot()
        edges = [
            (acc[0, tokens + r : tokens + r + 1, :] * scales[r]).astype(BF16).astype(F32) for r in range(3)
        ]
        sub = lax.broadcasted_iota(jnp.int32, (SEG, width), 0)
        for k in range(2):
            blk = acc[0, pl.ds(tokens - 16 + 8 * k, 8), :]
            mpad[pl.ds(8 * k, 8), :] = jnp.where(
                sub == 0, jnp.broadcast_to(edges[1 + k], (SEG, width)), pltpu.roll(blk, 1, 0)
            )
        blk = acc[0, pl.ds(0, 8), :]
        mpad[pl.ds(tokens + 16, 8), :] = jnp.where(
            sub == SEG - 1, jnp.broadcast_to(edges[0], (SEG, width)), pltpu.roll(blk, SEG - 1, 0)
        )
        taps = taps_ref[layer]
        maps = [jnp.concatenate([gates_ref[layer, g, b] for g in range(4)], axis=1) for b in range(width // 128)]

        def gate_maps(rows):
            for b in range(width // 128):
                pre[b, rows, :] = jnp.dot(convb[rows, b * 128 : (b + 1) * 128], maps[b], preferred_element_type=F32)

        def convolve(rows):
            terms = [
                mpad[pl.ds(aligned(rows.start + 8 * k, 8), rows.size), :] * taps[k : k + 1, :]
                for k in range(4)
            ]
            value = (terms[0] + terms[1]) + (terms[2] + terms[3])
            conv[rows, :] = value
            convb[rows, :] = value.astype(BF16)

        in_row_steps(tokens, convolve, 32)
        slot()
        gate_maps(pl.ds(0, tokens))
        slot()
        rate_all = -GATE_SCALE * rate_ref[layer]
        for b in range(width // 128):
            lanes = pl.ds(b * 128, 128)
            rates = [rate_all[e : e + 1, b * 128 : (b + 1) * 128] for e in range(2)]

            def body(k, carry, b=b, lanes=lanes, rates=rates):
                p_f, h_f, p_b, h_b = carry
                rows = pl.ds(pl.multiple_of(k * ROWS, ROWS), ROWS)
                cv = conv[rows, lanes]
                kept = []
                for e, (a_ref, u_ref) in enumerate(((a_f, u_f), (a_b, u_b))):
                    r = sigmoid(pre[b, rows, 256 * e : 256 * e + 128])
                    i = sigmoid(pre[b, rows, 256 * e + 128 : 256 * e + 256])
                    log_a = rates[e] * r
                    decay = jnp.exp(log_a)
                    drive = jnp.sqrt(drive_square(-2.0 * log_a)) * i * cv
                    a_ref[rows, lanes] = decay
                    u_ref[rows, lanes] = drive
                    kept.append((decay, drive))
                for j in range(ROWS // 8):
                    at = slice(8 * j, 8 * j + 8)
                    d, u = kept[0][0][at], kept[0][1][at]
                    h_f = d * h_f + u
                    p_f = p_f * d
                    d, u = kept[1][0][at], kept[1][1][at]
                    h_b = h_b + p_b * u
                    p_b = p_b * d
                return p_f, h_f, p_b, h_b

            one, zero = jnp.ones((SEG, 128), F32), jnp.zeros((SEG, 128), F32)
            ends = lax.fori_loop(0, tokens // ROWS, body, (one, zero, one, zero))
            for k in range(4):
                seg[k, :, lanes] = ends[k]
            slot()

        sides = ((0, range(SEG)), (2, range(SEG - 1, -1, -1)))
        for e, (k, order) in enumerate(sides):
            prod = jnp.ones((1, width), F32)
            state = jnp.zeros((1, width), F32)
            for s in order:
                d = seg[k, s : s + 1, :]
                state = d * state + seg[k + 1, s : s + 1, :]
                prod = prod * d
            for b in range(width // 128):
                msg[layer, e, b : b + 1, :] = prod[:, b * 128 : (b + 1) * 128]
                msg[layer, e, 4 + b : 5 + b, :] = state[:, b * 128 : (b + 1) * 128]
        cs, cr = csend.at[layer], crecv.at[layer]
        for step in range(1, n_sp):
            dev = lax.rem(sp + step, n_sp)
            side = jnp.where(dev > sp, 0, 1)
            remote(msg.at[layer, side], slots.at[layer, sp], cs, cr, {"sp": dev}).start()
        slots[layer, sp] = jnp.zeros((8, 128), F32)
        slot()
        others = slots.at[layer, pl.ds(0, n_sp - 1)]
        remote(others, others, cs, cr, {"sp": lax.rem(sp + 1, n_sp)}).wait()
        for e, (k, order) in enumerate(sides):
            carry = jnp.zeros((4, 128), F32)
            for q in range(n_sp) if e == 0 else range(n_sp - 1, -1, -1):
                live = (q < sp) if e == 0 else (q > sp)
                entry = slots[layer, q]
                carry = jnp.where(live, entry[0:4] * carry + entry[4:8], carry)
            state = jnp.concatenate([carry[b : b + 1, :] for b in range(width // 128)], axis=1)
            for s in order:
                ent[e, s : s + 1, :] = state
                state = seg[k, s : s + 1, :] * state + seg[k + 1, s : s + 1, :]
        def again(k, carry):
            h_f, h_b = carry
            for j in range(4):
                fwd = pl.ds(pl.multiple_of((4 * k + j) * SEG, SEG), SEG)
                bwd = pl.ds(pl.multiple_of((steps - 1 - 4 * k - j) * SEG, SEG), SEG)
                h_f = a_f[fwd, :] * h_f + u_f[fwd, :]
                u_f[fwd, :] = h_f
                h_b = a_b[bwd, :] * h_b + u_b[bwd, :]
                u_b[bwd, :] = h_b
            return h_f, h_b

        lax.fori_loop(0, steps // 4, again, (ent[0], ent[1]))

        def gated(rows):
            mixb[rows, :] = ((u_f[rows, :] + u_b[rows, :]) * sil[rows, :]).astype(BF16)

        in_row_steps(tokens, gated, 32)
        slot()

    half = tokens // 2
    top, low = pl.ds(0, half), pl.ds(half, half)

    def result(rows):
        return pltpu.make_async_copy(base.at[rows], out_hbm.at[rows], outs.at[rows.start // half])

    class Reduce:
        order = (2, 1, -1, 0)

        def __init__(self, layer, first, count, shard):
            self.layer, self.first, self.parts, self.shard = layer, first, range(first, first + count), shard
            self.sel = pl.ds(first, count)

        def product(self, k, other, part):
            return lax.dot_general(
                mixb[...],
                wo[self.layer, self.shard(self.order[k], other, part)],
                (((1,), (1,)), ((), ())),
                preferred_element_type=F32,
            )

        def across(self, k):
            return remote(
                psend.at[k, self.sel], precv.at[k, self.sel], ds.at[0], dr.at[k, self.first], {"tp": ring.sib}
            )

        def send(self, k, src, dst, dev):
            remote(src, dst, rs.at[0], rr.at[k, self.first], {"tp": dev}).start()

        def arrived(self, k, dst):
            remote(dst, dst, rs.at[0], rr.at[k, self.first], {"tp": right}).wait_recv()

        def paired(self, k, rows, into=None):
            def body(r):
                at = pl.ds(pl.multiple_of(rows.start + r.start, 32), r.size)
                for part in self.parts:
                    lanes = pl.ds(part * 256, 256)
                    value = pown[k, at, lanes] + precv[k, part, at, :].astype(F32)
                    if into is None:
                        pown[k, at, lanes] = value
                    elif into is fbuf:
                        fbuf[part, at, :] = value.astype(BF16)
                    else:
                        nbuf[into, part, r, :] = value.astype(BF16)

            in_row_steps(rows.size, body, 32)

        def near(self, k, dev):
            self.send(2 + k, nbuf.at[k, self.sel], near_in.at[k, self.sel], dev)

        def opening(self, chained):
            for k in range(4):
                for part in self.parts:
                    psend[k, part] = self.product(k, True, part).astype(BF16)
                self.across(k).start()
                for part in self.parts:
                    pown[k, :, part * 256 : (part + 1) * 256] = self.product(k, False, part)
                if k == 1:
                    self.across(0).wait_recv()
                    self.paired(0, top, fbuf)
                    self.send(0, fbuf.at[self.sel, top], far_in.at[0, self.sel], right)
                    self.paired(0, low, fbuf)
                    self.send(1, fbuf.at[self.sel, low], far_in.at[1, self.sel], left)
                if k == 2:
                    self.across(1).wait_recv()
                    self.paired(1, low, 0)
                    if not chained:
                        self.near(0, right)
                    self.paired(1, top)
                if k == 3:
                    self.across(2).wait_recv()
                    self.paired(2, top, 1)
                    self.near(1, left)
                    self.paired(2, low)
                if chained or not self.first:
                    slot()
            self.across(3).wait_recv()
            self.paired(3, pl.ds(0, tokens))

        def merge(self, k, rows, side):
            self.arrived(side, far_in.at[side, self.sel])

            def body(r):
                at = pl.ds(pl.multiple_of(rows.start + r.start, 32), r.size)
                for part in self.parts:
                    value = pown[k, at, pl.ds(part * 256, 256)] + far_in[side, part, r, :].astype(F32)
                    nbuf[2 + side, part, r, :] = value.astype(BF16)

            in_row_steps(half, body, 32)
            self.near(2 + side, left if side else right)

        def merges(self, chained):
            self.merge(1, top, 0)
            if chained:
                self.near(0, right)
            self.merge(2, low, 1)

        def got(self, k):
            self.arrived(2 + k, near_in.at[k, self.sel])

        def total(self, rows, one, two, source, target, column=None):
            def body(r):
                at = pl.ds(pl.multiple_of(rows.start + r.start, 32), r.size)
                for part in self.parts:
                    lanes = pl.ds(part * 256, 256)
                    branch = pown[3, at, lanes] + near_in[one, part, r, :].astype(F32)
                    branch = branch + near_in[two, part, r, :].astype(F32)
                    spot = lanes if column is None else column
                    target[at, spot] = (source[at, spot].astype(F32) + branch).astype(BF16)

            in_row_steps(half, body, 32)

    def reduce_done():
        remote(psend, precv, ds.at[0], dr.at[0, 0], {"tp": ring.sib}).wait_send()
        six = psend.at[pl.ds(0, 3)]
        remote(six, six, rs.at[0], rr.at[0, 0], {"tp": right}).wait_send()

    def reduce_chained(layer, source, target):
        work = Reduce(layer, 0, 2, lambda step, other, part: 2 * ring.at(step, other=other) + part)
        work.opening(True)
        slot()
        work.merges(True)
        slot()
        gather = gathers[layer + 1]
        work.got(1)
        slot()
        work.got(2)
        work.total(top, 1, 2, source, target)
        gather_own(layer + 1, target, 0)
        gather.begin(0)
        slot()
        work.got(0)
        slot()
        work.got(3)
        work.total(low, 0, 3, source, target)
        gather_own(layer + 1, target, 1)
        gather.begin(1)
        gather.begin_squares()
        edge_send(layer + 1, target)
        clear_all()
        slot()
        reduce_done()

    def reduce_last(layer, source, target):
        unit = 2 * layer + 1

        def stage(first, near_y, far_y):
            ya, yb = (lax.rem(net.y + d + net.side, net.side) for d in (near_y, far_y))
            mine = jnp.where(ya // 2 == ring.c, ya, yb)
            theirs = jnp.where(ya // 2 == ring.c, yb, ya)

            def shard(step, other, part):
                z = lax.rem(ring.x + step + ring.chips, ring.chips)
                return z * net.side + (theirs if other else mine)

            column = pl.ds(pl.multiple_of(lax.rem(mine, 2) * 256, 256), 256)
            return Reduce(layer, first, 1, shard), column

        one, one_column = stage(0, 1, -1)
        two, two_column = stage(1, 0, 2)
        for i in (-1, 1):
            net.group(unit, 0, i)
        for i in (0, -1, 1, 2):
            for j in (-1, 1):
                net.arrive(unit, 1, i, j)
        one.opening(False)
        slot()
        one.merges(False)
        slot()
        net.all(unit)
        two.opening(False)
        for k in range(4):
            one.got(k)
        one.total(top, 1, 2, source, target, one_column)
        one.total(low, 0, 3, source, target, one_column)
        two.merges(False)
        for k in range(4):
            two.got(k)
        two.total(top, 1, 2, source, target, two_column)
        result(top).start()
        two.total(low, 0, 3, source, target, two_column)
        result(low).start()
        reduce_done()

    steps = tokens // SEG

    def spread(rows):
        for b in range(feats // 128):
            perm[b, rows, :] = stream_ref[rows, b * 128 : (b + 1) * 128].astype(F32)

    def collect(rows):
        first = rows.start // SEG
        for b in range(feats // 128):
            parts = [perm[b, pl.ds(first + j, SEG, stride=steps), :] for j in range(rows.size // SEG)]
            base[rows, b * 128 : (b + 1) * 128] = jnp.concatenate(parts, axis=0).astype(BF16)

    inputs[0].wait()
    in_row_steps(tokens, spread)
    in_row_steps(tokens, collect, 32)
    inputs[1].wait()
    gather_own(0, base)
    joined()

    slot()
    gather = gathers[0]
    gather.begin(0)
    gather.begin(1)
    gather.begin_squares()
    edge_send(0, base)
    clear_all()
    slot()
    for pair in ((0, 2), (1, 3), (4, 5)):
        for k in pair:
            gather.got(k)
        if pair[0] == 0:
            edge_share(0)
        slot()
    gather.end()
    scales = edge_rows(0)
    column(0)
    slot()
    for layer in range(layers):
        unit = 2 * layer
        for i in (0, -1, 1, 2):
            for p in range(2):
                slot()
                net.group(unit, p, i)
                project(layer, p, i)
        mix(layer, scales)
        if layer + 1 < layers:
            net.all(unit + 1)
            reduce_chained(layer, base, own)
            gather = gathers[layer + 1]
            for k in (0, 3, 2, 1, 4, 5):
                gather.got(k)
                if k == 2:
                    edge_share(layer + 1)
                slot()
            gather.end()
            scales = edge_rows(layer + 1)
            column(layer + 1)
            slot()
        else:
            reduce_last(layer, own, base)
            result(top).wait()
            result(low).wait()
    for unit in range(2 * layers):
        net.drain(unit)


def whole_call(stream, gain, wv, wg, wo, taps, gates, rate, n_sp, n_tp):
    tokens, feats = stream.shape
    layers, rows, width = wv.shape
    half = tokens // 2
    blocks = width // 128
    hbm = pl.BlockSpec(memory_space=pl.ANY)
    f32 = pltpu.VMEM((tokens, width), F32)
    b16 = pltpu.VMEM((tokens, width), BF16)
    dma = pltpu.SemaphoreType.DMA
    return pl.pallas_call(
        functools.partial(whole_kernel, layers, n_sp, n_tp, float(gain.shape[1])),
        out_shape=jax.ShapeDtypeStruct((tokens, feats), BF16),
        in_specs=[hbm] * 8,
        out_specs=hbm,
        scratch_shapes=[
            pltpu.VMEM((layers, 2, n_sp, rows, width), BF16),
            pltpu.VMEM((layers, n_sp, rows, width), BF16),
            pltpu.VMEM((n_tp, tokens + EDGE, feats), BF16),
            pltpu.VMEM((layers, n_tp, 8, tokens), F32),
            pltpu.VMEM((layers, n_tp, 16, 128), BF16),
            pltpu.VMEM((layers, 2, 16, 128), BF16),
            pltpu.VMEM((layers, 16, 128), BF16),
            b16, b16,
            pltpu.VMEM((feats // 128, tokens, 128), F32),
            pltpu.VMEM((2, tokens + EDGE, width), F32),
            b16,
            pltpu.VMEM((tokens + 24, width), F32),
            f32, f32, b16,
            pltpu.VMEM((4, tokens, 512), F32),
            f32, f32, f32, f32,
            pltpu.VMEM((tokens, 128), F32),
            pltpu.VMEM((4, SEG, width), F32),
            pltpu.VMEM((2, SEG, width), F32),
            pltpu.VMEM((layers, 2, 8, 128), F32),
            pltpu.VMEM((layers, n_sp, 8, 128), F32),
            pltpu.VMEM((4, 2, tokens, feats // 2), BF16),
            pltpu.VMEM((4, 2, tokens, feats // 2), BF16),
            pltpu.VMEM((2, tokens, feats // 2), BF16),
            pltpu.VMEM((2, 2, half, feats // 2), BF16),
            pltpu.VMEM((4, 2, half, feats // 2), BF16),
            pltpu.VMEM((4, 2, half, feats // 2), BF16),
            b16,
            pltpu.VMEM(gain.shape, F32),
            pltpu.VMEM((layers, 4, width), F32),
            pltpu.VMEM(gates.shape, BF16),
            pltpu.VMEM((layers, 2, width), F32),
            dma((3 * layers,)),
            dma((5,)),
            dma((2,)),
            dma((4 * layers,)),
            dma((4 * layers, 16)),
            dma((1,)),
            dma((7,)),
            dma((layers,)),
            dma((layers,)),
            dma((layers, 2)),
            dma((layers, 2)),
            dma((layers,)),
            dma((layers,)),
            dma((layers,)),
            dma((layers,)),
            dma((1,)),
            dma((4, 2)),
            dma((1,)),
            dma((6, 2)),
        ],
        compiler_params=pltpu.CompilerParams(
            collective_id=0, has_side_effects=True, vmem_limit_bytes=63_000_000
        ),
        cost_estimate=pl.CostEstimate(flops=20_000_000_000, bytes_accessed=8_000_000, transcendentals=0),
        name="both_layers",
    )(stream, gain, wv, wg, wo, taps, gates, rate)


def per_device(
    n_sp, n_tp, stream_in, norm_gain, value_proj, gate_proj, out_proj, conv_taps, block_gates, forget_rate
):
    width = value_proj.shape[2]
    layers = value_proj.shape[0]
    gates = block_gates.reshape(layers, 4, width // 128, 128, 128)
    stream = whole_call(
        stream_in, norm_gain, value_proj, gate_proj, out_proj, conv_taps, gates, forget_rate, n_sp, n_tp
    )
    tokens, feats = stream.shape
    return stream.reshape(tokens // SEG, SEG, feats).transpose(1, 0, 2).reshape(tokens, feats)


def solution(mesh):
    placed = (
        P("sp", "tp"),
        P(),
        P(None, "sp", "tp"),
        P(None, "sp", "tp"),
        P(None, "sp", "tp"),
        P(),
        P(None, None, None, "tp", None),
        P(),
    )
    body = functools.partial(per_device, mesh.shape["sp"], mesh.shape["tp"])
    return jax.shard_map(body, mesh=mesh, in_specs=placed, out_specs=P("sp", "tp"), check_vma=False)
```

```python
import functools

import jax
import jax.numpy as jnp
from jax import lax
from jax.experimental import pallas as pl
from jax.experimental.pallas import tpu as pltpu
from jax.sharding import PartitionSpec as P

GATE_SCALE = 8.0
NORM_EPS = 1e-06
MESH = pl.DeviceIdType.MESH
F32 = jnp.float32
BF16 = jnp.bfloat16
EDGE = 16
SEG = 8
ROWS = 64
PLAN = ('0', '00', '00', '00', '01', '00', '00', '001', '1011', '1', '1', '', '1', '1', '', '', '', '', '11', '', '', '11112', '', '', '2', '2', '2', '2', '22', '', '2', '2', '222', '2', '3', '22', '', '3', '3', '', '', '', '', '', '33', '', '', '', '333', '3', '', '', '3', '', '', '33', '', '33', '3', '', '', '', '')


def remote(src, dst, send_sem, recv_sem, dev):
    return pltpu.make_async_remote_copy(
        src_ref=src, dst_ref=dst, send_sem=send_sem, recv_sem=recv_sem, device_id=dev, device_id_type=MESH
    )


def greet(groups):
    barrier = pltpu.get_barrier_semaphore()
    for axis, count, me in groups:
        for step in range(1, count):
            pl.semaphore_signal(barrier, inc=1, device_id={axis: lax.rem(me + step, count)}, device_id_type=MESH)
    return lambda: pl.semaphore_wait(barrier, sum(count - 1 for _, count, _ in groups))


def sigmoid(v):
    return 1.0 / (1.0 + jnp.exp(-v))


def drive_square(y):
    terms = [0.999999999543, -0.499999943611, 0.166665528456, -0.0416580188735, 0.00830184073719, -0.00132924407794, 0.000140574729006]
    total = jnp.full_like(y, terms[-1])
    for term in terms[-2::-1]:
        total = total * y + term
    return total * y


def in_row_steps(rows, body, size=ROWS, first=0):
    def step(k, carry):
        body(pl.ds(pl.multiple_of(first + k * size, size), size))
        return carry

    lax.fori_loop(0, rows // size, step, 0)


def aligned(at, size):
    return at if isinstance(at, int) else pl.multiple_of(at, size)


class Ring:
    def __init__(self, me, count):
        chips = count // 2
        self.chips = chips
        self.me = me
        self.x = me // 2
        self.c = lax.rem(me, 2)
        self.sib = self.x * 2 + 1 - self.c

    def at(self, step, other=False):
        core = 1 - self.c if other else self.c
        return lax.rem(self.x + step + self.chips, self.chips) * 2 + core


def gather_fill(own_ref, gain, xg, ssg, me, half=None):
    tokens = own_ref.shape[0]
    first, count = (0, tokens) if half is None else (half * tokens // 2, tokens // 2)

    def fill(rows):
        at = pl.ds(pl.multiple_of(first + rows.start, ROWS), rows.size)
        v = own_ref[at, :].astype(F32)
        xg[me, at, :] = (v * gain).astype(BF16)

    in_row_steps(count, fill)
    for k in range(first // 128, (first + count) // 128):
        v = own_ref[pl.ds(k * 128, 128), :].astype(F32)
        total = jnp.sum(v * v, axis=1, keepdims=True)
        ssg[me, :, pl.ds(k * 128, 128)] = jnp.broadcast_to(total, (128, 128)).T[0:8, :]


class Gather:
    def __init__(self, ring, xg, ssg, send, recv, ssend, srecv, count):
        self.ring, self.xg, self.ssg, self.count = ring, xg, ssg, count
        self.send, self.recv, self.ssend, self.srecv = send, recv, ssend, srecv
        half = (xg.shape[1] - EDGE) // 2
        self.rows = (pl.ds(0, half), pl.ds(half, half))

    def push(self, part, k, dev):
        remote(part, part, self.send.at[0], self.recv.at[min(k, 6)], {"tp": dev}).start()

    def begin(self, half):
        ring = self.ring
        part = self.xg.at[ring.me, self.rows[half]]
        right, left = ring.at(1), ring.at(-1)
        if half == 0:
            self.push(part, 0, right)
            self.push(part, 3, left)
            self.push(part, 6, ring.sib)
        else:
            self.push(part, 2, left)
            self.push(part, 1, right)
            self.push(part, 13, ring.sib)

    def begin_squares(self):
        ring, ssg = self.ring, self.ssg
        for step in range(1, self.count):
            dev = lax.rem(ring.me + step, self.count)
            remote(ssg.at[ring.me], ssg.at[ring.me], self.ssend, self.srecv, {"tp": dev}).start()

    def got(self, k):
        ring = self.ring
        step, half = {0: (-1, 0), 1: (-1, 1), 2: (1, 1), 3: (1, 0), 4: (2, 0), 5: (2, 1)}[k]
        part = self.xg.at[ring.at(step), self.rows[half]]
        remote(part, part, self.send.at[0], self.recv.at[k], {"tp": ring.sib}).wait_recv()
        if k == 0:
            self.push(part, 4, ring.at(1))
        if k == 2:
            self.push(part, 5, ring.at(-1))
        self.push(part, 7 + k, ring.sib)

    def end(self):
        count, dev = self.count, {"tp": self.ring.sib}
        half = self.rows[0].size
        came = self.xg.at[:, pl.ds(0, half)]
        remote(came, came, self.send.at[0], self.recv.at[6], dev).wait_recv()
        sent = self.xg.at[pl.ds(0, count - 1), pl.ds(0, 2 * half)]
        remote(sent, sent, self.send.at[0], self.recv.at[6], dev).wait_send()
        others = self.ssg.at[pl.ds(0, count - 1)]
        remote(others, others, self.ssend, self.srecv, dev).wait()


class Weights:
    def __init__(self, me, side, wvg, wo, gsend, grecv):
        self.y, self.z, self.side = lax.rem(me, side), me // side, side
        self.wvg, self.wo, self.gsend, self.grecv = wvg, wo, gsend, grecv
        self.waited = set()

    def idx(self, p, i, j):
        dy, dz = (i, j) if p == 0 else (j, i)
        return lax.rem(self.z + dz + self.side, self.side) * self.side + lax.rem(self.y + dy + self.side, self.side)

    def ref(self, unit, p, at):
        if unit % 2 == 0:
            return self.wvg.at[unit // 2, p, at]
        half = self.wo.shape[2] // 2
        return self.wo.at[unit // 2, at, pl.ds(p * half, half)]

    def push(self, unit, p, i, j, axis, d):
        ref = self.ref(unit, p, self.idx(p, i, j))
        di, dj = (d, 0) if axis == 0 else (0, d)
        slot = ((i - di) % 4) * 4 + (j - dj) % 4
        remote(
            ref, ref, self.gsend.at[2 * unit + p], self.grecv.at[2 * unit + p, slot], {"sp": self.idx(p, di, dj)}
        ).start()

    def arrive(self, unit, p, i, j):
        key = (unit, p, i % 4, j % 4)
        if key in self.waited or (i % 4, j % 4) == (0, 0):
            return
        self.waited.add(key)
        ref = self.ref(unit, p, self.idx(p, i, j))
        slot = (i % 4) * 4 + j % 4
        remote(
            ref, ref, self.gsend.at[2 * unit + p], self.grecv.at[2 * unit + p, slot], {"sp": self.idx(p, 1, 0)}
        ).wait_recv()

    def group(self, unit, p, i):
        for j in (0, -1, 1, 2):
            self.arrive(unit, p, i, j)

    def all(self, unit):
        for p in range(2):
            for i in (0, -1, 1, 2):
                self.group(unit, p, i)

    def opening(self, unit):
        for axis in range(2):
            for p in range(2):
                for d in (1, -1):
                    self.push(unit, p, 0, 0, axis, d)

    def events(self, unit):
        first = 1 if unit in (0, 3) else -1

        def turn(p, i, forward=None):
            def run():
                self.arrive(unit, p, i, 0)
                if forward:
                    self.push(unit, p, i, 0, 0, forward)
                for d in (1, -1):
                    self.push(unit, p, i, 0, 1, d)

            return run

        def relay(p, i):
            d = 1 if (i + unit) % 2 == 0 else -1

            def run():
                self.arrive(unit, p, i, -d)
                self.push(unit, p, i, -d, 1, d)

            return run

        both = range(2)
        steps = [turn(p, -first, first) for p in both] + [turn(p, first) for p in both]
        steps += [relay(p, 0) for p in both] + [turn(p, 2) for p in both]
        return steps + [relay(p, i) for i in (-1, 1, 2) for p in both]

    def drain(self, unit):
        for p in range(2):
            if unit % 2 == 0:
                ref = self.wvg.at[unit // 2, p, pl.ds(0, 15)]
            else:
                half = self.wo.shape[2] // 2
                ref = self.wo.at[unit // 2, pl.ds(0, 15), pl.ds(p * half, half)]
            remote(ref, ref, self.gsend.at[2 * unit + p], self.grecv.at[2 * unit + p, 0], {"sp": self.idx(p, 1, 0)}).wait_send()


def whole_kernel(
    layers, n_sp, n_tp, features,
    stream_hbm, gain_hbm, wv_hbm, wg_hbm, wo_hbm, taps_hbm, gates_hbm, rate_hbm, out_hbm,
    wvg, wo, xg, ssg, edge, near, tok, base, own, perm, acc, mixb, mpad, sil, conv, convb, big, a_f, u_f, a_b, u_b, col,
    seg, ent, msg, slots,
    psend, precv, fbuf, far_in, nbuf, near_in,
    stream_ref, gain_ref, taps_ref, gates_ref, rate_ref, ld, ins, outs, gsend, grecv, asend, arecv, ssend, srecv, hsend, hrecv, esend, erecv, csend, crecv, ds, dr, rs, rr,
):
    sp, tp = lax.axis_index("sp"), lax.axis_index("tp")
    tokens, width = mixb.shape
    feats = own.shape[1]
    joined = greet((("sp", n_sp, sp), ("tp", n_tp, tp)))
    ring = Ring(tp, n_tp)
    net = Weights(sp, 4, wvg, wo, gsend, grecv)
    pre = pown = big
    lanes_own = pl.ds(pl.multiple_of(tp * width, width), width)
    right, left = ring.at(1), ring.at(-1)

    inputs = [
        pltpu.make_async_copy(stream_hbm, stream_ref, ins.at[0]),
        pltpu.make_async_copy(gain_hbm, gain_ref, ins.at[1]),
        pltpu.make_async_copy(taps_hbm.at[:, :, lanes_own], taps_ref, ins.at[2]),
        pltpu.make_async_copy(gates_hbm, gates_ref, ins.at[3]),
        pltpu.make_async_copy(rate_hbm.at[:, :, lanes_own], rate_ref, ins.at[4]),
    ]
    for copy in inputs:
        copy.start()
    loads = []
    for layer in range(layers):
        loads.append([
            pltpu.make_async_copy(wv_hbm.at[layer], wvg.at[layer, 0, sp], ld.at[3 * layer]),
            pltpu.make_async_copy(wg_hbm.at[layer], wvg.at[layer, 1, sp], ld.at[3 * layer + 1]),
        ])
        loads.append([pltpu.make_async_copy(wo_hbm.at[layer], wo.at[layer, sp], ld.at[3 * layer + 2])])
    for copies in loads:
        for copy in copies:
            copy.start()
    def opening(unit):
        for copy in loads[unit]:
            copy.wait()
        net.opening(unit)

    waiting = [iter([functools.partial(opening, unit)] + net.events(unit)) for unit in range(2 * layers)]
    plan = iter(PLAN)

    def slot():
        for unit in next(plan):
            next(waiting[int(unit)])()

    def project(layer, p, i):
        if p == 0:
            spots = [net.idx(p, i, j) for j in range(4)]
            halves = [pl.ds(pl.multiple_of(lax.rem(at, 2) * 256, 256), 256) for at in spots]
            terms = [
                jnp.dot(xg[at // 2, :, lanes], wvg[layer, p, at], preferred_element_type=F32)
                for at, lanes in zip(spots, halves)
            ]
        else:
            first = lax.rem(net.z + i + net.side, net.side) * 2
            terms = [
                jnp.dot(
                    xg[first + j, 0:tokens, :],
                    wvg[layer, p, pl.ds(2 * (first + j), 2)].reshape(feats, width),
                    preferred_element_type=F32,
                )
                for j in range(2)
            ]
        total = functools.reduce(jnp.add, terms)
        acc[p, 0 : total.shape[0], :] += total

    def edge_send(layer, source):
        ends = (source[0:16, :].astype(F32), source[tokens - 16 : tokens, :].astype(F32))
        spots = ((0, 0), (1, 7), (1, 15))
        lines = [
            ends[side][row : row + 1, b * 128 : (b + 1) * 128] for side, row in spots for b in range(feats // 128)
        ]
        tok[layer] = jnp.concatenate(lines + [jnp.zeros((16 - len(lines), 128), F32)], axis=0).astype(BF16)
        for k in range(2):
            edge_copy(layer, k).start()

    def edge_copy(layer, k):
        place = lax.rem(sp + (1 if k == 0 else n_sp - 1), n_sp)
        return remote(tok.at[layer], near.at[layer, k], hsend.at[layer, k], hrecv.at[layer, k], {"sp": place})

    def edge_share(layer):
        for k in range(2):
            edge_copy(layer, k).wait()
        rows = lax.broadcasted_iota(jnp.int32, (16, 128), 0)
        after = jnp.where(sp < n_sp - 1, near[layer, 1].astype(F32), 0.0)
        before = jnp.where(sp > 0, near[layer, 0].astype(F32), 0.0)
        edge[layer, tp] = jnp.where(rows < 4, after, before).astype(BF16)
        for step in range(1, n_tp):
            dev = lax.rem(tp + step, n_tp)
            remote(
                edge.at[layer, tp], edge.at[layer, tp], esend.at[layer], erecv.at[layer], {"tp": dev}
            ).start()

    def edge_rows(layer):
        whole = edge.at[layer, pl.ds(0, n_tp - 1)]
        remote(whole, whole, esend.at[layer], erecv.at[layer], {"tp": ring.sib}).wait()
        squares = jnp.zeros((16, 128), F32)
        for block in range(n_tp):
            values = edge[layer, block].astype(F32)
            squares = squares + values * values
            lines = []
            for r in range(3):
                parts = [values[4 * r + b : 4 * r + b + 1, :] for b in range(feats // 128)]
                lines.append(jnp.concatenate(parts, axis=1))
            gain = gain_ref[layer : layer + 1, pl.ds(block * feats, feats)]
            rows = jnp.concatenate(lines, axis=0) * gain
            filled = jnp.concatenate([rows, jnp.zeros((EDGE - 3, feats), F32)], axis=0)
            xg[block, pl.ds(tokens, EDGE), :] = filled.astype(BF16)
        sums = jnp.sum(squares, axis=1, keepdims=True)
        return [
            lax.rsqrt(jnp.sum(sums[4 * r : 4 * r + 4, :], axis=0, keepdims=True) / features + NORM_EPS)
            for r in range(3)
        ]

    gathers = [
        Gather(ring, xg, ssg.at[layer], asend, arecv, ssend.at[layer], srecv.at[layer], n_tp)
        for layer in range(layers)
    ]

    def project_all(layer, p):
        rows = pl.ds(0, tokens + EDGE if p == 0 else tokens)

        def four(first):
            terms = [
                jnp.dot(
                    xg[block, rows, :],
                    wvg[layer, p, 2 * block : 2 * block + 2].reshape(feats, width),
                    preferred_element_type=F32,
                )
                for block in range(first, first + 4)
            ]
            return functools.reduce(jnp.add, terms)

        acc[p, rows, :] = four(0)
        acc[p, rows, :] += four(4)

    def gather_own(layer, source, half=None):
        gain = gain_ref[layer : layer + 1, lanes_own]
        gather_fill(source, gain, xg, ssg.at[layer], tp, half)

    def column(layer):
        total = jnp.sum(ssg[layer], axis=0)
        scale = lax.rsqrt(total / features + NORM_EPS)
        for k in range(tokens // 128):
            part = jnp.broadcast_to(scale[0:1, k * 128 : (k + 1) * 128], (128, 128))
            col[pl.ds(k * 128, 128), :] = part.T

    def clear(rows):
        zero = jnp.zeros((rows.size, width), F32)
        acc[0, rows, :] = zero
        acc[1, rows, :] = zero

    def clear_all():
        in_row_steps(tokens, clear, 32)
        acc[0, pl.ds(tokens, EDGE), :] = jnp.zeros((EDGE, width), F32)

    def mix(layer, scales):
        def finish_v(rows):
            wide = jnp.concatenate([col[rows, :]] * (width // 128), axis=1)
            value = (acc[0, rows, :] * wide).astype(BF16)
            mixb[rows, :] = value
            acc[0, rows, :] = value.astype(F32)

        if not layer:
            for copy in inputs[2:]:
                copy.wait()

        def finish_g(rows):
            wide = jnp.concatenate([col[rows, :]] * (width // 128), axis=1)
            gate = (acc[1, rows, :] * wide).astype(BF16).astype(F32)
            sil[rows, :] = gate * sigmoid(gate)
            mpad[pl.ds(aligned(rows.start + 16, 16), rows.size), :] = acc[0, rows, :]

        in_row_steps(tokens, finish_v, 32)
        in_row_steps(tokens, finish_g, 32)
        slot()
        edges = [
            (acc[0, tokens + r : tokens + r + 1, :] * scales[r]).astype(BF16).astype(F32) for r in range(3)
        ]
        sub = lax.broadcasted_iota(jnp.int32, (SEG, width), 0)
        for k in range(2):
            blk = acc[0, pl.ds(tokens - 16 + 8 * k, 8), :]
            mpad[pl.ds(8 * k, 8), :] = jnp.where(
                sub == 0, jnp.broadcast_to(edges[1 + k], (SEG, width)), pltpu.roll(blk, 1, 0)
            )
        blk = acc[0, pl.ds(0, 8), :]
        mpad[pl.ds(tokens + 16, 8), :] = jnp.where(
            sub == SEG - 1, jnp.broadcast_to(edges[0], (SEG, width)), pltpu.roll(blk, SEG - 1, 0)
        )
        taps = taps_ref[layer]
        maps = [jnp.concatenate([gates_ref[layer, g, b] for g in range(4)], axis=1) for b in range(width // 128)]

        def gate_maps(rows):
            for b in range(width // 128):
                pre[b, rows, :] = jnp.dot(convb[rows, b * 128 : (b + 1) * 128], maps[b], preferred_element_type=F32)

        def convolve(rows):
            terms = [
                mpad[pl.ds(aligned(rows.start + 8 * k, 8), rows.size), :] * taps[k : k + 1, :]
                for k in range(4)
            ]
            value = (terms[0] + terms[1]) + (terms[2] + terms[3])
            conv[rows, :] = value
            convb[rows, :] = value.astype(BF16)

        in_row_steps(tokens, convolve, 32)
        slot()
        gate_maps(pl.ds(0, tokens))
        slot()
        rate_all = -GATE_SCALE * rate_ref[layer]
        for b in range(width // 128):
            lanes = pl.ds(b * 128, 128)
            rates = [rate_all[e : e + 1, b * 128 : (b + 1) * 128] for e in range(2)]

            def body(k, carry, b=b, lanes=lanes, rates=rates):
                p_f, h_f, p_b, h_b = carry
                rows = pl.ds(pl.multiple_of(k * ROWS, ROWS), ROWS)
                cv = conv[rows, lanes]
                kept = []
                for e, (a_ref, u_ref) in enumerate(((a_f, u_f), (a_b, u_b))):
                    r = sigmoid(pre[b, rows, 256 * e : 256 * e + 128])
                    i = sigmoid(pre[b, rows, 256 * e + 128 : 256 * e + 256])
                    log_a = rates[e] * r
                    decay = jnp.exp(log_a)
                    drive = jnp.sqrt(drive_square(-2.0 * log_a)) * i * cv
                    a_ref[rows, lanes] = decay
                    u_ref[rows, lanes] = drive
                    kept.append((decay, drive))
                for j in range(ROWS // 8):
                    at = slice(8 * j, 8 * j + 8)
                    d, u = kept[0][0][at], kept[0][1][at]
                    h_f = d * h_f + u
                    p_f = p_f * d
                    d, u = kept[1][0][at], kept[1][1][at]
                    h_b = h_b + p_b * u
                    p_b = p_b * d
                return p_f, h_f, p_b, h_b

            one, zero = jnp.ones((SEG, 128), F32), jnp.zeros((SEG, 128), F32)
            ends = lax.fori_loop(0, tokens // ROWS, body, (one, zero, one, zero))
            for k in range(4):
                seg[k, :, lanes] = ends[k]
            slot()

        sides = ((0, range(SEG)), (2, range(SEG - 1, -1, -1)))
        for e, (k, order) in enumerate(sides):
            prod = jnp.ones((1, width), F32)
            state = jnp.zeros((1, width), F32)
            for s in order:
                d = seg[k, s : s + 1, :]
                state = d * state + seg[k + 1, s : s + 1, :]
                prod = prod * d
            for b in range(width // 128):
                msg[layer, e, b : b + 1, :] = prod[:, b * 128 : (b + 1) * 128]
                msg[layer, e, 4 + b : 5 + b, :] = state[:, b * 128 : (b + 1) * 128]
        cs, cr = csend.at[layer], crecv.at[layer]
        for step in range(1, n_sp):
            dev = lax.rem(sp + step, n_sp)
            side = jnp.where(dev > sp, 0, 1)
            remote(msg.at[layer, side], slots.at[layer, sp], cs, cr, {"sp": dev}).start()
        slots[layer, sp] = jnp.zeros((8, 128), F32)
        slot()
        others = slots.at[layer, pl.ds(0, n_sp - 1)]
        remote(others, others, cs, cr, {"sp": lax.rem(sp + 1, n_sp)}).wait()
        for e, (k, order) in enumerate(sides):
            carry = jnp.zeros((4, 128), F32)
            for q in range(n_sp) if e == 0 else range(n_sp - 1, -1, -1):
                live = (q < sp) if e == 0 else (q > sp)
                entry = slots[layer, q]
                carry = jnp.where(live, entry[0:4] * carry + entry[4:8], carry)
            state = jnp.concatenate([carry[b : b + 1, :] for b in range(width // 128)], axis=1)
            for s in order:
                ent[e, s : s + 1, :] = state
                state = seg[k, s : s + 1, :] * state + seg[k + 1, s : s + 1, :]
        def again(k, carry):
            h_f, h_b = carry
            for j in range(4):
                fwd = pl.ds(pl.multiple_of((4 * k + j) * SEG, SEG), SEG)
                bwd = pl.ds(pl.multiple_of((steps - 1 - 4 * k - j) * SEG, SEG), SEG)
                h_f = a_f[fwd, :] * h_f + u_f[fwd, :]
                u_f[fwd, :] = h_f
                h_b = a_b[bwd, :] * h_b + u_b[bwd, :]
                u_b[bwd, :] = h_b
            return h_f, h_b

        lax.fori_loop(0, steps // 4, again, (ent[0], ent[1]))

        def gated(rows):
            mixb[rows, :] = ((u_f[rows, :] + u_b[rows, :]) * sil[rows, :]).astype(BF16)

        in_row_steps(tokens, gated, 32)
        slot()

    half = tokens // 2
    top, low = pl.ds(0, half), pl.ds(half, half)

    def result(rows):
        return pltpu.make_async_copy(base.at[rows], out_hbm.at[rows], outs.at[rows.start // half])

    class Reduce:
        order = (2, 1, -1, 0)

        def __init__(self, layer, first, count, shard):
            self.layer, self.first, self.parts, self.shard = layer, first, range(first, first + count), shard
            self.sel = pl.ds(first, count)

        def product(self, k, other, part):
            return lax.dot_general(
                mixb[...],
                wo[self.layer, self.shard(self.order[k], other, part)],
                (((1,), (1,)), ((), ())),
                preferred_element_type=F32,
            )

        def across(self, k):
            return remote(
                psend.at[k, self.sel], precv.at[k, self.sel], ds.at[0], dr.at[k, self.first], {"tp": ring.sib}
            )

        def send(self, k, src, dst, dev):
            remote(src, dst, rs.at[0], rr.at[k, self.first], {"tp": dev}).start()

        def arrived(self, k, dst):
            remote(dst, dst, rs.at[0], rr.at[k, self.first], {"tp": right}).wait_recv()

        def paired(self, k, rows, into=None):
            def body(r):
                at = pl.ds(pl.multiple_of(rows.start + r.start, 32), r.size)
                for part in self.parts:
                    lanes = pl.ds(part * 256, 256)
                    value = pown[k, at, lanes] + precv[k, part, at, :].astype(F32)
                    if into is None:
                        pown[k, at, lanes] = value
                    elif into is fbuf:
                        fbuf[part, at, :] = value.astype(BF16)
                    else:
                        nbuf[into, part, r, :] = value.astype(BF16)

            in_row_steps(rows.size, body, 32)

        def near(self, k, dev):
            self.send(2 + k, nbuf.at[k, self.sel], near_in.at[k, self.sel], dev)

        def opening(self, chained):
            for k in range(4):
                others = [self.product(k, True, part) for part in self.parts]
                kept = [self.product(k, False, part) for part in self.parts]
                for part, term in zip(self.parts, others):
                    psend[k, part] = term.astype(BF16)
                for part, term in zip(self.parts, kept):
                    pown[k, :, part * 256 : (part + 1) * 256] = term
                self.across(k).start()
                if k == 1:
                    self.across(0).wait_recv()
                    self.paired(0, top, fbuf)
                    self.send(0, fbuf.at[self.sel, top], far_in.at[0, self.sel], right)
                    self.paired(0, low, fbuf)
                    self.send(1, fbuf.at[self.sel, low], far_in.at[1, self.sel], left)
                if k == 2:
                    self.across(1).wait_recv()
                    self.paired(1, low, 0)
                    if not chained:
                        self.near(0, right)
                    self.paired(1, top)
                if k == 3:
                    self.across(2).wait_recv()
                    self.paired(2, top, 1)
                    self.near(1, left)
                    self.paired(2, low)
                if chained or not self.first:
                    slot()
            self.across(3).wait_recv()
            self.paired(3, pl.ds(0, tokens))

        def merge(self, k, rows, side):
            self.arrived(side, far_in.at[side, self.sel])

            def body(r):
                at = pl.ds(pl.multiple_of(rows.start + r.start, 32), r.size)
                for part in self.parts:
                    value = pown[k, at, pl.ds(part * 256, 256)] + far_in[side, part, r, :].astype(F32)
                    nbuf[2 + side, part, r, :] = value.astype(BF16)

            in_row_steps(half, body, 32)
            self.near(2 + side, left if side else right)

        def merges(self, chained):
            self.merge(1, top, 0)
            if chained:
                self.near(0, right)
            self.merge(2, low, 1)

        def got(self, k):
            self.arrived(2 + k, near_in.at[k, self.sel])

        def total(self, rows, one, two, source, target, column=None):
            def body(r):
                at = pl.ds(pl.multiple_of(rows.start + r.start, 32), r.size)
                for part in self.parts:
                    lanes = pl.ds(part * 256, 256)
                    branch = pown[3, at, lanes] + near_in[one, part, r, :].astype(F32)
                    branch = branch + near_in[two, part, r, :].astype(F32)
                    spot = lanes if column is None else column
                    target[at, spot] = (source[at, spot].astype(F32) + branch).astype(BF16)

            in_row_steps(half, body, 32)

    def reduce_done():
        remote(psend, precv, ds.at[0], dr.at[0, 0], {"tp": ring.sib}).wait_send()
        six = psend.at[pl.ds(0, 3)]
        remote(six, six, rs.at[0], rr.at[0, 0], {"tp": right}).wait_send()

    def reduce_chained(layer, source, target):
        work = Reduce(layer, 0, 2, lambda step, other, part: 2 * ring.at(step, other=other) + part)
        work.opening(True)
        slot()
        work.merges(True)
        slot()
        gather = gathers[layer + 1]
        work.got(1)
        slot()
        work.got(2)
        work.total(top, 1, 2, source, target)
        gather_own(layer + 1, target, 0)
        gather.begin(0)
        slot()
        work.got(0)
        slot()
        work.got(3)
        work.total(low, 0, 3, source, target)
        gather_own(layer + 1, target, 1)
        gather.begin(1)
        gather.begin_squares()
        edge_send(layer + 1, target)
        clear_all()
        slot()
        reduce_done()

    def reduce_last(layer, source, target):
        unit = 2 * layer + 1

        def stage(first, near_y, far_y):
            ya, yb = (lax.rem(net.y + d + net.side, net.side) for d in (near_y, far_y))
            mine = jnp.where(ya // 2 == ring.c, ya, yb)
            theirs = jnp.where(ya // 2 == ring.c, yb, ya)

            def shard(step, other, part):
                z = lax.rem(ring.x + step + ring.chips, ring.chips)
                return z * net.side + (theirs if other else mine)

            column = pl.ds(pl.multiple_of(lax.rem(mine, 2) * 256, 256), 256)
            return Reduce(layer, first, 1, shard), column

        one, one_column = stage(0, 1, -1)
        two, two_column = stage(1, 0, 2)
        for i in (-1, 1):
            net.group(unit, 0, i)
        for i in (0, -1, 1, 2):
            for j in (-1, 1):
                net.arrive(unit, 1, i, j)
        one.opening(False)
        slot()
        one.merges(False)
        slot()
        net.all(unit)
        two.opening(False)
        for k in range(4):
            one.got(k)
        one.total(top, 1, 2, source, target, one_column)
        one.total(low, 0, 3, source, target, one_column)
        two.merges(False)
        for k in range(4):
            two.got(k)
        two.total(top, 1, 2, source, target, two_column)
        result(top).start()
        two.total(low, 0, 3, source, target, two_column)
        result(low).start()
        reduce_done()

    steps = tokens // SEG

    def spread(rows):
        for b in range(feats // 128):
            perm[b, rows, :] = stream_ref[rows, b * 128 : (b + 1) * 128].astype(F32)

    def collect(rows):
        first = rows.start // SEG
        for b in range(feats // 128):
            parts = [perm[b, pl.ds(first + j, SEG, stride=steps), :] for j in range(rows.size // SEG)]
            base[rows, b * 128 : (b + 1) * 128] = jnp.concatenate(parts, axis=0).astype(BF16)

    inputs[0].wait()
    in_row_steps(tokens, spread)
    in_row_steps(tokens, collect, 32)
    inputs[1].wait()
    gather_own(0, base)
    joined()

    slot()
    gather = gathers[0]
    gather.begin(0)
    gather.begin(1)
    gather.begin_squares()
    edge_send(0, base)
    clear_all()
    slot()
    for pair in ((0, 2), (1, 3), (4, 5)):
        for k in pair:
            gather.got(k)
        if pair[0] == 0:
            edge_share(0)
        slot()
    gather.end()
    scales = edge_rows(0)
    column(0)
    slot()
    for layer in range(layers):
        unit = 2 * layer
        for i in (0, -1, 1, 2):
            for p in range(2):
                slot()
                net.group(unit, p, i)
                if not layer:
                    project(layer, p, i)
        if layer:
            for p in range(2):
                project_all(layer, p)
        mix(layer, scales)
        if layer + 1 < layers:
            net.all(unit + 1)
            reduce_chained(layer, base, own)
            gather = gathers[layer + 1]
            for k in (0, 3, 2, 1, 4, 5):
                gather.got(k)
                if k == 2:
                    edge_share(layer + 1)
                slot()
            gather.end()
            scales = edge_rows(layer + 1)
            column(layer + 1)
            slot()
        else:
            reduce_last(layer, own, base)
            result(top).wait()
            result(low).wait()
    for unit in range(2 * layers):
        net.drain(unit)


def whole_call(stream, gain, wv, wg, wo, taps, gates, rate, n_sp, n_tp):
    tokens, feats = stream.shape
    layers, rows, width = wv.shape
    half = tokens // 2
    blocks = width // 128
    hbm = pl.BlockSpec(memory_space=pl.ANY)
    f32 = pltpu.VMEM((tokens, width), F32)
    b16 = pltpu.VMEM((tokens, width), BF16)
    dma = pltpu.SemaphoreType.DMA
    return pl.pallas_call(
        functools.partial(whole_kernel, layers, n_sp, n_tp, float(gain.shape[1])),
        out_shape=jax.ShapeDtypeStruct((tokens, feats), BF16),
        in_specs=[hbm] * 8,
        out_specs=hbm,
        scratch_shapes=[
            pltpu.VMEM((layers, 2, n_sp, rows, width), BF16),
            pltpu.VMEM((layers, n_sp, rows, width), BF16),
            pltpu.VMEM((n_tp, tokens + EDGE, feats), BF16),
            pltpu.VMEM((layers, n_tp, 8, tokens), F32),
            pltpu.VMEM((layers, n_tp, 16, 128), BF16),
            pltpu.VMEM((layers, 2, 16, 128), BF16),
            pltpu.VMEM((layers, 16, 128), BF16),
            b16, b16,
            pltpu.VMEM((feats // 128, tokens, 128), F32),
            pltpu.VMEM((2, tokens + EDGE, width), F32),
            b16,
            pltpu.VMEM((tokens + 24, width), F32),
            f32, f32, b16,
            pltpu.VMEM((4, tokens, 512), F32),
            f32, f32, f32, f32,
            pltpu.VMEM((tokens, 128), F32),
            pltpu.VMEM((4, SEG, width), F32),
            pltpu.VMEM((2, SEG, width), F32),
            pltpu.VMEM((layers, 2, 8, 128), F32),
            pltpu.VMEM((layers, n_sp, 8, 128), F32),
            pltpu.VMEM((4, 2, tokens, feats // 2), BF16),
            pltpu.VMEM((4, 2, tokens, feats // 2), BF16),
            pltpu.VMEM((2, tokens, feats // 2), BF16),
            pltpu.VMEM((2, 2, half, feats // 2), BF16),
            pltpu.VMEM((4, 2, half, feats // 2), BF16),
            pltpu.VMEM((4, 2, half, feats // 2), BF16),
            b16,
            pltpu.VMEM(gain.shape, F32),
            pltpu.VMEM((layers, 4, width), F32),
            pltpu.VMEM(gates.shape, BF16),
            pltpu.VMEM((layers, 2, width), F32),
            dma((3 * layers,)),
            dma((5,)),
            dma((2,)),
            dma((4 * layers,)),
            dma((4 * layers, 16)),
            dma((1,)),
            dma((7,)),
            dma((layers,)),
            dma((layers,)),
            dma((layers, 2)),
            dma((layers, 2)),
            dma((layers,)),
            dma((layers,)),
            dma((layers,)),
            dma((layers,)),
            dma((1,)),
            dma((4, 2)),
            dma((1,)),
            dma((6, 2)),
        ],
        compiler_params=pltpu.CompilerParams(
            collective_id=0, has_side_effects=True, vmem_limit_bytes=63_000_000
        ),
        cost_estimate=pl.CostEstimate(flops=20_000_000_000, bytes_accessed=8_000_000, transcendentals=0),
        name="both_layers",
    )(stream, gain, wv, wg, wo, taps, gates, rate)


def per_device(
    n_sp, n_tp, stream_in, norm_gain, value_proj, gate_proj, out_proj, conv_taps, block_gates, forget_rate
):
    width = value_proj.shape[2]
    layers = value_proj.shape[0]
    gates = block_gates.reshape(layers, 4, width // 128, 128, 128)
    stream = whole_call(
        stream_in, norm_gain, value_proj, gate_proj, out_proj, conv_taps, gates, forget_rate, n_sp, n_tp
    )
    tokens, feats = stream.shape
    return stream.reshape(tokens // SEG, SEG, feats).transpose(1, 0, 2).reshape(tokens, feats)


def solution(mesh):
    placed = (
        P("sp", "tp"),
        P(),
        P(None, "sp", "tp"),
        P(None, "sp", "tp"),
        P(None, "sp", "tp"),
        P(),
        P(None, None, None, "tp", None),
        P(),
    )
    body = functools.partial(per_device, mesh.shape["sp"], mesh.shape["tp"])
    return jax.shard_map(body, mesh=mesh, in_specs=placed, out_specs=P("sp", "tp"), check_vma=False)
```
